512 devices in a mesh: sp: 64 (over z, y), tp: 8 (over x, core).
Axes of the slice: x: 4, y: 8, z: 8, core: 2. Of those that a mesh axis runs over, the one named last changes fastest.
Arguments:
- tokens: bfloat16 [8192, 2048], P('sp', 'tp'), may hold values from -6 to 6
- pre_gain: float32 [2048], replicated, may hold values from 0.1 to 1.9
- w_query_stick: bfloat16 [2048, 1024], P(None, 'tp'), may hold values from -0.125 to 0.125
- w_key_stick: bfloat16 [2048, 1024], P(None, 'tp'), may hold values from -0.125 to 0.125
- w_value_stick: bfloat16 [2048, 1024], P(None, 'tp'), may hold values from -2 to 2, as said below
- w_query_window: bfloat16 [2048, 1024], P(None, 'tp'), may hold values from -20 to 20, as said below
- w_key_window: bfloat16 [2048, 512], P(None, 'tp'), may hold values from -1 to 1, as said below
- w_value_window: bfloat16 [2048, 512], P(None, 'tp'), may hold values from -2 to 2, as said below
- stick_bias: float32 [16], P('tp'), may hold values from -14 to -3
- sinks: float32 [16], P('tp'), may hold values from 2 to 6
- stick_gain: float32 [1024], P('tp'), may hold values from 0.1 to 1.9
- window_gain: float32 [1024], P('tp'), may hold values from 0.1 to 1.9
- w_out_stick: bfloat16 [1024, 2048], P('tp'), may hold values from -0.125 to 0.125
- w_out_window: bfloat16 [1024, 2048], P('tp'), may hold values from -0.125 to 0.125
- post_gain: float32 [2048], replicated, may hold values from 0.1 to 1.9
Outputs:
- layer_out: bfloat16 [8192, 2048], P(('sp', 'tp'))
The draws below stay inside these ranges and needn't reach their ends.
Inputs may be any that keep to these rules, and one draw needn't show every extreme that they name: `w_key_window`: key weights of the windowed heads. `w_query_window`: query weights of the windowed heads. `w_value_stick`: value weights of the stick-breaking heads. `w_value_window`: value weights of the windowed heads.
All inputs are finite; a program needn't handle non-finite values.
Results may differ from the reference program's by a relative error of at most 0.018.
Values may be sent and summed in bfloat16 or wider, within the bound.
A program may use at most 64 MiB of HBM per device.

```python
import jax
import jax.numpy as jnp
from jax import lax

D = 2048
HEAD_DIM = 64
SB_HEADS = 16
SW_KV_HEADS = 8
GROUP = 2
WINDOW = 128
TOK_DEV = 128
TOKENS = 8192
SW_HEADS = 16
SB_WIDTH = 1024
SW_WIDTH = 1024


def clipped_normal(key, shape):
    return jnp.clip(jax.random.normal(key, shape, jnp.float32), -4.0, 4.0)


def window_pair(key):
    salted = jax.random.fold_in(key, 17)
    keys_w = clipped_normal(jax.random.fold_in(salted, 1), (D, SW_KV_HEADS * HEAD_DIM)) * D ** (-0.5)
    queries_w = clipped_normal(jax.random.fold_in(salted, 2), (D, SW_HEADS * HEAD_DIM)) * D ** (-0.5)
    return (keys_w, queries_w)


def draw_w_key_window(key, part):
    return window_pair(key)[0].astype(jnp.bfloat16)


def draw_w_query_window(key, part):
    keys_w, queries_w = window_pair(key)
    return queries_w.astype(jnp.bfloat16)


def scaled_values(key, salt, head_count):
    salted = jax.random.fold_in(key, salt)
    head_scale = jnp.exp(jax.random.uniform(jax.random.fold_in(salted, 1), (head_count,), jnp.float32, -1.2, 1.2))
    normals = clipped_normal(jax.random.fold_in(salted, 2), (D, head_count * HEAD_DIM)) * D ** (-0.5)
    return normals * jnp.repeat(head_scale, HEAD_DIM)[None, :]


def draw_w_value_stick(key, part):
    return scaled_values(key, 23, SB_HEADS).astype(jnp.bfloat16)


def draw_w_value_window(key, part):
    return scaled_values(key, 31, SW_KV_HEADS).astype(jnp.bfloat16)


def draw_stick_bias(key, part):
    salted = jax.random.fold_in(key, 29)
    slow_bias = -jnp.log(TOKENS * 1.0) - jax.random.uniform(jax.random.fold_in(salted, 1), (SB_HEADS,), jnp.float32, 0.0, 1.0)
    fast_bias = jax.random.uniform(jax.random.fold_in(salted, 2), (SB_HEADS,), jnp.float32, -4.0, -3.5)
    chosen = jax.random.permutation(jax.random.fold_in(salted, 3), SB_HEADS) < SB_HEADS // 2
    return jnp.where(chosen, slow_bias, fast_bias)


def steps_of(own_key, shape, split, smallest, high):
    def one(position, blocks):
        heights = jax.random.uniform(jax.random.fold_in(jax.random.fold_in(own_key, 6), position), (blocks,), jnp.float32, smallest / len(split), high / len(split))
        return jnp.repeat(jnp.exp(heights), shape[position] // blocks).reshape((-1,) + (1,) * (len(shape) - position - 1))

    level = one(*split[0])
    for cut in split[1:]:
        level = level * one(*cut)
    return level


def scatter_about(own_key, shape, width, most, split=(), held_as=jnp.bfloat16):
    values = width * jax.random.normal(own_key, shape, jnp.float32)
    if split:
        values = values * steps_of(own_key, shape, split, -0.22, 0.18)
    return jnp.clip(values, -most, most).astype(held_as)


def setup_inputs(seed: int = 0) -> dict:
    key_of = jax.random.split(jax.random.key(seed), 16)
    return {
        "tokens": scatter_about(key_of[0], (TOKENS, D), 1.0, 6.0, ((0, 64), (1, 8))),
        "pre_gain": jnp.clip(1.0 + 0.18 * jax.random.normal(key_of[1], (D,), jnp.float32), 0.1, 1.9),
        "w_query_stick": scatter_about(key_of[2], (D, SB_WIDTH), D ** -0.5, 0.125, ((1, 8),)),
        "w_key_stick": scatter_about(key_of[3], (D, SB_WIDTH), D ** -0.5, 0.125, ((1, 8),)),
        "w_value_stick": draw_w_value_stick(jax.random.fold_in(key_of[15], 71), 0),
        "w_query_window": draw_w_query_window(jax.random.fold_in(key_of[15], 71), 0),
        "w_key_window": draw_w_key_window(jax.random.fold_in(key_of[15], 71), 0),
        "w_value_window": draw_w_value_window(jax.random.fold_in(key_of[15], 71), 0),
        "stick_bias": draw_stick_bias(jax.random.fold_in(key_of[15], 71), 0),
        "sinks": jnp.clip(2.0 + 4.0 * jax.random.uniform(key_of[9], (SW_HEADS,), jnp.float32) ** steps_of(key_of[9], (SW_HEADS,), ((0, 8),), -0.2, 0.2), 2.0, 6.0),
        "stick_gain": jnp.clip(1.0 + 0.18 * jax.random.normal(key_of[10], (SB_WIDTH,), jnp.float32), 0.1, 1.9),
        "window_gain": jnp.clip(1.0 + 0.18 * jax.random.normal(key_of[11], (SW_WIDTH,), jnp.float32), 0.1, 1.9),
        "w_out_stick": scatter_about(key_of[12], (SB_WIDTH, D), (SB_WIDTH + SW_WIDTH) ** -0.5, 0.125, ((0, 8),)),
        "w_out_window": scatter_about(key_of[13], (SW_WIDTH, D), (SB_WIDTH + SW_WIDTH) ** -0.5, 0.125, ((0, 8),)),
        "post_gain": jnp.clip(1.0 + 0.18 * jax.random.normal(key_of[14], (D,), jnp.float32), 0.1, 1.9),
    }


epsilon = 1e-06

def rounded(values):
    return lax.optimization_barrier(values.astype(jnp.bfloat16)).astype(jnp.float32)

def norm_rows(values, gain):
    stats = lax.optimization_barrier(jnp.mean(values * values, axis=-1, keepdims=True))
    return values * lax.rsqrt(stats + epsilon) * gain

def stick_attention(queries, key_rows, values, stick_bias):
    blocks = TOKENS // TOK_DEV
    q_blocks = queries.reshape(blocks, TOK_DEV, SB_HEADS, HEAD_DIM).astype(jnp.float32)
    k_blocks = key_rows.reshape(blocks, TOK_DEV, SB_HEADS, HEAD_DIM).astype(jnp.float32)
    v_blocks = values.reshape(blocks, TOK_DEV, SB_HEADS, HEAD_DIM).astype(jnp.float32)
    offsets = jnp.arange(TOK_DEV, dtype=jnp.int32)
    scaling = HEAD_DIM ** (-0.5)

    def one_query(block_args):
        q_blk, q_index = block_args
        q_pos = q_index * TOK_DEV + offsets

        def key_step(carried, inputs):
            result, logsum = carried
            k_blk, v_blk, k_index = inputs
            k_pos = k_index * TOK_DEV + offsets
            before = (k_pos[None, :] < q_pos[:, None])[None]
            scores = jnp.einsum('thd,shd->hts', q_blk, k_blk) * scaling + stick_bias[:, None, None]
            log_keep = jnp.where(before, jax.nn.log_sigmoid(-scores), 0.0)
            suffix = lax.cumsum(log_keep, axis=2, reverse=True) - log_keep
            stick_weights = jnp.where(before, jnp.exp(jax.nn.log_sigmoid(scores) + suffix + logsum[:, :, None]), 0.0)
            stick_weights = rounded(stick_weights)
            result = result + jnp.einsum('hts,shd->htd', stick_weights, v_blk)
            logsum = logsum + lax.optimization_barrier(jnp.sum(log_keep, axis=2))
            return ((result, logsum), None)
        initial = (jnp.zeros((SB_HEADS, TOK_DEV, HEAD_DIM), jnp.float32), jnp.zeros((SB_HEADS, TOK_DEV), jnp.float32))
        (result, _), _ = lax.scan(key_step, initial, (k_blocks, v_blocks, jnp.arange(blocks, dtype=jnp.int32)), reverse=True)
        return result.transpose(1, 0, 2)
    outputs = lax.map(one_query, (q_blocks, jnp.arange(blocks, dtype=jnp.int32)))
    return outputs.reshape(TOKENS, SB_WIDTH).astype(jnp.bfloat16)

def window_attention(queries, key_rows, values, sinks):
    block_count = TOKENS // WINDOW
    q_blocks = queries.reshape(block_count, WINDOW, SW_KV_HEADS, GROUP, HEAD_DIM).astype(jnp.float32)
    k_heads = key_rows.reshape(block_count, WINDOW, SW_KV_HEADS, HEAD_DIM).astype(jnp.float32)
    v_heads = values.reshape(block_count, WINDOW, SW_KV_HEADS, HEAD_DIM).astype(jnp.float32)
    zero_block = jnp.zeros((1, WINDOW, SW_KV_HEADS, HEAD_DIM), jnp.float32)
    k_band = jnp.concatenate([jnp.concatenate([zero_block, k_heads[:-1]], axis=0), k_heads], axis=1)
    v_band = jnp.concatenate([jnp.concatenate([zero_block, v_heads[:-1]], axis=0), v_heads], axis=1)
    logits = jnp.einsum('nqhgd,nchd->nhgqc', q_blocks, k_band) * HEAD_DIM ** (-0.5)
    query_offs = jnp.arange(WINDOW, dtype=jnp.int32)[:, None]
    key_offs = jnp.arange(2 * WINDOW, dtype=jnp.int32)[None, :]
    distance = query_offs + WINDOW - key_offs
    key_pos = jnp.arange(block_count, dtype=jnp.int32)[:, None] * WINDOW - WINDOW + key_offs
    usable = ((distance >= 0) & (distance < WINDOW))[None] & (key_pos >= 0)[:, None, :]
    logits = jnp.where(usable[:, None, None], logits, -jnp.inf)
    sink_logit = sinks.reshape(SW_KV_HEADS, GROUP)[None, :, :, None, None]
    row_top = jnp.maximum(lax.optimization_barrier(jnp.max(logits, axis=-1, keepdims=True)), sink_logit)
    weights_exp = jnp.exp(logits - row_top)
    normalizer = lax.optimization_barrier(jnp.sum(weights_exp, axis=-1, keepdims=True)) + jnp.exp(sink_logit - row_top)
    window_weights = rounded(weights_exp / normalizer)
    result = jnp.einsum('nhgqc,nchd->nqhgd', window_weights, v_band)
    return result.reshape(TOKENS, SW_WIDTH).astype(jnp.bfloat16)

def reference(tokens, pre_gain, w_query_stick, w_key_stick, w_value_stick, w_query_window, w_key_window, w_value_window, stick_bias, sinks, stick_gain, window_gain, w_out_stick, w_out_window, post_gain):
    normed = norm_rows(tokens.astype(jnp.float32), pre_gain).astype(jnp.bfloat16)

    def project(weight):
        return jnp.dot(normed, weight, preferred_element_type=jnp.float32).astype(jnp.bfloat16)
    stick_out = stick_attention(project(w_query_stick), project(w_key_stick), project(w_value_stick), stick_bias)
    window_out = window_attention(project(w_query_window), project(w_key_window), project(w_value_window), sinks)
    stick_normed = norm_rows(stick_out.astype(jnp.float32), stick_gain).astype(jnp.bfloat16)
    window_normed = norm_rows(window_out.astype(jnp.float32), window_gain).astype(jnp.bfloat16)
    combined = jnp.dot(stick_normed, w_out_stick, preferred_element_type=jnp.float32)
    combined = combined + jnp.dot(window_normed, w_out_window, preferred_element_type=jnp.float32)
    combined = rounded(combined)
    return norm_rows(combined, post_gain).astype(jnp.bfloat16)
```

```python
import functools

import jax
import jax.numpy as jnp
from jax import lax
from jax.experimental import pallas as pl
from jax.experimental.pallas import tpu as pltpu
from jax.sharding import PartitionSpec as P

HEAD_DIM = 64
WINDOW = 128
EPS = 1e-06
LOG2E = 1.4426950408889634
MESH = pl.DeviceIdType.MESH
NY = 8
NZ = 8
NT = 8
NX = 4
N_SP = NY * NZ


def dot(a, b):
    return jnp.dot(a, b, preferred_element_type=jnp.float32)


def dot_t(a, b):
    return lax.dot_general(a, b, (((1,), (1,)), ((), ())), preferred_element_type=jnp.float32)


def kernel(
    tokens, pre_gain_in, wqs, wks, wvs, wqw, wkw, wvw, bias_in, sinks_in, sgain_in, wgain_in, wos, wow,
    post_gain_in, out,
    pre_gain, bias, sinks, sgain, wgain, post_gain, x, sq_acc, normed, vqs, vkv, vqw, vkw, vvw, vos, vow,
    kv_all, q_all, o_seg, t_seg, kvw, kvw_prev, o_send, o_recv, t_send, t_recv,
    a_send, a_recv, b_send, b_recv, total,
    w_sem, tok_sem, x_ss, x_rs, kv_ss, kv_rs, q_ss, q_rs, p_ss, p_rs, o_ss, o_rs, t_ss, t_rs,
    a_ss, a_rs, b_ss, b_rs,
):
    bf = jnp.bfloat16
    f32 = jnp.float32
    s = lax.axis_index("sp")
    t = lax.axis_index("tp")
    z = s // NY
    y = lax.rem(s, NY)
    chip = t // 2
    core = lax.rem(t, 2)
    partner = chip * 2 + 1 - core
    rows, chunk = tokens.shape
    feats = NT * chunk
    hd = HEAD_DIM
    cut = rows // NT

    barrier = pltpu.get_barrier_semaphore()

    def greet(sp, tp):
        pl.semaphore_signal(barrier, inc=1, device_id={"sp": sp, "tp": tp}, device_id_type=MESH)

    for k in range(1, NZ):
        greet(lax.rem(z + k, NZ) * NY + y, t)
    for k in range(1, NY):
        greet(z * NY + lax.rem(y + k, NY), t)
    for k in range(1, NT):
        greet(s, lax.rem(t + k, NT))
    greet(lax.rem(s + 1, N_SP), t)
    greet(lax.rem(s + N_SP - 1, N_SP), t)

    half = rows // 2
    loads = [
        pltpu.make_async_copy(src, dst, w_sem.at[n])
        for n, (src, dst) in enumerate(
            [(wks, vkv.at[:, :rows]), (wvs, vkv.at[:, rows:]), (wqs, vqs), (wkw, vkw), (wvw, vvw), (wqw, vqw),
             (wow, vow), (wos.at[:half], vos.at[half:]), (wos.at[half:], vos.at[:half]),
             (bias_in, bias), (pre_gain_in, pre_gain), (sinks_in, sinks), (sgain_in, sgain),
             (wgain_in, wgain), (post_gain_in, post_gain)]
        )
    ]
    l_ks, l_vs, l_qs, l_kw, l_vw, l_qw, l_ow, l_os, l_os2, *l_small = loads
    tok_load = pltpu.make_async_copy(tokens, x.at[t], tok_sem)
    tok_load.start()
    for load in l_small + loads[:9]:
        load.start()

    for j in range(1, NZ):
        @pl.when(z + j >= NZ)
        def _():
            q_all[j] = jnp.zeros((rows, rows), bf)

        @pl.when(z - j < 0)
        def _():
            o_recv[j] = jnp.zeros((rows, rows), bf)
            t_recv[j] = jnp.zeros((8, rows), f32)

    for load in l_small:
        load.wait()
    tok_load.wait()
    pl.semaphore_wait(barrier, NZ + NY + NT - 3 + 2)

    def remote(src, dst, ss, rs, sp, tp):
        return pltpu.make_async_remote_copy(
            src_ref=src, dst_ref=dst, send_sem=ss, recv_sem=rs,
            device_id={"sp": sp, "tp": tp}, device_id_type=MESH,
        )

    sends = []

    def x_copy(slot, sem, tp):
        return remote(x.at[slot], x.at[slot], x_ss.at[sem], x_rs.at[slot], s, tp)

    def start(copy):
        copy.start()
        sends.append(copy)

    for dx in (2, 1, 3):
        start(x_copy(t, dx, lax.rem(chip + dx, NX) * 2 + core))
    start(x_copy(t, 0, partner))

    def squares(slot):
        v = x[slot].astype(f32)
        v = v * v
        return v[:, : chunk // 2] + v[:, chunk // 2 :]

    sq_acc[...] = squares(t)
    for dx in (1, 3, 2):
        slot = lax.rem(chip + NX - dx, NX) * 2 + core
        x_copy(slot, dx, partner).wait_recv()
        start(x_copy(slot, NX + dx, partner))
        sq_acc[...] += squares(slot)
    for dx in (0, 1, 3, 2):
        slot = lax.rem(chip + NX - dx, NX) * 2 + 1 - core
        x_copy(slot, dx, partner).wait_recv()
        sq_acc[...] += squares(slot)
    inv = lax.rsqrt(jnp.sum(sq_acc[...], axis=1, keepdims=True) * (1.0 / feats) + EPS)
    for k in range(NT):
        cols = slice(k * chunk, (k + 1) * chunk)
        normed[:, cols] = (x[k].astype(f32) * inv * pre_gain[cols].reshape(1, chunk)).astype(bf)

    lane = lax.broadcasted_iota(jnp.int32, (rows, rows), 1)
    left = lane < hd

    l_ks.wait()
    l_vs.wait()
    kv = dot(normed[...], vkv[...])
    keys = kv[:, :rows]
    values = pltpu.roll(kv[:, rows:], hd, 1)
    kv_all[y, 0] = jnp.where(left, keys, values).astype(bf)
    kv_all[y, 1] = jnp.where(left, values, keys).astype(bf)

    def kv_copy(slot, sem, to_y):
        return remote(kv_all.at[slot], kv_all.at[slot], kv_ss.at[sem], kv_rs.at[slot], z * NY + to_y, t)

    for k in (1, 7, 2, 6, 3, 5, 4):
        start(kv_copy(y, k, lax.rem(y + k, NY)))

    l_qs.wait()
    q_all[0] = dot(normed[...], vqs[...]).astype(bf)

    def q_copy(j, to_z):
        return remote(q_all.at[0], q_all.at[j], q_ss.at[j], q_rs.at[j], to_z * NY + y, t)

    for j in range(1, NZ):
        @pl.when(z - j >= 0)
        def _():
            q_copy(j, z - j).start()

    l_kw.wait()
    kvw[:, :hd] = dot(normed[...], vkw[...]).astype(bf)
    l_vw.wait()
    kvw[:, hd:] = dot(normed[...], vvw[...]).astype(bf)

    def prev_copy(to):
        return remote(kvw, kvw_prev, p_ss, p_rs, to, t)

    @pl.when(s < N_SP - 1)
    def _():
        prev_copy(s + 1).start()

    @pl.when(s == 0)
    def _():
        kvw_prev[...] = jnp.zeros_like(kvw_prev)

    l_qw.wait()
    qw = dot(normed[...], vqw[...])

    @pl.when(s > 0)
    def _():
        prev_copy(s - 1).wait_recv()

    two = 2 * rows
    r_iota = lax.broadcasted_iota(jnp.int32, (two, two), 0)
    c_iota = lax.broadcasted_iota(jnp.int32, (two, two), 1)
    dist = lax.rem(r_iota, rows) + rows - c_iota
    in_window = (dist >= 0) & (dist < WINDOW) & ((c_iota >= rows) | (s > 0))
    first_rows = lax.broadcasted_iota(jnp.int32, (two, 1), 0) < rows
    kk = jnp.concatenate([kvw_prev[...], kvw[...]], axis=0)
    qq = jnp.concatenate([jnp.where(left, qw, 0.0), jnp.where(left, pltpu.roll(qw, hd, 1), 0.0)], axis=0).astype(bf)
    logits = jnp.where(in_window, dot_t(qq, kk) * hd**-0.5, -jnp.inf)
    sink = jnp.where(first_rows, sinks[0], sinks[1])
    top = jnp.maximum(jnp.max(logits, axis=1, keepdims=True), sink)
    grown = jnp.exp(logits - top)
    norm = jnp.sum(grown, axis=1, keepdims=True) + jnp.exp(sink - top)
    res = dot((grown / norm).astype(bf), kk)
    w_out = jnp.where(left, pltpu.roll(res[:rows], hd, 1), res[rows:]).astype(bf).astype(f32)

    def give(send, recv, ss, rs, values, weights):
        sums = jnp.sum(values * values, axis=1, keepdims=True)
        high = sums.astype(bf)
        low = (sums - high.astype(f32)).astype(bf)
        send[:, :, feats:] = jnp.where(left, high.astype(f32), low.astype(f32)).astype(bf).reshape(NT, cut, rows)
        gained, w = weights
        n_cut = 4
        part = feats // n_cut
        for n in range(n_cut):
            cols = slice(n * part, (n + 1) * part)
            send[:, :, cols] = dot(gained, w[:, cols]).astype(bf).reshape(NT, cut, part)
        for dx, dc in ((2, 0), (2, 1), (1, 0), (1, 1), (3, 0), (3, 1), (0, 1)):
            to = lax.rem(chip + dx, NX) * 2 + lax.rem(core + dc, 2)
            start(remote(send.at[to], recv.at[t], ss.at[2 * dx + dc], rs.at[t], s, to))

    def take(send, recv, ss, rs, acc, width):
        own = send[t].astype(f32)
        acc[...] = own[:, :feats]
        sums = own[:, feats:]
        for dx, dc in ((0, 1), (1, 0), (1, 1), (3, 0), (3, 1), (2, 0), (2, 1)):
            frm = lax.rem(chip + dx, NX) * 2 + lax.rem(core + dc, 2)
            remote(send.at[frm], recv.at[frm], ss.at[2 * dx + dc], rs.at[frm], s, partner).wait_recv()
            got = recv[frm].astype(f32)
            acc[...] += got[:, :feats]
            sums += got[:, feats:]
        return lax.rsqrt((sums[:, :1] + sums[:, hd : hd + 1]) * (1.0 / width) + EPS)

    l_ow.wait()
    give(b_send, b_recv, b_ss, b_rs, w_out, ((w_out * wgain[...].reshape(1, rows)).astype(bf), vow))

    for j in range(1, NZ):
        @pl.when(z + j < NZ)
        def _():
            remote(
                q_all.at[0], q_all.at[j], q_ss.at[j], q_rs.at[j], lax.rem(z + j, NZ) * NY + y, t
            ).wait_recv()

    kt = 2 * rows
    mb = 2 * rows
    n_mb = NZ // 2
    later = (
        lax.broadcasted_iota(jnp.int32, (kt, kt), 0) > lax.broadcasted_iota(jnp.int32, (kt, kt), 1)
    ).astype(bf)
    row2 = lax.broadcasted_iota(jnp.int32, (mb, kt), 0)
    lane2 = lax.broadcasted_iota(jnp.int32, (mb, kt), 1)
    left2 = lax.broadcasted_iota(jnp.int32, (mb, rows), 1) < hd
    scale = LOG2E * hd**-0.5
    biases = (bias[0] * LOG2E, bias[1] * LOG2E)

    def step(i, carry):
        tile = lax.rem(y // 2 + i + i // 2 - 2 * (i // 3), NY // 2)
        for u in range(2):
            src = 2 * tile + u

            @pl.when(src != y)
            def _():
                kv_copy(src, 0, lax.rem(y + 1, NY)).wait_recv()

        pair = [kv_all[pl.ds(2 * tile, 2), h].reshape(kt, rows) for h in range(2)]
        for m in range(n_mb):
            part = slice(m * mb, (m + 1) * mb)
            queries = q_all[2 * m : 2 * m + 2].reshape(mb, rows).astype(f32)
            outs = []
            sums = []
            for h in range(2):
                qh = jnp.where(left2 if h == 0 else jnp.logical_not(left2), queries, 0.0).astype(bf)
                score = dot_t(qh, pair[h]) * scale + biases[h]
                pos = jnp.maximum(score, 0.0)
                neg = score - pos
                soft = jnp.log2(1.0 + jnp.exp2(neg - pos))
                drop = pos + soft
                hold = neg - soft
                if m == 0:
                    usable = (row2 >= rows) | (lane2 + tile * kt < row2 + y * rows)
                    drop = jnp.where(usable, drop, 0.0)
                    hold = jnp.where(usable, hold, -jnp.inf)
                suffix = dot(drop.astype(bf), later)
                weights = jnp.exp2(hold - suffix).astype(bf)
                outs.append(dot(weights, pair[h]))
                sums.append(suffix[:, :1] + drop[:, :1])
            o_seg[tile, part] = jnp.where(left2, outs[1], outs[0])
            t_seg[tile, part] = jnp.where(left2, sums[1], sums[0])
        return carry

    lax.fori_loop(0, NY // 2, step, 0)

    first = lax.broadcasted_iota(jnp.int32, (8, rows), 0) < 4
    own_t = None
    for j in range(NZ - 1, -1, -1):
        part = slice(j * rows, (j + 1) * rows)
        last = NY // 2 - 1
        acc = o_seg[last, part]
        carry = t_seg[last, part]
        for n in range(last - 1, -1, -1):
            acc = acc + jnp.exp2(-carry) * o_seg[n, part]
            carry = carry + t_seg[n, part]
        turned = carry.T
        compact = jnp.where(first, turned[0:8], turned[hd : hd + 8])
        if j == 0:
            own_t = compact
            own_o = acc
        else:
            o_send[j] = acc.astype(bf)
            t_send[j] = compact

            @pl.when(z + j < NZ)
            def _():
                to = (z + j) * NY + y
                remote(t_send.at[j], t_recv.at[j], t_ss.at[j], t_rs.at[j], to, t).start()
                remote(o_send.at[j], o_recv.at[j], o_ss.at[j], o_rs.at[j], to, t).start()

    for j in range(1, NZ):
        @pl.when(z - j >= 0)
        def _():
            frm = lax.rem(z + NZ - j, NZ) * NY + y
            remote(t_send.at[j], t_recv.at[j], t_ss.at[j], t_rs.at[j], frm, t).wait_recv()

    carry = own_t
    scales = []
    for j in range(1, NZ):
        scales.append(jnp.exp2(-carry))
        carry = carry + t_recv[j]
    scales = jnp.concatenate(scales + [jnp.zeros((rows - 8 * (NZ - 1), rows), f32)], axis=0).T
    acc = own_o
    for j in range(1, NZ):
        @pl.when(z - j >= 0)
        def _():
            frm = lax.rem(z + NZ - j, NZ) * NY + y
            remote(o_send.at[j], o_recv.at[j], o_ss.at[j], o_rs.at[j], frm, t).wait_recv()

    for j in range(1, NZ):
        at = 8 * (j - 1)
        acc = acc + jnp.where(left, scales[:, at : at + 1], scales[:, at + 4 : at + 5]) * o_recv[j].astype(f32)
    s_out = acc.astype(bf).astype(f32)
    gain = sgain[...].reshape(1, rows)
    gain = jnp.concatenate([gain[:, hd:], gain[:, :hd]], axis=1)
    l_os.wait()
    l_os2.wait()
    give(a_send, a_recv, a_ss, a_rs, s_out, ((s_out * gain).astype(bf), vos))

    inv_w = take(b_send, b_recv, b_ss, b_rs, total.at[1], NT * rows)
    total[1] = total[1] * inv_w
    inv_s = take(a_send, a_recv, a_ss, a_rs, total.at[0], NT * rows)
    both = (total[0] * inv_s + total[1]).astype(bf).astype(f32)
    stats = jnp.sum(both * both, axis=1, keepdims=True) * (1.0 / feats)
    out[...] = (both * lax.rsqrt(stats + EPS) * post_gain[...].reshape(1, feats)).astype(bf)

    for copy in sends:
        copy.wait_send()
    for j in range(1, NZ):
        @pl.when(z - j >= 0)
        def _():
            q_copy(j, z - j).wait_send()

        @pl.when(z + j < NZ)
        def _():
            to = (z + j) * NY + y
            remote(t_send.at[j], t_recv.at[j], t_ss.at[j], t_rs.at[j], to, t).wait_send()
            remote(o_send.at[j], o_recv.at[j], o_ss.at[j], o_rs.at[j], to, t).wait_send()

    @pl.when(s < N_SP - 1)
    def _():
        prev_copy(s + 1).wait_send()


def one_kernel(*args):
    tokens, pre_gain, wqs, wks, wvs, wqw, wkw, wvw, bias, sinks, sgain, wgain, wos, wow, post_gain = args
    bf = jnp.bfloat16
    f32 = jnp.float32
    rows, chunk = tokens.shape
    feats = NT * chunk
    cut = rows // NT
    v = pltpu.VMEM
    dma = pltpu.SemaphoreType.DMA
    anywhere = pl.BlockSpec(memory_space=pl.ANY)
    vmem = pl.BlockSpec(memory_space=pltpu.VMEM)
    scratch = [
        v(pre_gain.shape, f32), pltpu.SMEM(bias.shape, f32), pltpu.SMEM(sinks.shape, f32),
        v(sgain.shape, f32), v(wgain.shape, f32), v(post_gain.shape, f32),
        v((NT, rows, chunk), bf), v((rows, rows), f32), v((rows, feats), bf),
        v(wqs.shape, bf), v((feats, 2 * rows), bf), v(wqw.shape, bf), v(wkw.shape, bf), v(wvw.shape, bf),
        v(wos.shape, bf), v(wow.shape, bf),
        v((NY, 2, rows, rows), bf), v((NZ, rows, rows), bf),
        v((NY // 2, NZ * rows, rows), f32), v((NY // 2, NZ * rows, rows), f32),
        v((rows, rows), bf), v((rows, rows), bf),
        v((NZ, rows, rows), bf), v((NZ, rows, rows), bf), v((NZ, 8, rows), f32), v((NZ, 8, rows), f32),
        v((NT, cut, feats + rows), bf), v((NT, cut, feats + rows), bf),
        v((NT, cut, feats + rows), bf), v((NT, cut, feats + rows), bf), v((2, cut, feats), f32),
        dma((15,)), dma, dma((8,)), dma((NT,)), dma((NY,)), dma((NY,)), dma((NZ,)), dma((NZ,)), dma, dma,
        dma((NZ,)), dma((NZ,)), dma((NZ,)), dma((NZ,)), dma((NT,)), dma((NT,)), dma((NT,)), dma((NT,)),
    ]
    return pl.pallas_call(
        kernel,
        out_shape=jax.ShapeDtypeStruct((cut, feats), bf),
        in_specs=[anywhere] * len(args),
        out_specs=vmem,
        scratch_shapes=scratch,
        compiler_params=pltpu.CompilerParams(
            collective_id=0, has_side_effects=True, vmem_limit_bytes=67043328
        ),
        name="layer",
    )(*args)


def solution(mesh):
    in_specs = (
        P("sp", "tp"),
        P(),
        P(None, "tp"),
        P(None, "tp"),
        P(None, "tp"),
        P(None, "tp"),
        P(None, "tp"),
        P(None, "tp"),
        P("tp"),
        P("tp"),
        P("tp"),
        P("tp"),
        P("tp", None),
        P("tp", None),
        P(),
    )
    return jax.shard_map(
        one_kernel,
        mesh=mesh,
        in_specs=in_specs,
        out_specs=P(("sp", "tp"), None),
        check_vma=False,
    )
```

```python
import functools

import jax
import jax.numpy as jnp
from jax import lax
from jax.experimental import pallas as pl
from jax.experimental.pallas import tpu as pltpu
from jax.sharding import PartitionSpec as P

HEAD_DIM = 64
WINDOW = 128
EPS = 1e-06
LOG2E = 1.4426950408889634
MESH = pl.DeviceIdType.MESH
NY = 8
NZ = 8
NT = 8
NX = 4
N_SP = NY * NZ


def dot(a, b):
    return jnp.dot(a, b, preferred_element_type=jnp.float32)


def dot_t(a, b):
    return lax.dot_general(a, b, (((1,), (1,)), ((), ())), preferred_element_type=jnp.float32)


def kernel(
    tokens, pre_gain_in, wqs, wks, wvs, wqw, wkw, wvw, bias_in, sinks_in, sgain_in, wgain_in, wos, wow,
    post_gain_in, out,
    pre_gain, bias, sinks, sgain, wgain, post_gain, x, sq_acc, normed, vqs, vkv, vqw, vkvw, vos, vow,
    kv_all, kv_other, q_all, q_other, o_seg, t_seg, kvw, qw_buf, kvw_prev, o_send, o_recv, t_send, t_recv,
    a_send, a_recv, b_send, b_recv, total,
    w_sem, tok_sem, x_ss, x_rs, kv_ss, kv_rs, q_ss, q_rs, p_ss, p_rs, o_ss, o_rs, t_ss, t_rs,
    a_ss, a_rs, b_ss, b_rs,
):
    bf = jnp.bfloat16
    f32 = jnp.float32
    s = lax.axis_index("sp")
    t = lax.axis_index("tp")
    z = s // NY
    y = lax.rem(s, NY)
    chip = t // 2
    core = lax.rem(t, 2)
    head = lax.rem(y, 2)
    y_other = y + 1 - 2 * head
    partner = chip * 2 + 1 - core
    rows, chunk = tokens.shape
    feats = NT * chunk
    hd = HEAD_DIM
    cut = rows // NT

    barrier = pltpu.get_barrier_semaphore()

    def greet(sp, tp):
        pl.semaphore_signal(barrier, inc=1, device_id={"sp": sp, "tp": tp}, device_id_type=MESH)

    for k in range(1, NZ):
        greet(lax.rem(z + k, NZ) * NY + y, t)
        greet(lax.rem(z + k, NZ) * NY + y_other, t)
    for k in range(1, NY):
        greet(z * NY + lax.rem(y + k, NY), t)
    for k in range(1, NT):
        greet(s, lax.rem(t + k, NT))
    greet(lax.rem(s + 1, N_SP), t)
    greet(lax.rem(s + N_SP - 1, N_SP), t)

    half = rows // 2
    loads = [
        pltpu.make_async_copy(src, dst, w_sem.at[n])
        for n, (src, dst) in enumerate(
            [(wks, vkv.at[:, :rows]), (wvs, vkv.at[:, rows:]), (wqs, vqs), (wkw, vkvw.at[:half]), (wvw, vkvw.at[half:]), (wqw, vqw),
             (wow, vow), (wos, vos),
             (bias_in, bias), (pre_gain_in, pre_gain), (sinks_in, sinks), (sgain_in, sgain),
             (wgain_in, wgain), (post_gain_in, post_gain)]
        )
    ]
    l_ks, l_vs, l_qs, l_kw, l_vw, l_qw, l_ow, l_os, *l_small = loads
    tok_load = pltpu.make_async_copy(tokens, x.at[t], tok_sem)
    tok_load.start()
    for load in l_small + loads[:8]:
        load.start()

    for j in range(1, NZ):
        @pl.when(z + j >= NZ)
        def _():
            q_all[j] = jnp.zeros((2, half, rows), bf)

        @pl.when(z - j < 0)
        def _():
            o_recv[j] = jnp.zeros((2, half, rows), bf)
            t_recv[j] = jnp.zeros((2, 8, rows), f32)

    for load in l_small:
        load.wait()
    tok_load.wait()
    pl.semaphore_wait(barrier, 2 * NZ + NY + NT - 4 + 2)

    def remote(src, dst, ss, rs, sp, tp):
        return pltpu.make_async_remote_copy(
            src_ref=src, dst_ref=dst, send_sem=ss, recv_sem=rs,
            device_id={"sp": sp, "tp": tp}, device_id_type=MESH,
        )

    sends = []

    def x_copy(slot, sem, tp):
        return remote(x.at[slot], x.at[slot], x_ss.at[sem], x_rs.at[slot], s, tp)

    def start(copy):
        copy.start()
        sends.append(copy)

    for dx in (2, 1, 3):
        start(x_copy(t, dx, lax.rem(chip + dx, NX) * 2 + core))
    start(x_copy(t, 0, partner))

    def squares(slot):
        v = x[slot].astype(f32)
        v = v * v
        return v[:, : chunk // 2] + v[:, chunk // 2 :]

    sq_acc[...] = squares(t)
    for dx in (1, 3, 2):
        slot = lax.rem(chip + NX - dx, NX) * 2 + core
        x_copy(slot, dx, partner).wait_recv()
        start(x_copy(slot, NX + dx, partner))
        sq_acc[...] += squares(slot)
    for dx in (0, 1, 3, 2):
        slot = lax.rem(chip + NX - dx, NX) * 2 + 1 - core
        x_copy(slot, dx, partner).wait_recv()
        sq_acc[...] += squares(slot)
    inv = lax.rsqrt(jnp.sum(sq_acc[...], axis=1, keepdims=True) * (1.0 / feats) + EPS)
    for k in range(NT):
        cols = slice(k * chunk, (k + 1) * chunk)
        normed[:, cols] = (x[k].astype(f32) * inv * pre_gain[cols].reshape(1, chunk)).astype(bf)

    left = lax.broadcasted_iota(jnp.int32, (rows, rows), 1) < hd
    left_half = left[:half]

    l_ks.wait()
    l_vs.wait()
    kv = dot(normed[...], vkv[...])
    keys, values = kv[:, :rows], kv[:, rows:]
    head0 = jnp.where(left, keys, pltpu.roll(values, hd, 1))
    head1 = jnp.where(left, pltpu.roll(keys, hd, 1), values)
    kv_all[y] = jnp.where(head == 0, head0, head1).astype(bf)
    kv_other[...] = jnp.where(head == 0, head1, head0).astype(bf)

    def kv_copy(src, slot, sem, to_y):
        return remote(src, kv_all.at[slot], kv_ss.at[sem], kv_rs.at[slot], z * NY + to_y, t)

    def kv_send(k):
        start(kv_copy(kv_other if k % 2 else kv_all.at[y], y, k, lax.rem(y + k, NY)))

    for k in (1, 7, 2, 6):
        kv_send(k)

    l_qs.wait()
    qs = dot(normed[...], vqs[...])
    q0 = jnp.where(left_half, qs[:half], pltpu.roll(qs[half:], hd, 1))
    q1 = jnp.where(left_half, pltpu.roll(qs[:half], hd, 1), qs[half:])
    q_all[0, 0] = jnp.where(head == 0, q0, q1).astype(bf)
    q_other[...] = jnp.where(head == 0, q1, q0).astype(bf)

    def q_copy(j, e, to_z):
        src = q_other if e else q_all.at[0, 0]
        return remote(
            src, q_all.at[j, e], q_ss.at[j, e], q_rs.at[j, e], to_z * NY + (y_other if e else y), t
        )

    start(q_copy(0, 1, z))
    for j in range(1, NZ):
        @pl.when(z - j >= 0)
        def _():
            q_copy(j, 0, z - j).start()
            q_copy(j, 1, z - j).start()

    l_kw.wait()
    l_vw.wait()
    kvw[...] = dot_t(normed[...], vkvw[...]).astype(bf)

    def prev_copy(to):
        return remote(kvw, kvw_prev, p_ss, p_rs, to, t)

    @pl.when(s < N_SP - 1)
    def _():
        prev_copy(s + 1).start()

    for k in (3, 5, 4):
        kv_send(k)

    @pl.when(s == 0)
    def _():
        kvw_prev[...] = jnp.zeros_like(kvw_prev)

    l_qw.wait()
    qw_buf[...] = dot(normed[...], vqw[...])

    def given(send, recv, ss, rs):
        for dx, dc in ((2, 0), (2, 1), (1, 0), (1, 1), (3, 0), (3, 1), (0, 1)):
            to = lax.rem(chip + dx, NX) * 2 + lax.rem(core + dc, 2)
            yield remote(send.at[to], recv.at[t], ss.at[2 * dx + dc], rs.at[t], s, to)

    def give(send, recv, ss, rs, values, weights):
        sums = jnp.sum(values * values, axis=1, keepdims=True)
        high = sums.astype(bf)
        low = (sums - high.astype(f32)).astype(bf)
        send[:, :, feats:] = jnp.where(left, high.astype(f32), low.astype(f32)).astype(bf).reshape(NT, cut, rows)
        gained, w = weights
        n_cut = 4
        part = feats // n_cut
        for n in range(n_cut):
            cols = slice(n * part, (n + 1) * part)
            send[:, :, cols] = dot(gained, w[:, cols]).astype(bf).reshape(NT, cut, part)
        for copy in given(send, recv, ss, rs):
            copy.start()

    def take(send, recv, ss, rs, acc, width):
        own = send[t].astype(f32)
        acc[...] = own[:, :feats]
        sums = own[:, feats:]
        for dx, dc in ((0, 1), (1, 0), (1, 1), (3, 0), (3, 1), (2, 0), (2, 1)):
            frm = lax.rem(chip + dx, NX) * 2 + lax.rem(core + dc, 2)
            remote(send.at[frm], recv.at[frm], ss.at[2 * dx + dc], rs.at[frm], s, partner).wait_recv()
            got = recv[frm].astype(f32)
            acc[...] += got[:, :feats]
            sums += got[:, feats:]
        return lax.rsqrt((sums[:, :1] + sums[:, hd : hd + 1]) * (1.0 / width) + EPS)

    def windowed():
        @pl.when(s > 0)
        def _():
            prev_copy(s - 1).wait_recv()

        two = 2 * rows
        r_iota = lax.broadcasted_iota(jnp.int32, (two, two), 0)
        c_iota = lax.broadcasted_iota(jnp.int32, (two, two), 1)
        dist = lax.rem(r_iota, rows) + rows - c_iota
        in_window = (dist >= 0) & (dist < WINDOW) & ((c_iota >= rows) | (s > 0))
        first_rows = lax.broadcasted_iota(jnp.int32, (two, 1), 0) < rows
        qw = qw_buf[...]
        kk = jnp.concatenate([kvw_prev[...], kvw[...]], axis=0)
        qq = jnp.concatenate([jnp.where(left, qw, 0.0), jnp.where(left, pltpu.roll(qw, hd, 1), 0.0)], axis=0).astype(bf)
        logits = jnp.where(in_window, dot_t(qq, kk) * hd**-0.5, -jnp.inf)
        sink = jnp.where(first_rows, sinks[0], sinks[1])
        top = jnp.maximum(jnp.max(logits, axis=1, keepdims=True), sink)
        grown = jnp.exp(logits - top)
        norm = jnp.sum(grown, axis=1, keepdims=True) + jnp.exp(sink - top)
        res = dot((grown / norm).astype(bf), kk)
        w_out = jnp.where(left, pltpu.roll(res[:rows], hd, 1), res[rows:]).astype(bf).astype(f32)

        l_ow.wait()
        give(b_send, b_recv, b_ss, b_rs, w_out, ((w_out * wgain[...].reshape(1, rows)).astype(bf), vow))

    def q_wait(j, e):
        frm = lax.rem(z + j, NZ) * NY + (y_other if e else y)
        remote(q_other, q_all.at[j, e], q_ss.at[j, e], q_rs.at[j, e], frm, t).wait_recv()

    q_wait(0, 1)
    for j in range(1, NZ):
        @pl.when(z + j < NZ)
        def _():
            q_wait(j, 0)
            q_wait(j, 1)

    kt = 2 * rows
    mb = 2 * rows
    n_mb = NZ * rows // mb
    later = (
        lax.broadcasted_iota(jnp.int32, (kt, kt), 0) > lax.broadcasted_iota(jnp.int32, (kt, kt), 1)
    ).astype(bf)
    row2 = lax.broadcasted_iota(jnp.int32, (mb, kt), 0)
    lane2 = lax.broadcasted_iota(jnp.int32, (mb, kt), 1)
    place = lax.rem(row2, half) + jnp.where(row2 < half, y, y_other) * rows
    left2 = lax.broadcasted_iota(jnp.int32, (mb, rows), 1) < hd
    scale = LOG2E * hd**-0.5
    head_bias = bias[head] * LOG2E

    def step(i, carry):
        @pl.when(i == 1)
        def _():
            windowed()

        tile = lax.rem(y // 2 + i + i // 2 - 2 * (i // 3), NY // 2)
        for u in range(2):
            src = 2 * tile + u

            @pl.when(src != y)
            def _():
                kv_copy(kv_other, src, 0, lax.rem(y + 1, NY)).wait_recv()

        straight = kv_all[pl.ds(2 * tile, 2)].reshape(kt, rows)
        turned = pltpu.roll(straight.astype(f32), hd, 1).astype(bf)
        for m in range(n_mb):
            part = slice(m * mb, (m + 1) * mb)
            per = mb // rows
            queries = q_all[m * per : (m + 1) * per].reshape(mb, rows).astype(f32)
            outs = []
            sums = []
            for u in range(2):
                qh = jnp.where(jnp.logical_not(left2) if u else left2, queries, 0.0).astype(bf)
                score = dot_t(qh, turned if u else straight) * scale + head_bias
                pos = jnp.maximum(score, 0.0)
                neg = score - pos
                soft = jnp.log2(1.0 + jnp.exp2(neg - pos))
                drop = pos + soft
                hold = neg - soft
                if m == 0:
                    usable = (row2 >= rows) | (lane2 + tile * kt < place + u * half)
                    drop = jnp.where(usable, drop, 0.0)
                    hold = jnp.where(usable, hold, -jnp.inf)
                suffix = dot(drop.astype(bf), later)
                weights = jnp.exp2(hold - suffix).astype(bf)
                outs.append(dot(weights, straight if u else turned))
                sums.append(suffix[:, :1] + drop[:, :1])
            o_seg[tile, part] = jnp.where(left2, outs[0], outs[1])
            t_seg[tile, part] = jnp.where(left2, sums[0], sums[1])
        return carry

    lax.fori_loop(0, NY // 2, step, 0)

    def to_owner(j, e, sp, which):
        if which:
            return remote(o_send.at[j, e], o_recv.at[j, e], o_ss.at[j, e], o_rs.at[j, e], sp, t)
        return remote(t_send.at[j], t_recv.at[j, e], t_ss.at[j, e], t_rs.at[j, e], sp, t)

    first = lax.broadcasted_iota(jnp.int32, (8, rows), 0) < 4
    for j in range(NZ - 1, -1, -1):
        part = slice(j * rows, (j + 1) * rows)
        last = NY // 2 - 1
        acc = o_seg[last, part]
        carry = t_seg[last, part]
        for n in range(last - 1, -1, -1):
            acc = acc + jnp.exp2(-carry) * o_seg[n, part]
            carry = carry + t_seg[n, part]
        over = carry.T
        compact = jnp.where(first, over[0:8], over[hd : hd + 8])
        o_send[j] = acc.astype(bf).reshape(2, half, rows)
        t_send[j] = compact
        if j == 0:
            own_t = compact
            own_o = acc[:half]
            for which in range(2):
                start(to_owner(0, 1, z * NY + y_other, which))
        else:
            @pl.when(z + j < NZ)
            def _():
                for e in range(2):
                    for which in range(2):
                        to_owner(j, e, (z + j) * NY + (y_other if e else y), which).start()

    def from_owner(j, e, which):
        frm = lax.rem(z + NZ - j, NZ) * NY + (y_other if e else y)
        to_owner(j, e, frm, which).wait_recv()

    def arrivals(which):
        from_owner(0, 1, which)
        for j in range(1, NZ):
            @pl.when(z - j >= 0)
            def _():
                from_owner(j, 0, which)
                from_owner(j, 1, which)

    arrivals(0)
    left8 = left[:8]
    carry = jnp.where(left8, own_t, t_recv[0, 1])
    scales = []
    for j in range(1, NZ):
        scales.append(jnp.exp2(-carry))
        carry = carry + jnp.where(left8, t_recv[j, 0], t_recv[j, 1])
    scales = jnp.concatenate(scales + [jnp.zeros((rows - 8 * (NZ - 1), rows), f32)], axis=0).T
    arrivals(1)
    acc = jnp.concatenate([own_o, o_recv[0, 1].astype(f32)], axis=0)
    for j in range(1, NZ):
        at = 8 * (j - 1)
        here = o_recv[j].reshape(rows, rows).astype(f32)
        acc = acc + jnp.where(left, scales[:, at : at + 1], scales[:, at + 4 : at + 5]) * here
    head0 = jnp.where(head == 0, acc[:half], acc[half:])
    head1 = jnp.where(head == 0, acc[half:], acc[:half])
    s_out = jnp.concatenate(
        [
            jnp.where(left_half, head0, pltpu.roll(head1, hd, 1)),
            jnp.where(left_half, pltpu.roll(head0, hd, 1), head1),
        ],
        axis=0,
    ).astype(bf).astype(f32)
    l_os.wait()
    give(a_send, a_recv, a_ss, a_rs, s_out, ((s_out * sgain[...].reshape(1, rows)).astype(bf), vos))

    inv_w = take(b_send, b_recv, b_ss, b_rs, total.at[1], NT * rows)
    total[1] = total[1] * inv_w
    inv_s = take(a_send, a_recv, a_ss, a_rs, total.at[0], NT * rows)
    both = (total[0] * inv_s + total[1]).astype(bf).astype(f32)
    stats = jnp.sum(both * both, axis=1, keepdims=True) * (1.0 / feats)
    out[...] = (both * lax.rsqrt(stats + EPS) * post_gain[...].reshape(1, feats)).astype(bf)

    for refs in ((a_send, a_recv, a_ss, a_rs), (b_send, b_recv, b_ss, b_rs)):
        for copy in given(*refs):
            copy.wait_send()
    for copy in sends:
        copy.wait_send()
    for j in range(1, NZ):
        for e in range(2):
            @pl.when(z - j >= 0)
            def _():
                q_copy(j, e, z - j).wait_send()

            @pl.when(z + j < NZ)
            def _():
                for which in range(2):
                    to_owner(j, e, (z + j) * NY + (y_other if e else y), which).wait_send()

    @pl.when(s < N_SP - 1)
    def _():
        prev_copy(s + 1).wait_send()


def one_kernel(*args):
    tokens, pre_gain, wqs, wks, wvs, wqw, wkw, wvw, bias, sinks, sgain, wgain, wos, wow, post_gain = args
    bf = jnp.bfloat16
    f32 = jnp.float32
    rows, chunk = tokens.shape
    feats = NT * chunk
    cut = rows // NT
    v = pltpu.VMEM
    dma = pltpu.SemaphoreType.DMA
    anywhere = pl.BlockSpec(memory_space=pl.ANY)
    vmem = pl.BlockSpec(memory_space=pltpu.VMEM)
    scratch = [
        v(pre_gain.shape, f32), pltpu.SMEM(bias.shape, f32), pltpu.SMEM(sinks.shape, f32),
        v(sgain.shape, f32), v(wgain.shape, f32), v(post_gain.shape, f32),
        v((NT, rows, chunk), bf), v((rows, rows), f32), v((rows, feats), bf),
        v(wqs.shape, bf), v((feats, 2 * rows), bf), v(wqw.shape, bf), v((rows, feats), bf),
        v(wos.shape, bf), v(wow.shape, bf),
        v((NY, rows, rows), bf), v((rows, rows), bf), v((NZ, 2, rows // 2, rows), bf), v((rows // 2, rows), bf),
        v((NY // 2, NZ * rows, rows), f32), v((NY // 2, NZ * rows, rows), f32),
        v((rows, rows), bf), v((rows, rows), f32), v((rows, rows), bf),
        v((NZ, 2, rows // 2, rows), bf), v((NZ, 2, rows // 2, rows), bf),
        v((NZ, 8, rows), f32), v((NZ, 2, 8, rows), f32),
        v((NT, cut, feats + rows), bf), v((NT, cut, feats + rows), bf),
        v((NT, cut, feats + rows), bf), v((NT, cut, feats + rows), bf), v((2, cut, feats), f32),
        dma((14,)), dma, dma((8,)), dma((NT,)), dma((NY,)), dma((NY,)), dma((NZ, 2)), dma((NZ, 2)), dma, dma,
        dma((NZ, 2)), dma((NZ, 2)), dma((NZ, 2)), dma((NZ, 2)), dma((NT,)), dma((NT,)), dma((NT,)), dma((NT,)),
    ]
    return pl.pallas_call(
        kernel,
        out_shape=jax.ShapeDtypeStruct((cut, feats), bf),
        in_specs=[anywhere] * len(args),
        out_specs=vmem,
        scratch_shapes=scratch,
        compiler_params=pltpu.CompilerParams(
            collective_id=0, has_side_effects=True, vmem_limit_bytes=67043328
        ),
        name="layer",
    )(*args[:6], wkw.T, wvw.T, *args[8:])


def solution(mesh):
    in_specs = (
        P("sp", "tp"),
        P(),
        P(None, "tp"),
        P(None, "tp"),
        P(None, "tp"),
        P(None, "tp"),
        P(None, "tp"),
        P(None, "tp"),
        P("tp"),
        P("tp"),
        P("tp"),
        P("tp"),
        P("tp", None),
        P("tp", None),
        P(),
    )
    return jax.shard_map(
        one_kernel,
        mesh=mesh,
        in_specs=in_specs,
        out_specs=P(("sp", "tp"), None),
        check_vma=False,
    )
```

```python
import functools

import jax
import jax.numpy as jnp
from jax import lax
from jax.experimental import pallas as pl
from jax.experimental.pallas import tpu as pltpu
from jax.sharding import PartitionSpec as P

HEAD_DIM = 64
WINDOW = 128
EPS = 1e-06
LOG2E = 1.4426950408889634
MESH = pl.DeviceIdType.MESH
NY = 8
NZ = 8
NT = 8
NX = 4
N_SP = NY * NZ


def dot(a, b):
    return jnp.dot(a, b, preferred_element_type=jnp.float32)


def dot_t(a, b):
    return lax.dot_general(a, b, (((1,), (1,)), ((), ())), preferred_element_type=jnp.float32)


def kernel(
    tokens, pre_gain_in, wqs, wks, wvs, wqw, wkw, wvw, bias_in, sinks_in, sgain_in, wgain_in, wos, wow,
    post_gain_in, out,
    pre_gain, bias, sinks, sgain, wgain, post_gain, x, sq_acc, normed, vqs, vkv, vqw, vkvw, vos, vow,
    kv_all, kv_other, q_all, q_other, o_seg, t_seg, kvw, qw_buf, kvw_prev, o_send, o_recv, t_send, t_recv,
    a_send, a_recv, b_send, b_recv, total,
    w_sem, tok_sem, x_ss, x_rs, kv_ss, kv_rs, q_ss, q_rs, p_ss, p_rs, o_ss, o_rs, t_ss, t_rs,
    a_ss, a_rs, b_ss, b_rs,
):
    bf = jnp.bfloat16
    f32 = jnp.float32
    s = lax.axis_index("sp")
    t = lax.axis_index("tp")
    z = s // NY
    y = lax.rem(s, NY)
    chip = t // 2
    core = lax.rem(t, 2)
    head = lax.rem(y, 2)
    y_other = y + 1 - 2 * head
    partner = chip * 2 + 1 - core
    rows, chunk = tokens.shape
    feats = NT * chunk
    hd = HEAD_DIM
    cut = rows // NT

    barrier = pltpu.get_barrier_semaphore()

    def greet(sp, tp):
        pl.semaphore_signal(barrier, inc=1, device_id={"sp": sp, "tp": tp}, device_id_type=MESH)

    for k in range(1, NZ):
        greet(lax.rem(z + k, NZ) * NY + y, t)
        greet(lax.rem(z + k, NZ) * NY + y_other, t)
    for k in range(1, NY):
        greet(z * NY + lax.rem(y + k, NY), t)
    for k in range(1, NT):
        greet(s, lax.rem(t + k, NT))
    greet(lax.rem(s + 1, N_SP), t)
    greet(lax.rem(s + N_SP - 1, N_SP), t)

    half = rows // 2
    loads = [
        pltpu.make_async_copy(src, dst, w_sem.at[n])
        for n, (src, dst) in enumerate(
            [(wks, vkv.at[:, :rows]), (wvs, vkv.at[:, rows:]), (wqs, vqs), (wkw, vkvw.at[:half]), (wvw, vkvw.at[half:]), (wqw, vqw),
             (wow, vow), (wos, vos),
             (bias_in, bias), (pre_gain_in, pre_gain), (sinks_in, sinks), (sgain_in, sgain),
             (wgain_in, wgain), (post_gain_in, post_gain)]
        )
    ]
    l_ks, l_vs, l_qs, l_kw, l_vw, l_qw, l_ow, l_os, *l_small = loads
    tok_load = pltpu.make_async_copy(tokens, x.at[t], tok_sem)
    tok_load.start()
    for load in l_small + loads[:8]:
        load.start()

    for j in range(1, NZ):
        @pl.when(z + j >= NZ)
        def _():
            q_all[j] = jnp.zeros((2, half, rows), bf)

        @pl.when(z - j < 0)
        def _():
            o_recv[j] = jnp.zeros((2, half, rows), bf)
            t_recv[j] = jnp.zeros((2, 8, rows), f32)

    for load in l_small:
        load.wait()
    tok_load.wait()
    pl.semaphore_wait(barrier, 2 * NZ + NY + NT - 4 + 2)

    def remote(src, dst, ss, rs, sp, tp):
        return pltpu.make_async_remote_copy(
            src_ref=src, dst_ref=dst, send_sem=ss, recv_sem=rs,
            device_id={"sp": sp, "tp": tp}, device_id_type=MESH,
        )

    sends = []

    def x_copy(slot, sem, tp):
        return remote(x.at[slot], x.at[slot], x_ss.at[sem], x_rs.at[slot], s, tp)

    def start(copy):
        copy.start()
        sends.append(copy)

    for dx in (2, 1, 3):
        start(x_copy(t, dx, lax.rem(chip + dx, NX) * 2 + core))
    start(x_copy(t, 0, partner))

    def squares(slot):
        v = x[slot].astype(f32)
        v = v * v
        return v[:, : chunk // 2] + v[:, chunk // 2 :]

    sq_acc[...] = squares(t)
    for dx in (1, 3, 2):
        slot = lax.rem(chip + NX - dx, NX) * 2 + core
        x_copy(slot, dx, partner).wait_recv()
        start(x_copy(slot, NX + dx, partner))
        sq_acc[...] += squares(slot)
    for dx in (0, 1, 3, 2):
        slot = lax.rem(chip + NX - dx, NX) * 2 + 1 - core
        x_copy(slot, dx, partner).wait_recv()
        sq_acc[...] += squares(slot)
    inv = lax.rsqrt(jnp.sum(sq_acc[...], axis=1, keepdims=True) * (1.0 / feats) + EPS)
    for k in range(NT):
        cols = slice(k * chunk, (k + 1) * chunk)
        normed[:, cols] = (x[k].astype(f32) * inv * pre_gain[cols].reshape(1, chunk)).astype(bf)

    left = lax.broadcasted_iota(jnp.int32, (rows, rows), 1) < hd
    left_half = left[:half]

    l_ks.wait()
    l_vs.wait()
    kv = dot(normed[...], vkv[...])
    keys, values = kv[:, :rows], kv[:, rows:]
    head0 = jnp.where(left, keys, pltpu.roll(values, hd, 1))
    head1 = jnp.where(left, pltpu.roll(keys, hd, 1), values)
    kv_all[y] = jnp.where(head == 0, head0, head1).astype(bf)
    kv_other[...] = jnp.where(head == 0, head1, head0).astype(bf)

    def kv_copy(src, slot, sem, to_y):
        return remote(src, kv_all.at[slot], kv_ss.at[sem], kv_rs.at[slot], z * NY + to_y, t)

    def kv_send(k):
        start(kv_copy(kv_other if k % 2 else kv_all.at[y], y, k, lax.rem(y + k, NY)))

    for k in (1, 7, 2, 6):
        kv_send(k)

    l_qs.wait()
    qs = dot(normed[...], vqs[...])
    q0 = jnp.where(left_half, qs[:half], pltpu.roll(qs[half:], hd, 1))
    q1 = jnp.where(left_half, pltpu.roll(qs[:half], hd, 1), qs[half:])
    q_all[0, 0] = jnp.where(head == 0, q0, q1).astype(bf)
    q_other[...] = jnp.where(head == 0, q1, q0).astype(bf)

    def q_copy(j, e, to_z):
        src = q_other if e else q_all.at[0, 0]
        return remote(
            src, q_all.at[j, e], q_ss.at[j, e], q_rs.at[j, e], to_z * NY + (y_other if e else y), t
        )

    start(q_copy(0, 1, z))
    for j in (1, 2, 3, 4, 5, 6, 7):
        @pl.when(z - j >= 0)
        def _():
            q_copy(j, 0, z - j).start()
            q_copy(j, 1, z - j).start()

    l_kw.wait()
    l_vw.wait()
    kvw[...] = dot_t(normed[...], vkvw[...]).astype(bf)

    def prev_copy(to):
        return remote(kvw, kvw_prev, p_ss, p_rs, to, t)

    @pl.when(s < N_SP - 1)
    def _():
        prev_copy(s + 1).start()

    for k in (3, 5, 4):
        kv_send(k)

    @pl.when(s == 0)
    def _():
        kvw_prev[...] = jnp.zeros_like(kvw_prev)

    l_qw.wait()
    qw_buf[...] = dot(normed[...], vqw[...])

    def given(send, recv, ss, rs):
        for dx, dc in ((2, 0), (2, 1), (1, 0), (1, 1), (3, 0), (3, 1), (0, 1)):
            to = lax.rem(chip + dx, NX) * 2 + lax.rem(core + dc, 2)
            yield remote(send.at[to], recv.at[t], ss.at[2 * dx + dc], rs.at[t], s, to)

    def give(send, recv, ss, rs, values, weights):
        sums = jnp.sum(values * values, axis=1, keepdims=True)
        high = sums.astype(bf)
        low = (sums - high.astype(f32)).astype(bf)
        send[:, :, feats:] = jnp.where(left, high.astype(f32), low.astype(f32)).astype(bf).reshape(NT, cut, rows)
        gained, w = weights
        n_cut = 4
        part = feats // n_cut
        for n in range(n_cut):
            cols = slice(n * part, (n + 1) * part)
            send[:, :, cols] = dot(gained, w[:, cols]).astype(bf).reshape(NT, cut, part)
        for copy in given(send, recv, ss, rs):
            copy.start()

    def take(send, recv, ss, rs, acc, width):
        own = send[t].astype(f32)
        acc[...] = own[:, :feats]
        sums = own[:, feats:]
        for dx, dc in ((0, 1), (1, 0), (1, 1), (3, 0), (3, 1), (2, 0), (2, 1)):
            frm = lax.rem(chip + dx, NX) * 2 + lax.rem(core + dc, 2)
            remote(send.at[frm], recv.at[frm], ss.at[2 * dx + dc], rs.at[frm], s, partner).wait_recv()
            got = recv[frm].astype(f32)
            acc[...] += got[:, :feats]
            sums += got[:, feats:]
        return lax.rsqrt((sums[:, :1] + sums[:, hd : hd + 1]) * (1.0 / width) + EPS)

    def windowed():
        @pl.when(s > 0)
        def _():
            prev_copy(s - 1).wait_recv()

        two = 2 * rows
        r_iota = lax.broadcasted_iota(jnp.int32, (two, two), 0)
        c_iota = lax.broadcasted_iota(jnp.int32, (two, two), 1)
        dist = lax.rem(r_iota, rows) + rows - c_iota
        in_window = (dist >= 0) & (dist < WINDOW) & ((c_iota >= rows) | (s > 0))
        first_rows = lax.broadcasted_iota(jnp.int32, (two, 1), 0) < rows
        qw = qw_buf[...]
        kk = jnp.concatenate([kvw_prev[...], kvw[...]], axis=0)
        qq = jnp.concatenate([jnp.where(left, qw, 0.0), jnp.where(left, pltpu.roll(qw, hd, 1), 0.0)], axis=0).astype(bf)
        logits = jnp.where(in_window, dot_t(qq, kk) * hd**-0.5, -jnp.inf)
        sink = jnp.where(first_rows, sinks[0], sinks[1])
        top = jnp.maximum(jnp.max(logits, axis=1, keepdims=True), sink)
        grown = jnp.exp(logits - top)
        norm = jnp.sum(grown, axis=1, keepdims=True) + jnp.exp(sink - top)
        res = dot((grown / norm).astype(bf), kk)
        w_out = jnp.where(left, pltpu.roll(res[:rows], hd, 1), res[rows:]).astype(bf).astype(f32)

        l_ow.wait()
        give(b_send, b_recv, b_ss, b_rs, w_out, ((w_out * wgain[...].reshape(1, rows)).astype(bf), vow))

    def q_wait(j, e):
        frm = lax.rem(z + j, NZ) * NY + (y_other if e else y)
        remote(q_other, q_all.at[j, e], q_ss.at[j, e], q_rs.at[j, e], frm, t).wait_recv()

    def q_waits(js):
        for j in js:
            @pl.when(z + j < NZ)
            def _():
                if j:
                    q_wait(j, 0)
                q_wait(j, 1)

    kt = 2 * rows
    mb = 2 * rows
    per = mb // rows
    later = (
        lax.broadcasted_iota(jnp.int32, (kt, kt), 0) > lax.broadcasted_iota(jnp.int32, (kt, kt), 1)
    ).astype(bf)
    row2 = lax.broadcasted_iota(jnp.int32, (mb, kt), 0)
    lane2 = lax.broadcasted_iota(jnp.int32, (mb, kt), 1)
    place = lax.rem(row2, half) + jnp.where(row2 < half, y, y_other) * rows
    left2 = lax.broadcasted_iota(jnp.int32, (mb, rows), 1) < hd
    scale = LOG2E * hd**-0.5
    head_bias = bias[head] * LOG2E

    def segment(m, tile, straight, turned):
        part = slice(m * mb, (m + 1) * mb)
        queries = q_all[m * per : (m + 1) * per].reshape(mb, rows).astype(f32)
        outs = []
        sums = []
        for u in range(2):
            qh = jnp.where(jnp.logical_not(left2) if u else left2, queries, 0.0).astype(bf)
            score = dot_t(qh, turned if u else straight) * scale + head_bias
            pos = jnp.maximum(score, 0.0)
            neg = score - pos
            soft = jnp.log2(1.0 + jnp.exp2(neg - pos))
            drop = pos + soft
            hold = neg - soft
            if m == 0:
                usable = (row2 >= rows) | (lane2 + tile * kt < place + u * half)
                drop = jnp.where(usable, drop, 0.0)
                hold = jnp.where(usable, hold, -jnp.inf)
            suffix = dot(drop.astype(bf), later)
            weights = jnp.exp2(hold - suffix).astype(bf)
            outs.append(dot(weights, straight if u else turned))
            sums.append(suffix[:, :1] + drop[:, :1])
        o_seg[tile, part] = jnp.where(left2, outs[0], outs[1])
        t_seg[tile, part] = jnp.where(left2, sums[0], sums[1])

    def keys_of(tile):
        straight = kv_all[pl.ds(2 * tile, 2)].reshape(kt, rows)
        return straight, pltpu.roll(straight.astype(f32), hd, 1).astype(bf)

    def step(i, carry):
        @pl.when(i == 1)
        def _():
            windowed()

        tile = lax.rem(y // 2 + i + i // 2 - 2 * (i // 3), NY // 2)
        for u in range(2):
            src = 2 * tile + u

            @pl.when(src != y)
            def _():
                kv_copy(kv_other, src, 0, lax.rem(y + 1, NY)).wait_recv()

        straight, turned = keys_of(tile)
        for m in range(2):
            segment(m, tile, straight, turned)
        return carry

    def to_owner(j, e, sp, which):
        if which:
            return remote(o_send.at[j, e], o_recv.at[j, e], o_ss.at[j, e], o_rs.at[j, e], sp, t)
        return remote(t_send.at[j], t_recv.at[j, e], t_ss.at[j, e], t_rs.at[j, e], sp, t)

    first = lax.broadcasted_iota(jnp.int32, (8, rows), 0) < 4

    def finish(j):
        part = slice(j * rows, (j + 1) * rows)
        last = NY // 2 - 1
        acc = o_seg[last, part]
        carry = t_seg[last, part]
        for n in range(last - 1, -1, -1):
            acc = acc + jnp.exp2(-carry) * o_seg[n, part]
            carry = carry + t_seg[n, part]
        over = carry.T
        compact = jnp.where(first, over[0:8], over[hd : hd + 8])
        o_send[j] = acc.astype(bf).reshape(2, half, rows)
        t_send[j] = compact
        if j == 0:
            for which in range(2):
                start(to_owner(0, 1, z * NY + y_other, which))
        else:
            @pl.when(z + j < NZ)
            def _():
                for e in range(2):
                    for which in range(2):
                        to_owner(j, e, (z + j) * NY + (y_other if e else y), which).start()
        return acc[:half], compact

    q_waits((0, 1, 2, 3))
    lax.fori_loop(0, NY // 2, step, 0)
    for j in (3, 2, 1, 0):
        own_o, own_t = finish(j)
    for m in (2, 3):
        q_waits((2 * m, 2 * m + 1))

        def far_step(i, carry):
            for u in range(2):
                segment(m, 2 * i + u, *keys_of(2 * i + u))
            return carry

        lax.fori_loop(0, NY // 4, far_step, 0)
        for j in (2 * m, 2 * m + 1):
            finish(j)

    def from_owner(j, e, which):
        frm = lax.rem(z + NZ - j, NZ) * NY + (y_other if e else y)
        to_owner(j, e, frm, which).wait_recv()

    def arrivals(which):
        from_owner(0, 1, which)
        for j in range(1, NZ):
            @pl.when(z - j >= 0)
            def _():
                from_owner(j, 0, which)
                from_owner(j, 1, which)

    arrivals(0)
    left8 = left[:8]
    carry = jnp.where(left8, own_t, t_recv[0, 1])
    scales = []
    for j in range(1, NZ):
        scales.append(jnp.exp2(-carry))
        carry = carry + jnp.where(left8, t_recv[j, 0], t_recv[j, 1])
    scales = jnp.concatenate(scales + [jnp.zeros((rows - 8 * (NZ - 1), rows), f32)], axis=0).T
    arrivals(1)
    acc = jnp.concatenate([own_o, o_recv[0, 1].astype(f32)], axis=0)
    for j in range(1, NZ):
        at = 8 * (j - 1)
        here = o_recv[j].reshape(rows, rows).astype(f32)
        acc = acc + jnp.where(left, scales[:, at : at + 1], scales[:, at + 4 : at + 5]) * here
    head0 = jnp.where(head == 0, acc[:half], acc[half:])
    head1 = jnp.where(head == 0, acc[half:], acc[:half])
    s_out = jnp.concatenate(
        [
            jnp.where(left_half, head0, pltpu.roll(head1, hd, 1)),
            jnp.where(left_half, pltpu.roll(head0, hd, 1), head1),
        ],
        axis=0,
    ).astype(bf).astype(f32)
    l_os.wait()
    give(a_send, a_recv, a_ss, a_rs, s_out, ((s_out * sgain[...].reshape(1, rows)).astype(bf), vos))

    inv_w = take(b_send, b_recv, b_ss, b_rs, total.at[1], NT * rows)
    total[1] = total[1] * inv_w
    inv_s = take(a_send, a_recv, a_ss, a_rs, total.at[0], NT * rows)
    both = (total[0] * inv_s + total[1]).astype(bf).astype(f32)
    stats = jnp.sum(both * both, axis=1, keepdims=True) * (1.0 / feats)
    out[...] = (both * lax.rsqrt(stats + EPS) * post_gain[...].reshape(1, feats)).astype(bf)

    for refs in ((a_send, a_recv, a_ss, a_rs), (b_send, b_recv, b_ss, b_rs)):
        for copy in given(*refs):
            copy.wait_send()
    for copy in sends:
        copy.wait_send()
    for j in range(1, NZ):
        for e in range(2):
            @pl.when(z - j >= 0)
            def _():
                q_copy(j, e, z - j).wait_send()

            @pl.when(z + j < NZ)
            def _():
                for which in range(2):
                    to_owner(j, e, (z + j) * NY + (y_other if e else y), which).wait_send()

    @pl.when(s < N_SP - 1)
    def _():
        prev_copy(s + 1).wait_send()


def one_kernel(*args):
    tokens, pre_gain, wqs, wks, wvs, wqw, wkw, wvw, bias, sinks, sgain, wgain, wos, wow, post_gain = args
    bf = jnp.bfloat16
    f32 = jnp.float32
    rows, chunk = tokens.shape
    feats = NT * chunk
    cut = rows // NT
    v = pltpu.VMEM
    dma = pltpu.SemaphoreType.DMA
    anywhere = pl.BlockSpec(memory_space=pl.ANY)
    vmem = pl.BlockSpec(memory_space=pltpu.VMEM)
    scratch = [
        v(pre_gain.shape, f32), pltpu.SMEM(bias.shape, f32), pltpu.SMEM(sinks.shape, f32),
        v(sgain.shape, f32), v(wgain.shape, f32), v(post_gain.shape, f32),
        v((NT, rows, chunk), bf), v((rows, rows), f32), v((rows, feats), bf),
        v(wqs.shape, bf), v((feats, 2 * rows), bf), v(wqw.shape, bf), v((rows, feats), bf),
        v(wos.shape, bf), v(wow.shape, bf),
        v((NY, rows, rows), bf), v((rows, rows), bf), v((NZ, 2, rows // 2, rows), bf), v((rows // 2, rows), bf),
        v((NY // 2, NZ * rows, rows), f32), v((NY // 2, NZ * rows, rows), f32),
        v((rows, rows), bf), v((rows, rows), f32), v((rows, rows), bf),
        v((NZ, 2, rows // 2, rows), bf), v((NZ, 2, rows // 2, rows), bf),
        v((NZ, 8, rows), f32), v((NZ, 2, 8, rows), f32),
        v((NT, cut, feats + rows), bf), v((NT, cut, feats + rows), bf),
        v((NT, cut, feats + rows), bf), v((NT, cut, feats + rows), bf), v((2, cut, feats), f32),
        dma((14,)), dma, dma((8,)), dma((NT,)), dma((NY,)), dma((NY,)), dma((NZ, 2)), dma((NZ, 2)), dma, dma,
        dma((NZ, 2)), dma((NZ, 2)), dma((NZ, 2)), dma((NZ, 2)), dma((NT,)), dma((NT,)), dma((NT,)), dma((NT,)),
    ]
    return pl.pallas_call(
        kernel,
        out_shape=jax.ShapeDtypeStruct((cut, feats), bf),
        in_specs=[anywhere] * len(args),
        out_specs=vmem,
        scratch_shapes=scratch,
        compiler_params=pltpu.CompilerParams(
            collective_id=0, has_side_effects=True, vmem_limit_bytes=67043328
        ),
        name="layer",
    )(*args[:6], wkw.T, wvw.T, *args[8:])


def solution(mesh):
    in_specs = (
        P("sp", "tp"),
        P(),
        P(None, "tp"),
        P(None, "tp"),
        P(None, "tp"),
        P(None, "tp"),
        P(None, "tp"),
        P(None, "tp"),
        P("tp"),
        P("tp"),
        P("tp"),
        P("tp"),
        P("tp", None),
        P("tp", None),
        P(),
    )
    return jax.shard_map(
        one_kernel,
        mesh=mesh,
        in_specs=in_specs,
        out_specs=P(("sp", "tp"), None),
        check_vma=False,
    )
```

```python
import functools

import jax
import jax.numpy as jnp
from jax import lax
from jax.experimental import pallas as pl
from jax.experimental.pallas import tpu as pltpu
from jax.sharding import PartitionSpec as P

HEAD_DIM = 64
WINDOW = 128
EPS = 1e-06
LOG2E = 1.4426950408889634
MESH = pl.DeviceIdType.MESH
NY = 8
NZ = 8
NT = 8
NX = 4
N_SP = NY * NZ
PLACE = (0, 1, 3, 5, 7, 6, 4, 2)


def dot(a, b):
    return jnp.dot(a, b, preferred_element_type=jnp.float32)


def dot_t(a, b):
    return lax.dot_general(a, b, (((1,), (1,)), ((), ())), preferred_element_type=jnp.float32)


def kernel(
    tokens, pre_gain_in, wqs, wks, wvs, wqw, wkw, wvw, bias_in, sinks_in, sgain_in, wgain_in, wos, wow,
    post_gain_in, out,
    pre_gain, bias, sinks, sgain, wgain, post_gain, x, sq_acc, normed, vqs, vkv, vqw, vkvw, vos, vow,
    kv_all, kv_other, q_all, q_other, o_seg, t_seg, kvw, qw_buf, kvw_prev, o_send, o_recv, t_send, t_recv,
    a_send, a_recv, b_send, b_recv, total, out_buf,
    w_sem, tok_sem, x_ss, x_rs, kv_ss, kv_rs, q_ss, q_rs, p_ss, p_rs, o_ss, o_rs, t_ss, t_rs,
    a_ss, a_rs, b_ss, b_rs, out_sem,
):
    bf = jnp.bfloat16
    f32 = jnp.float32
    s = lax.axis_index("sp")
    t = lax.axis_index("tp")
    z = s // NY
    y = lax.rem(s, NY)
    chip = t // 2
    core = lax.rem(t, 2)
    head = lax.rem(y, 2)
    y_other = y + 1 - 2 * head
    partner = chip * 2 + 1 - core
    rows, chunk = tokens.shape
    feats = NT * chunk
    hd = HEAD_DIM
    cut = rows // NT

    barrier = pltpu.get_barrier_semaphore()

    def greet(sp, tp):
        pl.semaphore_signal(barrier, inc=1, device_id={"sp": sp, "tp": tp}, device_id_type=MESH)

    for k in range(1, NZ):
        greet(lax.rem(z + k, NZ) * NY + y, t)
        greet(lax.rem(z + k, NZ) * NY + y_other, t)
    for k in range(1, NY):
        greet(z * NY + lax.rem(y + k, NY), t)
    for k in range(1, NT):
        greet(s, lax.rem(t + k, NT))
    greet(lax.rem(s + 1, N_SP), t)
    greet(lax.rem(s + N_SP - 1, N_SP), t)

    half = rows // 2
    loads = [
        pltpu.make_async_copy(src, dst, w_sem.at[n])
        for n, (src, dst) in enumerate(
            [(wks, vkv.at[:, :rows]), (wvs, vkv.at[:, rows:]), (wqs, vqs), (wkw, vkvw.at[:half]), (wvw, vkvw.at[half:]), (wqw, vqw),
             (wow, vow), (wos, vos),
             (bias_in, bias), (pre_gain_in, pre_gain), (sinks_in, sinks), (sgain_in, sgain),
             (wgain_in, wgain), (post_gain_in, post_gain)]
        )
    ]
    l_ks, l_vs, l_qs, l_kw, l_vw, l_qw, l_ow, l_os, *l_small = loads
    tok_load = pltpu.make_async_copy(tokens, x.at[t], tok_sem)
    tok_load.start()
    for load in l_small + loads[:8]:
        load.start()

    for j in range(1, NZ):
        @pl.when(z + j >= NZ)
        def _():
            q_all[PLACE[j]] = jnp.zeros((2, half, rows), bf)

        @pl.when(z - j < 0)
        def _():
            o_recv[j] = jnp.zeros((2, half, rows), bf)
            t_recv[j] = jnp.zeros((2, 8, rows), f32)

    for load in l_small:
        load.wait()
    tok_load.wait()
    pl.semaphore_wait(barrier, 2 * NZ + NY + NT - 4 + 2)

    def remote(src, dst, ss, rs, sp, tp):
        return pltpu.make_async_remote_copy(
            src_ref=src, dst_ref=dst, send_sem=ss, recv_sem=rs,
            device_id={"sp": sp, "tp": tp}, device_id_type=MESH,
        )

    sends = []

    def x_copy(slot, sem, tp):
        return remote(x.at[slot], x.at[slot], x_ss.at[sem], x_rs.at[slot], s, tp)

    def start(copy):
        copy.start()
        sends.append(copy)

    for dx in (2, 1, 3):
        start(x_copy(t, dx, lax.rem(chip + dx, NX) * 2 + core))
    start(x_copy(t, 0, partner))

    def squares(slot):
        v = x[slot].astype(f32)
        v = v * v
        return v[:, : chunk // 2] + v[:, chunk // 2 :]

    sq_acc[...] = squares(t)
    for dx in (1, 3, 2):
        slot = lax.rem(chip + NX - dx, NX) * 2 + core
        x_copy(slot, dx, partner).wait_recv()
        start(x_copy(slot, NX + dx, partner))
        sq_acc[...] += squares(slot)
    for dx in (0, 1, 3, 2):
        slot = lax.rem(chip + NX - dx, NX) * 2 + 1 - core
        x_copy(slot, dx, partner).wait_recv()
        sq_acc[...] += squares(slot)
    inv = lax.rsqrt(jnp.sum(sq_acc[...], axis=1, keepdims=True) * (1.0 / feats) + EPS)
    for k in range(NT):
        cols = slice(k * chunk, (k + 1) * chunk)
        normed[:, cols] = (x[k].astype(f32) * inv * pre_gain[cols].reshape(1, chunk)).astype(bf)

    left = lax.broadcasted_iota(jnp.int32, (rows, rows), 1) < hd
    left_half = left[:half]

    l_ks.wait()
    l_vs.wait()
    kv = dot(normed[...], vkv[...])
    keys, values = kv[:, :rows], kv[:, rows:]
    head0 = jnp.where(left, keys, pltpu.roll(values, hd, 1))
    head1 = jnp.where(left, pltpu.roll(keys, hd, 1), values)
    kv_all[y] = jnp.where(head == 0, head0, head1).astype(bf)
    kv_other[...] = jnp.where(head == 0, head1, head0).astype(bf)

    def kv_copy(src, slot, sem, to_y):
        return remote(src, kv_all.at[slot], kv_ss.at[sem], kv_rs.at[slot], z * NY + to_y, t)

    def kv_send(k):
        start(kv_copy(kv_other if k % 2 else kv_all.at[y], y, k, lax.rem(y + k, NY)))

    for k in (1, 7):
        kv_send(k)

    l_qs.wait()
    qs = dot(normed[...], vqs[...])
    q0 = jnp.where(left_half, qs[:half], pltpu.roll(qs[half:], hd, 1))
    q1 = jnp.where(left_half, pltpu.roll(qs[:half], hd, 1), qs[half:])
    q_all[0, 0] = jnp.where(head == 0, q0, q1).astype(bf)
    q_other[...] = jnp.where(head == 0, q1, q0).astype(bf)

    def q_copy(j, e, to_z):
        src = q_other if e else q_all.at[0, 0]
        return remote(
            src, q_all.at[PLACE[j], e], q_ss.at[j, e], q_rs.at[j, e], to_z * NY + (y_other if e else y), t
        )

    start(q_copy(0, 1, z))
    for j in (1, 7, 2, 6, 3, 5, 4):
        @pl.when(z - j >= 0)
        def _():
            q_copy(j, 0, z - j).start()
            q_copy(j, 1, z - j).start()

    l_kw.wait()
    l_vw.wait()
    kvw[...] = dot_t(normed[...], vkvw[...]).astype(bf)

    def prev_copy(to):
        return remote(kvw, kvw_prev, p_ss, p_rs, to, t)

    @pl.when(s < N_SP - 1)
    def _():
        prev_copy(s + 1).start()

    for k in (2, 6, 3, 5, 4):
        kv_send(k)

    @pl.when(s == 0)
    def _():
        kvw_prev[...] = jnp.zeros_like(kvw_prev)

    l_qw.wait()
    qw_buf[...] = dot(normed[...], vqw[...])

    def given(send, recv, ss, rs):
        for dx, dc in ((2, 0), (2, 1), (1, 0), (1, 1), (3, 0), (3, 1), (0, 1)):
            to = lax.rem(chip + dx, NX) * 2 + lax.rem(core + dc, 2)
            yield remote(send.at[to], recv.at[t], ss.at[2 * dx + dc], rs.at[t], s, to)

    def give(send, recv, ss, rs, values, weights):
        sums = jnp.sum(values * values, axis=1, keepdims=True)
        high = sums.astype(bf)
        low = (sums - high.astype(f32)).astype(bf)
        send[:, :, feats:] = jnp.where(left, high.astype(f32), low.astype(f32)).astype(bf).reshape(NT, cut, rows)
        gained, w = weights
        n_cut = 4
        part = feats // n_cut
        for n in range(n_cut):
            cols = slice(n * part, (n + 1) * part)
            send[:, :, cols] = dot(gained, w[:, cols]).astype(bf).reshape(NT, cut, part)
        for copy in given(send, recv, ss, rs):
            copy.start()

    def take(send, recv, ss, rs, acc, width):
        own = send[t].astype(f32)
        acc[...] = own[:, :feats]
        sums = own[:, feats:]
        for dx, dc in ((0, 1), (1, 0), (1, 1), (3, 0), (3, 1), (2, 0), (2, 1)):
            frm = lax.rem(chip + dx, NX) * 2 + lax.rem(core + dc, 2)
            remote(send.at[frm], recv.at[frm], ss.at[2 * dx + dc], rs.at[frm], s, partner).wait_recv()
            got = recv[frm].astype(f32)
            acc[...] += got[:, :feats]
            sums += got[:, feats:]
        return lax.rsqrt((sums[:, :1] + sums[:, hd : hd + 1]) * (1.0 / width) + EPS)

    def windowed():
        @pl.when(s > 0)
        def _():
            prev_copy(s - 1).wait_recv()

        two = 2 * rows
        r_iota = lax.broadcasted_iota(jnp.int32, (two, two), 0)
        c_iota = lax.broadcasted_iota(jnp.int32, (two, two), 1)
        dist = lax.rem(r_iota, rows) + rows - c_iota
        in_window = (dist >= 0) & (dist < WINDOW) & ((c_iota >= rows) | (s > 0))
        first_rows = lax.broadcasted_iota(jnp.int32, (two, 1), 0) < rows
        qw = qw_buf[...]
        kk = jnp.concatenate([kvw_prev[...], kvw[...]], axis=0)
        qq = jnp.concatenate([jnp.where(left, qw, 0.0), jnp.where(left, pltpu.roll(qw, hd, 1), 0.0)], axis=0).astype(bf)
        logits = jnp.where(in_window, dot_t(qq, kk) * hd**-0.5, -jnp.inf)
        sink = jnp.where(first_rows, sinks[0], sinks[1])
        top = jnp.maximum(jnp.max(logits, axis=1, keepdims=True), sink)
        grown = jnp.exp(logits - top)
        norm = jnp.sum(grown, axis=1, keepdims=True) + jnp.exp(sink - top)
        res = dot((grown / norm).astype(bf), kk)
        w_out = jnp.where(left, pltpu.roll(res[:rows], hd, 1), res[rows:]).astype(bf).astype(f32)

        l_ow.wait()
        give(b_send, b_recv, b_ss, b_rs, w_out, ((w_out * wgain[...].reshape(1, rows)).astype(bf), vow))

    def q_wait(j, e):
        frm = lax.rem(z + j, NZ) * NY + (y_other if e else y)
        remote(q_other, q_all.at[PLACE[j], e], q_ss.at[j, e], q_rs.at[j, e], frm, t).wait_recv()

    def q_waits(js):
        for j in js:
            @pl.when(z + j < NZ)
            def _():
                if j:
                    q_wait(j, 0)
                q_wait(j, 1)

    kt = 2 * rows
    mb = 2 * rows
    per = mb // rows
    later = (
        lax.broadcasted_iota(jnp.int32, (kt, kt), 0) > lax.broadcasted_iota(jnp.int32, (kt, kt), 1)
    ).astype(bf)
    row2 = lax.broadcasted_iota(jnp.int32, (mb, kt), 0)
    lane2 = lax.broadcasted_iota(jnp.int32, (mb, kt), 1)
    place = lax.rem(row2, half) + jnp.where(row2 < half, y, y_other) * rows
    left2 = lax.broadcasted_iota(jnp.int32, (mb, rows), 1) < hd
    scale = LOG2E * hd**-0.5
    head_bias = bias[head] * LOG2E

    def segment(m, tile):
        part = slice(m * mb, (m + 1) * mb)
        straight, turned = keys_of(tile)
        queries = q_all[m * per : (m + 1) * per].reshape(mb, rows).astype(f32)
        outs = []
        sums = []
        for u in range(2):
            qh = jnp.where(jnp.logical_not(left2) if u else left2, queries, 0.0).astype(bf)
            score = dot_t(qh, turned if u else straight) * scale + head_bias
            pos = jnp.maximum(score, 0.0)
            neg = score - pos
            soft = jnp.log2(1.0 + jnp.exp2(neg - pos))
            drop = pos + soft
            hold = neg - soft
            if m == 0:
                usable = (row2 >= rows) | (lane2 + tile * kt < place + u * half)
                drop = jnp.where(usable, drop, 0.0)
                hold = jnp.where(usable, hold, -jnp.inf)
            suffix = dot(drop.astype(bf), later)
            weights = jnp.exp2(hold - suffix).astype(bf)
            outs.append(dot(weights, straight if u else turned))
            sums.append(suffix[:, :1] + drop[:, :1])
        o_seg[tile, part] = jnp.where(left2, outs[0], outs[1])
        t_seg[tile, part] = jnp.where(left2, sums[0], sums[1])

    def keys_of(tile):
        straight = kv_all[pl.ds(2 * tile, 2)].reshape(kt, rows)
        return straight, pltpu.roll(straight.astype(f32), hd, 1).astype(bf)

    near = y // 2
    side = 2 * head - 1
    tiles = [lax.rem(near + k * side + NY // 2, NY // 2) for k in (0, 1, -1, 2)]

    def kv_waits(k):
        for u in range(2):
            src = 2 * tiles[k] + u

            @pl.when(src != y)
            def _():
                kv_copy(kv_other, src, 0, lax.rem(y + 1, NY)).wait_recv()

    def to_owner(j, e, sp, which):
        if which:
            return remote(o_send.at[j, e], o_recv.at[j, e], o_ss.at[j, e], o_rs.at[j, e], sp, t)
        return remote(t_send.at[j], t_recv.at[j, e], t_ss.at[j, e], t_rs.at[j, e], sp, t)

    first = lax.broadcasted_iota(jnp.int32, (8, rows), 0) < 4

    def finish(j):
        part = slice(PLACE[j] * rows, (PLACE[j] + 1) * rows)
        last = NY // 2 - 1
        acc = o_seg[last, part]
        carry = t_seg[last, part]
        for n in range(last - 1, -1, -1):
            acc = acc + jnp.exp2(-carry) * o_seg[n, part]
            carry = carry + t_seg[n, part]
        over = carry.T
        compact = jnp.where(first, over[0:8], over[hd : hd + 8])
        o_send[j] = acc.astype(bf).reshape(2, half, rows)
        t_send[j] = compact
        if j == 0:
            for which in range(2):
                start(to_owner(0, 1, z * NY + y_other, which))
        else:
            @pl.when(z + j < NZ)
            def _():
                for e in range(2):
                    for which in range(2):
                        to_owner(j, e, (z + j) * NY + (y_other if e else y), which).start()
        return acc[:half], compact

    def segments(*pairs):
        for m, k in pairs:
            segment(m, tiles[k])

    q_waits((0, 1))
    kv_waits(0)
    segments((0, 0))
    windowed()
    q_waits((7, 2))
    kv_waits(1)
    segments((0, 1), (1, 0))
    segments((1, 1))
    q_waits((6, 3))
    segments((2, 0), (2, 1))
    kv_waits(2)
    segments((0, 2), (1, 2))
    kv_waits(3)
    segments((0, 3), (1, 3))
    own_o, own_t = finish(0)
    for j in (2, 1, 7):
        finish(j)
    segments((2, 2), (2, 3))
    for j in (3, 6):
        finish(j)
    q_waits((5, 4))
    segments((3, 0), (3, 1))
    segments((3, 2), (3, 3))
    for j in (4, 5):
        finish(j)

    def from_owner(j, e, which):
        frm = lax.rem(z + NZ - j, NZ) * NY + (y_other if e else y)
        to_owner(j, e, frm, which).wait_recv()

    def arrivals(which):
        from_owner(0, 1, which)
        for j in range(1, NZ):
            @pl.when(z - j >= 0)
            def _():
                from_owner(j, 0, which)
                from_owner(j, 1, which)

    arrivals(0)
    left8 = left[:8]
    carry = jnp.where(left8, own_t, t_recv[0, 1])
    scales = []
    for j in range(1, NZ):
        scales.append(jnp.exp2(-carry))
        carry = carry + jnp.where(left8, t_recv[j, 0], t_recv[j, 1])
    scales = jnp.concatenate(scales + [jnp.zeros((rows - 8 * (NZ - 1), rows), f32)], axis=0).T
    arrivals(1)
    acc = jnp.concatenate([own_o, o_recv[0, 1].astype(f32)], axis=0)
    for j in range(1, NZ):
        at = 8 * (j - 1)
        here = o_recv[j].reshape(rows, rows).astype(f32)
        acc = acc + jnp.where(left, scales[:, at : at + 1], scales[:, at + 4 : at + 5]) * here
    head0 = jnp.where(head == 0, acc[:half], acc[half:])
    head1 = jnp.where(head == 0, acc[half:], acc[:half])
    s_out = jnp.concatenate(
        [
            jnp.where(left_half, head0, pltpu.roll(head1, hd, 1)),
            jnp.where(left_half, pltpu.roll(head0, hd, 1), head1),
        ],
        axis=0,
    ).astype(bf).astype(f32)
    l_os.wait()
    give(a_send, a_recv, a_ss, a_rs, s_out, ((s_out * sgain[...].reshape(1, rows)).astype(bf), vos))

    inv_w = take(b_send, b_recv, b_ss, b_rs, total.at[1], NT * rows)
    total[1] = total[1] * inv_w
    inv_s = take(a_send, a_recv, a_ss, a_rs, total.at[0], NT * rows)
    both = (total[0] * inv_s + total[1]).astype(bf).astype(f32)
    stats = jnp.sum(both * both, axis=1, keepdims=True) * (1.0 / feats)
    out_buf[...] = (both * lax.rsqrt(stats + EPS) * post_gain[...].reshape(1, feats)).astype(bf)

    out_copy = pltpu.make_async_copy(out_buf, out, out_sem)
    out_copy.start()
    for refs in ((a_send, a_recv, a_ss, a_rs), (b_send, b_recv, b_ss, b_rs)):
        for copy in given(*refs):
            copy.wait_send()
    for copy in sends:
        copy.wait_send()
    for j in range(1, NZ):
        for e in range(2):
            @pl.when(z - j >= 0)
            def _():
                q_copy(j, e, z - j).wait_send()

            @pl.when(z + j < NZ)
            def _():
                for which in range(2):
                    to_owner(j, e, (z + j) * NY + (y_other if e else y), which).wait_send()

    @pl.when(s < N_SP - 1)
    def _():
        prev_copy(s + 1).wait_send()

    out_copy.wait()


def one_kernel(*args):
    tokens, pre_gain, wqs, wks, wvs, wqw, wkw, wvw, bias, sinks, sgain, wgain, wos, wow, post_gain = args
    bf = jnp.bfloat16
    f32 = jnp.float32
    rows, chunk = tokens.shape
    feats = NT * chunk
    cut = rows // NT
    v = pltpu.VMEM
    dma = pltpu.SemaphoreType.DMA
    anywhere = pl.BlockSpec(memory_space=pl.ANY)
    scratch = [
        v(pre_gain.shape, f32), pltpu.SMEM(bias.shape, f32), pltpu.SMEM(sinks.shape, f32),
        v(sgain.shape, f32), v(wgain.shape, f32), v(post_gain.shape, f32),
        v((NT, rows, chunk), bf), v((rows, rows), f32), v((rows, feats), bf),
        v(wqs.shape, bf), v((feats, 2 * rows), bf), v(wqw.shape, bf), v((rows, feats), bf),
        v(wos.shape, bf), v(wow.shape, bf),
        v((NY, rows, rows), bf), v((rows, rows), bf), v((NZ, 2, rows // 2, rows), bf), v((rows // 2, rows), bf),
        v((NY // 2, NZ * rows, rows), f32), v((NY // 2, NZ * rows, rows), f32),
        v((rows, rows), bf), v((rows, rows), f32), v((rows, rows), bf),
        v((NZ, 2, rows // 2, rows), bf), v((NZ, 2, rows // 2, rows), bf),
        v((NZ, 8, rows), f32), v((NZ, 2, 8, rows), f32),
        v((NT, cut, feats + rows), bf), v((NT, cut, feats + rows), bf),
        v((NT, cut, feats + rows), bf), v((NT, cut, feats + rows), bf), v((2, cut, feats), f32), v((cut, feats), bf),
        dma((14,)), dma, dma((8,)), dma((NT,)), dma((NY,)), dma((NY,)), dma((NZ, 2)), dma((NZ, 2)), dma, dma,
        dma((NZ, 2)), dma((NZ, 2)), dma((NZ, 2)), dma((NZ, 2)), dma((NT,)), dma((NT,)), dma((NT,)), dma((NT,)), dma,
    ]
    return pl.pallas_call(
        kernel,
        out_shape=jax.ShapeDtypeStruct((cut, feats), bf),
        in_specs=[anywhere] * len(args),
        out_specs=anywhere,
        scratch_shapes=scratch,
        compiler_params=pltpu.CompilerParams(
            collective_id=0, has_side_effects=True, vmem_limit_bytes=67043328
        ),
        name="layer",
    )(*args[:6], wkw.T, wvw.T, *args[8:])


def solution(mesh):
    in_specs = (
        P("sp", "tp"),
        P(),
        P(None, "tp"),
        P(None, "tp"),
        P(None, "tp"),
        P(None, "tp"),
        P(None, "tp"),
        P(None, "tp"),
        P("tp"),
        P("tp"),
        P("tp"),
        P("tp"),
        P("tp", None),
        P("tp", None),
        P(),
    )
    return jax.shard_map(
        one_kernel,
        mesh=mesh,
        in_specs=in_specs,
        out_specs=P(("sp", "tp"), None),
        check_vma=False,
    )
```

```python
import functools

import jax
import jax.numpy as jnp
from jax import lax
from jax.experimental import pallas as pl
from jax.experimental.pallas import tpu as pltpu
from jax.sharding import PartitionSpec as P

HEAD_DIM = 64
WINDOW = 128
EPS = 1e-06
LOG2E = 1.4426950408889634
MESH = pl.DeviceIdType.MESH
NY = 8
NZ = 8
NT = 8
NX = 4
N_SP = NY * NZ
PLACE = (0, 1, 3, 5, 7, 6, 4, 2)


def dot(a, b):
    return jnp.dot(a, b, preferred_element_type=jnp.float32)


def dot_t(a, b):
    return lax.dot_general(a, b, (((1,), (1,)), ((), ())), preferred_element_type=jnp.float32)


def kernel(
    tokens, pre_gain_in, wqs, wks, wvs, wqw, wkw, wvw, bias_in, sinks_in, sgain_in, wgain_in, wos, wow,
    post_gain_in, out,
    pre_gain, bias, sinks, sgain, wgain, post_gain, x, sq_acc, proj, vproj, kvw_acc, vkvw, vos, vow,
    kv_all, kv_other, q_all, q_other, o_seg, t_seg, kvw, qw_buf, kvw_prev, o_send, o_recv, t_send, t_recv,
    a_keep0, a_keep1, d_send0, d_send1, d_recv0, d_recv1, r_send0, r_send1, r_recv0, r_recv1,
    b_send, b_recv, total, out_buf,
    w_sem, tok_sem, x_ss, x_rs, kv_ss, kv_rs, q_ss, q_rs, p_ss, p_rs, o_ss, o_rs, t_ss, t_rs,
    d_ss, d_rs, r_ss, r_rs, b_ss, b_rs, out_sem,
):
    bf = jnp.bfloat16
    f32 = jnp.float32
    s = lax.axis_index("sp")
    t = lax.axis_index("tp")
    z = s // NY
    y = lax.rem(s, NY)
    chip = t // 2
    core = lax.rem(t, 2)
    head = lax.rem(y, 2)
    y_other = y + 1 - 2 * head
    partner = chip * 2 + 1 - core
    rows, chunk = tokens.shape
    feats = NT * chunk
    hd = HEAD_DIM
    cut = rows // NT

    barrier = pltpu.get_barrier_semaphore()

    def greet(sp, tp):
        pl.semaphore_signal(barrier, inc=1, device_id={"sp": sp, "tp": tp}, device_id_type=MESH)

    for k in range(1, NZ):
        greet(lax.rem(z + k, NZ) * NY + y, t)
        greet(lax.rem(z + k, NZ) * NY + y_other, t)
    for k in range(1, NY):
        greet(z * NY + lax.rem(y + k, NY), t)
    for k in range(1, NT):
        greet(s, lax.rem(t + k, NT))
    greet(lax.rem(s + 1, N_SP), t)
    greet(lax.rem(s + N_SP - 1, N_SP), t)

    half = rows // 2
    loads = [
        pltpu.make_async_copy(src, dst, w_sem.at[n])
        for n, (src, dst) in enumerate(
            [(wks, vproj.at[:, :rows]), (wvs, vproj.at[:, rows : 2 * rows]), (wqs, vproj.at[:, 2 * rows : 3 * rows]),
             (wqw, vproj.at[:, 3 * rows :]), (wkw, vkvw.at[:half]), (wvw, vkvw.at[half:]),
             (wow, vow), (wos, vos),
             (bias_in, bias), (pre_gain_in, pre_gain), (sinks_in, sinks), (sgain_in, sgain),
             (wgain_in, wgain), (post_gain_in, post_gain)]
        )
    ]
    l_proj = loads[:6]
    l_ow, l_os, *l_small = loads[6:]
    tok_load = pltpu.make_async_copy(tokens, x.at[t], tok_sem)
    tok_load.start()
    for load in l_small + loads[:8]:
        load.start()

    for j in range(1, NZ):
        @pl.when(z + j >= NZ)
        def _():
            q_all[PLACE[j]] = jnp.zeros((2, half, rows), bf)

        @pl.when(z - j < 0)
        def _():
            o_recv[j] = jnp.zeros((2, half, rows), bf)
            t_recv[j] = jnp.zeros((2, 8, rows), f32)

    for load in l_small:
        load.wait()
    tok_load.wait()
    pl.semaphore_wait(barrier, 2 * NZ + NY + NT - 4 + 2)

    def remote(src, dst, ss, rs, sp, tp):
        return pltpu.make_async_remote_copy(
            src_ref=src, dst_ref=dst, send_sem=ss, recv_sem=rs,
            device_id={"sp": sp, "tp": tp}, device_id_type=MESH,
        )

    sends = []

    def x_copy(slot, sem, tp):
        return remote(x.at[slot], x.at[slot], x_ss.at[sem], x_rs.at[slot], s, tp)

    def start(copy):
        copy.start()
        sends.append(copy)

    for dx in (2, 1, 3):
        start(x_copy(t, dx, lax.rem(chip + dx, NX) * 2 + core))
    start(x_copy(t, 0, partner))

    def absorb(slot, first=False):
        v = x[slot].astype(f32)
        part = pl.ds(pl.multiple_of(slot * chunk, chunk), chunk)
        gained = (v * pre_gain[part].reshape(1, chunk)).astype(bf)
        v = v * v
        v = v[:, : chunk // 2] + v[:, chunk // 2 :]
        sq_acc[...] = v if first else sq_acc[...] + v
        more = dot(gained, vproj[part, :])
        proj[...] = more if first else proj[...] + more
        more = dot_t(gained, vkvw[:, part])
        kvw_acc[...] = more if first else kvw_acc[...] + more

    for load in l_proj:
        load.wait()
    absorb(t, True)
    for dx, relayed in ((0, 1), (1, 0), (3, 0), (1, 1), (3, 1), (2, 0), (2, 1)):
        slot = lax.rem(chip + NX - dx, NX) * 2 + (1 - core if relayed else core)
        x_copy(slot, dx, partner).wait_recv()
        if not relayed:
            start(x_copy(slot, NX + dx, partner))
        absorb(slot)
    inv = lax.rsqrt(jnp.sum(sq_acc[...], axis=1, keepdims=True) * (1.0 / feats) + EPS)

    left = lax.broadcasted_iota(jnp.int32, (rows, rows), 1) < hd
    left_half = left[:half]

    keys, values = proj[:, :rows] * inv, proj[:, rows : 2 * rows] * inv
    head0 = jnp.where(left, keys, pltpu.roll(values, hd, 1))
    head1 = jnp.where(left, pltpu.roll(keys, hd, 1), values)
    kv_all[y] = jnp.where(head == 0, head0, head1).astype(bf)
    kv_other[...] = jnp.where(head == 0, head1, head0).astype(bf)

    def kv_copy(src, slot, sem, to_y):
        return remote(src, kv_all.at[slot], kv_ss.at[sem], kv_rs.at[slot], z * NY + to_y, t)

    def kv_send(k):
        start(kv_copy(kv_other if k % 2 else kv_all.at[y], y, k, lax.rem(y + k, NY)))

    for k in (1, 7):
        kv_send(k)

    qs = proj[:, 2 * rows : 3 * rows] * inv
    q0 = jnp.where(left_half, qs[:half], pltpu.roll(qs[half:], hd, 1))
    q1 = jnp.where(left_half, pltpu.roll(qs[:half], hd, 1), qs[half:])
    q_all[0, 0] = jnp.where(head == 0, q0, q1).astype(bf)
    q_other[...] = jnp.where(head == 0, q1, q0).astype(bf)

    def q_copy(j, e, to_z):
        src = q_other if e else q_all.at[0, 0]
        return remote(
            src, q_all.at[PLACE[j], e], q_ss.at[j, e], q_rs.at[j, e], to_z * NY + (y_other if e else y), t
        )

    start(q_copy(0, 1, z))
    for j in (1, 7, 2, 6, 3, 5, 4):
        @pl.when(z - j >= 0)
        def _():
            q_copy(j, 0, z - j).start()
            q_copy(j, 1, z - j).start()

    kvw[...] = (kvw_acc[...] * inv).astype(bf)

    def prev_copy(to):
        return remote(kvw, kvw_prev, p_ss, p_rs, to, t)

    @pl.when(s < N_SP - 1)
    def _():
        prev_copy(s + 1).start()

    for k in (2, 6, 3, 5, 4):
        kv_send(k)

    @pl.when(s == 0)
    def _():
        kvw_prev[...] = jnp.zeros_like(kvw_prev)

    qw_buf[...] = proj[:, 3 * rows :] * inv

    def given(send, recv, ss, rs):
        for dx, dc in ((2, 0), (2, 1), (1, 0), (1, 1), (3, 0), (3, 1), (0, 1)):
            to = lax.rem(chip + dx, NX) * 2 + lax.rem(core + dc, 2)
            yield remote(send.at[to], recv.at[t], ss.at[2 * dx + dc], rs.at[t], s, to)

    def give(send, recv, ss, rs, values, weights):
        sums = jnp.sum(values * values, axis=1, keepdims=True)
        high = sums.astype(bf)
        low = (sums - high.astype(f32)).astype(bf)
        send[:, :, feats:] = jnp.where(left, high.astype(f32), low.astype(f32)).astype(bf).reshape(NT, cut, rows)
        gained, w = weights
        n_cut = 4
        part = feats // n_cut
        for n in range(n_cut):
            cols = slice(n * part, (n + 1) * part)
            send[:, :, cols] = dot(gained, w[:, cols]).astype(bf).reshape(NT, cut, part)
        for copy in given(send, recv, ss, rs):
            copy.start()

    def take(send, recv, ss, rs, acc, width):
        own = send[t].astype(f32)
        acc[...] = own[:, :feats]
        sums = own[:, feats:]
        for dx, dc in ((0, 1), (1, 0), (1, 1), (3, 0), (3, 1), (2, 0), (2, 1)):
            frm = lax.rem(chip + dx, NX) * 2 + lax.rem(core + dc, 2)
            remote(send.at[frm], recv.at[frm], ss.at[2 * dx + dc], rs.at[frm], s, partner).wait_recv()
            got = recv[frm].astype(f32)
            acc[...] += got[:, :feats]
            sums += got[:, feats:]
        return lax.rsqrt((sums[:, :1] + sums[:, hd : hd + 1]) * (1.0 / width) + EPS)

    def windowed():
        @pl.when(s > 0)
        def _():
            prev_copy(s - 1).wait_recv()

        two = 2 * rows
        r_iota = lax.broadcasted_iota(jnp.int32, (two, two), 0)
        c_iota = lax.broadcasted_iota(jnp.int32, (two, two), 1)
        dist = lax.rem(r_iota, rows) + rows - c_iota
        in_window = (dist >= 0) & (dist < WINDOW) & ((c_iota >= rows) | (s > 0))
        first_rows = lax.broadcasted_iota(jnp.int32, (two, 1), 0) < rows
        qw = qw_buf[...]
        kk = jnp.concatenate([kvw_prev[...], kvw[...]], axis=0)
        qq = jnp.concatenate([jnp.where(left, qw, 0.0), jnp.where(left, pltpu.roll(qw, hd, 1), 0.0)], axis=0).astype(bf)
        logits = jnp.where(in_window, dot_t(qq, kk) * hd**-0.5, -jnp.inf)
        sink = jnp.where(first_rows, sinks[0], sinks[1])
        top = jnp.maximum(jnp.max(logits, axis=1, keepdims=True), sink)
        grown = jnp.exp(logits - top)
        norm = jnp.sum(grown, axis=1, keepdims=True) + jnp.exp(sink - top)
        res = dot((grown / norm).astype(bf), kk)
        w_out = jnp.where(left, pltpu.roll(res[:rows], hd, 1), res[rows:]).astype(bf).astype(f32)

        l_ow.wait()
        give(b_send, b_recv, b_ss, b_rs, w_out, ((w_out * wgain[...].reshape(1, rows)).astype(bf), vow))

    def q_wait(j, e):
        frm = lax.rem(z + j, NZ) * NY + (y_other if e else y)
        remote(q_other, q_all.at[PLACE[j], e], q_ss.at[j, e], q_rs.at[j, e], frm, t).wait_recv()

    def q_waits(js):
        for j in js:
            @pl.when(z + j < NZ)
            def _():
                if j:
                    q_wait(j, 0)
                q_wait(j, 1)

    kt = 2 * rows
    mb = 2 * rows
    per = mb // rows
    later = (
        lax.broadcasted_iota(jnp.int32, (kt, kt), 0) > lax.broadcasted_iota(jnp.int32, (kt, kt), 1)
    ).astype(bf)
    row2 = lax.broadcasted_iota(jnp.int32, (mb, kt), 0)
    lane2 = lax.broadcasted_iota(jnp.int32, (mb, kt), 1)
    place = lax.rem(row2, half) + jnp.where(row2 < half, y, y_other) * rows
    left2 = lax.broadcasted_iota(jnp.int32, (mb, rows), 1) < hd
    scale = LOG2E * hd**-0.5
    head_bias = bias[head] * LOG2E

    def segment(pairs):
        weights_of = {}
        chains = []
        for m, k in pairs:
            if k not in weights_of:
                weights_of[k] = keys_of(tiles[k])
            queries = q_all[m * per : (m + 1) * per].reshape(mb, rows).astype(f32)
            for u in range(2):
                qh = jnp.where(jnp.logical_not(left2) if u else left2, queries, 0.0).astype(bf)
                chains.append((m, k, u, qh))

        def by_weights(values, flip):
            res = [None] * len(chains)
            for k in weights_of:
                for u in range(2):
                    own = [n for n, c in enumerate(chains) if c[1] == k and c[2] == u]
                    joint = jnp.concatenate([values[n] for n in own], axis=0)
                    w = weights_of[k][1 - u if flip else u]
                    got = dot(joint, w) if flip else dot_t(joint, w)
                    for at, n in enumerate(own):
                        res[n] = got[at * mb : (at + 1) * mb]
            return res

        drops = []
        holds = []
        for (m, k, u, _), raw in zip(chains, by_weights([c[3] for c in chains], False)):
            score = raw * scale + head_bias
            pos = jnp.maximum(score, 0.0)
            neg = score - pos
            soft = jnp.log2(1.0 + jnp.exp2(neg - pos))
            drop = pos + soft
            hold = neg - soft
            if m == 0:
                usable = (row2 >= rows) | (lane2 + tiles[k] * kt < place + u * half)
                drop = jnp.where(usable, drop, 0.0)
                hold = jnp.where(usable, hold, -jnp.inf)
            drops.append(drop)
            holds.append(hold)
        suffix = dot(jnp.concatenate([d.astype(bf) for d in drops], axis=0), later)
        suffix = [suffix[n * mb : (n + 1) * mb] for n in range(len(chains))]
        outs = by_weights([jnp.exp2(h - f).astype(bf) for h, f in zip(holds, suffix)], True)
        sums = [f[:, :1] + d[:, :1] for f, d in zip(suffix, drops)]
        for n in range(0, len(chains), 2):
            m, k, _, _ = chains[n]
            part = slice(m * mb, (m + 1) * mb)
            o_seg[tiles[k], part] = jnp.where(left2, outs[n], outs[n + 1])
            t_seg[tiles[k], part] = jnp.where(left2, sums[n], sums[n + 1])

    def keys_of(tile):
        straight = kv_all[pl.ds(2 * tile, 2)].reshape(kt, rows)
        return straight, pltpu.roll(straight.astype(f32), hd, 1).astype(bf)

    near = y // 2
    side = 2 * head - 1
    tiles = [lax.rem(near + k * side + NY // 2, NY // 2) for k in (0, 1, -1, 2)]

    def kv_waits(k):
        for u in range(2):
            src = 2 * tiles[k] + u

            @pl.when(src != y)
            def _():
                kv_copy(kv_other, src, 0, lax.rem(y + 1, NY)).wait_recv()

    def to_owner(j, e, sp, which):
        if which:
            return remote(o_send.at[j, e], o_recv.at[j, e], o_ss.at[j, e], o_rs.at[j, e], sp, t)
        return remote(t_send.at[j], t_recv.at[j, e], t_ss.at[j, e], t_rs.at[j, e], sp, t)

    first = lax.broadcasted_iota(jnp.int32, (8, rows), 0) < 4

    def finish(j):
        part = slice(PLACE[j] * rows, (PLACE[j] + 1) * rows)
        last = NY // 2 - 1
        acc = o_seg[last, part]
        carry = t_seg[last, part]
        for n in range(last - 1, -1, -1):
            acc = acc + jnp.exp2(-carry) * o_seg[n, part]
            carry = carry + t_seg[n, part]
        over = carry.T
        compact = jnp.where(first, over[0:8], over[hd : hd + 8])
        o_send[j] = acc.astype(bf).reshape(2, half, rows)
        t_send[j] = compact
        if j == 0:
            for which in range(2):
                start(to_owner(0, 1, z * NY + y_other, which))
        else:
            @pl.when(z + j < NZ)
            def _():
                for e in range(2):
                    for which in range(2):
                        to_owner(j, e, (z + j) * NY + (y_other if e else y), which).start()
        return acc[:half], compact

    def segments(*pairs):
        segment(pairs)

    q_waits((0, 1))
    kv_waits(0)
    segments((0, 0))
    windowed()
    q_waits((7, 2))
    kv_waits(1)
    segments((0, 1), (1, 1))
    segments((1, 0))
    q_waits((6, 3, 5, 4))
    segments((2, 0), (3, 0))
    segments((2, 1), (3, 1))
    kv_waits(2)
    segments((2, 2), (3, 2))
    kv_waits(3)
    segments((2, 3), (3, 3))
    for j in (4, 5, 3, 6):
        finish(j)
    segments((0, 2), (1, 2))
    segments((0, 3), (1, 3))
    for j in (2, 1, 7):
        finish(j)
    own_o, own_t = finish(0)

    def from_owner(j, e, which):
        frm = lax.rem(z + NZ - j, NZ) * NY + (y_other if e else y)
        to_owner(j, e, frm, which).wait_recv()

    def arrivals(which):
        from_owner(0, 1, which)
        for j in range(1, NZ):
            @pl.when(z - j >= 0)
            def _():
                from_owner(j, 0, which)
                from_owner(j, 1, which)

    arrivals(0)
    left8 = left[:8]
    carry = jnp.where(left8, own_t, t_recv[0, 1])
    scales = []
    for j in range(1, NZ):
        scales.append(jnp.exp2(-carry))
        carry = carry + jnp.where(left8, t_recv[j, 0], t_recv[j, 1])
    scales = jnp.concatenate(scales + [jnp.zeros((rows - 8 * (NZ - 1), rows), f32)], axis=0).T
    arrivals(1)
    acc = jnp.concatenate([own_o, o_recv[0, 1].astype(f32)], axis=0)
    for j in range(1, NZ):
        at = 8 * (j - 1)
        here = o_recv[j].reshape(rows, rows).astype(f32)
        acc = acc + jnp.where(left, scales[:, at : at + 1], scales[:, at + 4 : at + 5]) * here
    head0 = jnp.where(head == 0, acc[:half], acc[half:])
    head1 = jnp.where(head == 0, acc[half:], acc[:half])
    s_out = jnp.concatenate(
        [
            jnp.where(left_half, head0, pltpu.roll(head1, hd, 1)),
            jnp.where(left_half, pltpu.roll(head0, hd, 1), head1),
        ],
        axis=0,
    ).astype(bf).astype(f32)
    l_os.wait()
    gained = (s_out * sgain[...].reshape(1, rows)).astype(bf)
    own_sums = jnp.broadcast_to(jnp.sum(s_out * s_out, axis=1, keepdims=True), (rows, rows))
    part = feats // 2
    pieces = ((a_keep0, d_send0, d_recv0, r_send0, r_recv0), (a_keep1, d_send1, d_recv1, r_send1, r_recv1))
    left_cut = left[:cut].reshape(1, cut, rows)

    def halves(values):
        return jnp.where(core == 0, values[:, 0], values[:, 1]), jnp.where(core == 0, values[:, 1], values[:, 0])

    def in_two(values):
        high = values.astype(bf).astype(f32)
        return jnp.where(left_cut, high, values - high).astype(bf)

    def joined(values):
        return values + pltpu.roll(values, hd, values.ndim - 1)

    def across(n):
        return remote(pieces[n][1], pieces[n][2], d_ss.at[n], d_rs.at[n], s, partner)

    def along(n, dx):
        to = lax.rem(chip + dx, NX)
        return remote(
            pieces[n][3].at[to], pieces[n][4].at[chip], r_ss.at[n, dx], r_rs.at[n, chip], s, to * 2 + core
        )

    for n, (keep, d_send, _, _, _) in enumerate(pieces):
        mine, theirs = halves(dot(gained, vos[:, n * part : (n + 1) * part]).reshape(NX, 2, cut, part))
        keep[:, :, :part] = mine
        d_send[:, :, :part] = theirs.astype(bf)
        if n == 0:
            mine, theirs = halves(own_sums.reshape(NX, 2, cut, rows))
            keep[:, :, part:] = mine
            d_send[:, :, part:] = in_two(theirs)
        start(across(n))
    inv_w = take(b_send, b_recv, b_ss, b_rs, total.at[1], NT * rows)
    total[1] = total[1] * inv_w
    for n, (keep, _, d_recv, r_send, _) in enumerate(pieces):
        across(n).wait_recv()
        r_send[:, :, :part] = (keep[:, :, :part] + d_recv[:, :, :part].astype(f32)).astype(bf)
        if n == 0:
            r_send[:, :, part:] = in_two(keep[:, :, part:] + joined(d_recv[:, :, part:].astype(f32)))
        for dx in (2, 1, 3):
            start(along(n, dx))
    sums = None
    for n, (_, _, _, r_send, r_recv) in enumerate(pieces):
        got = r_send[chip].astype(f32)
        for dx in (1, 3, 2):
            frm = lax.rem(chip + dx, NX)
            remote(
                r_send.at[frm], r_recv.at[frm], r_ss.at[n, dx], r_rs.at[n, frm], s, partner
            ).wait_recv()
            got = got + r_recv[frm].astype(f32)
        total[0, :, n * part : (n + 1) * part] = got[:, :part]
        if n == 0:
            sums = joined(got[:, part:])
    inv_s = lax.rsqrt(sums[:, :1] * (1.0 / (NT * rows)) + EPS)
    both = (total[0] * inv_s + total[1]).astype(bf).astype(f32)
    stats = jnp.sum(both * both, axis=1, keepdims=True) * (1.0 / feats)
    out_buf[...] = (both * lax.rsqrt(stats + EPS) * post_gain[...].reshape(1, feats)).astype(bf)

    out_copy = pltpu.make_async_copy(out_buf, out, out_sem)
    out_copy.start()
    for copy in given(b_send, b_recv, b_ss, b_rs):
        copy.wait_send()
    for copy in sends:
        copy.wait_send()
    for j in range(1, NZ):
        for e in range(2):
            @pl.when(z - j >= 0)
            def _():
                q_copy(j, e, z - j).wait_send()

            @pl.when(z + j < NZ)
            def _():
                for which in range(2):
                    to_owner(j, e, (z + j) * NY + (y_other if e else y), which).wait_send()

    @pl.when(s < N_SP - 1)
    def _():
        prev_copy(s + 1).wait_send()

    out_copy.wait()


def one_kernel(*args):
    tokens, pre_gain, wqs, wks, wvs, wqw, wkw, wvw, bias, sinks, sgain, wgain, wos, wow, post_gain = args
    bf = jnp.bfloat16
    f32 = jnp.float32
    rows, chunk = tokens.shape
    feats = NT * chunk
    cut = rows // NT
    widths = (feats // 2 + rows, feats // 2)
    v = pltpu.VMEM
    dma = pltpu.SemaphoreType.DMA
    anywhere = pl.BlockSpec(memory_space=pl.ANY)
    scratch = [
        v(pre_gain.shape, f32), pltpu.SMEM(bias.shape, f32), pltpu.SMEM(sinks.shape, f32),
        v(sgain.shape, f32), v(wgain.shape, f32), v(post_gain.shape, f32),
        v((NT, rows, chunk), bf), v((rows, rows), f32), v((rows, 4 * rows), f32), v((feats, 4 * rows), bf),
        v((rows, rows), f32), v((rows, feats), bf),
        v(wos.shape, bf), v(wow.shape, bf),
        v((NY, rows, rows), bf), v((rows, rows), bf), v((NZ, 2, rows // 2, rows), bf), v((rows // 2, rows), bf),
        v((NY // 2, NZ * rows, rows), f32), v((NY // 2, NZ * rows, rows), f32),
        v((rows, rows), bf), v((rows, rows), f32), v((rows, rows), bf),
        v((NZ, 2, rows // 2, rows), bf), v((NZ, 2, rows // 2, rows), bf),
        v((NZ, 8, rows), f32), v((NZ, 2, 8, rows), f32),
        *(v((NX, cut, width), f32) for width in widths),
        *(v((NX, cut, width), bf) for _ in range(4) for width in widths),
        v((NT, cut, feats + rows), bf), v((NT, cut, feats + rows), bf), v((2, cut, feats), f32), v((cut, feats), bf),
        dma((14,)), dma, dma((8,)), dma((NT,)), dma((NY,)), dma((NY,)), dma((NZ, 2)), dma((NZ, 2)), dma, dma,
        dma((NZ, 2)), dma((NZ, 2)), dma((NZ, 2)), dma((NZ, 2)), dma((2,)), dma((2,)), dma((2, NX)), dma((2, NX)), dma((NT,)), dma((NT,)), dma,
    ]
    return pl.pallas_call(
        kernel,
        out_shape=jax.ShapeDtypeStruct((cut, feats), bf),
        in_specs=[anywhere] * len(args),
        out_specs=anywhere,
        scratch_shapes=scratch,
        compiler_params=pltpu.CompilerParams(
            collective_id=0, has_side_effects=True, vmem_limit_bytes=67043328
        ),
        name="layer",
    )(*args[:6], wkw.T, wvw.T, *args[8:])


def solution(mesh):
    in_specs = (
        P("sp", "tp"),
        P(),
        P(None, "tp"),
        P(None, "tp"),
        P(None, "tp"),
        P(None, "tp"),
        P(None, "tp"),
        P(None, "tp"),
        P("tp"),
        P("tp"),
        P("tp"),
        P("tp"),
        P("tp", None),
        P("tp", None),
        P(),
    )
    return jax.shard_map(
        one_kernel,
        mesh=mesh,
        in_specs=in_specs,
        out_specs=P(("sp", "tp"), None),
        check_vma=False,
    )
```

```python
import functools

import jax
import jax.numpy as jnp
from jax import lax
from jax.experimental import pallas as pl
from jax.experimental.pallas import tpu as pltpu
from jax.sharding import PartitionSpec as P

HEAD_DIM = 64
WINDOW = 128
EPS = 1e-06
LOG2E = 1.4426950408889634
MESH = pl.DeviceIdType.MESH
NY = 8
NZ = 8
NT = 8
NX = 4
N_SP = NY * NZ
PLACE = (0, 1, 2, 3, 7, 6, 5, 4)


def dot(a, b):
    return jnp.dot(a, b, preferred_element_type=jnp.float32)


def dot_t(a, b):
    return lax.dot_general(a, b, (((1,), (1,)), ((), ())), preferred_element_type=jnp.float32)


def kernel(
    tokens, pre_gain_in, wqs, wks, wvs, wqw, wkw, wvw, bias_in, sinks_in, sgain_in, wgain_in, wos, wow,
    post_gain_in, out,
    pre_gain, bias, sinks, sgain, wgain, post_gain, x, sq_acc, proj, vproj, kvw_acc, vkvw, vos, vow,
    kv_all, kv_other, q_all, q_other, o_seg, t_seg, kvw, qw_buf, kvw_prev, o_send, o_recv, t_send, t_recv,
    a_keep0, a_keep1, d_send0, d_send1, d_recv0, d_recv1, r_send0, r_send1, r_recv0, r_recv1,
    b_send, b_recv, total, out_buf,
    w_sem, tok_sem, x_ss, x_rs, kv_ss, kv_rs, q_ss, q_rs, p_ss, p_rs, o_ss, o_rs, t_ss, t_rs,
    d_ss, d_rs, r_ss, r_rs, b_ss, b_rs, out_sem, ready,
):
    bf = jnp.bfloat16
    f32 = jnp.float32
    s = lax.axis_index("sp")
    t = lax.axis_index("tp")
    z = s // NY
    y = lax.rem(s, NY)
    chip = t // 2
    core = lax.rem(t, 2)
    head = lax.rem(y, 2)
    y_other = y + 1 - 2 * head
    partner = chip * 2 + 1 - core
    rows, chunk = tokens.shape
    feats = NT * chunk
    hd = HEAD_DIM
    cut = rows // NT

    barrier = pltpu.get_barrier_semaphore()

    def greet(sp, tp):
        pl.semaphore_signal(barrier, inc=1, device_id={"sp": sp, "tp": tp}, device_id_type=MESH)

    for k in range(1, NT):
        greet(s, lax.rem(t + k, NT))
    for k in range(1, NY):
        greet(z * NY + lax.rem(y + k, NY), t)
    for k in range(1, NZ):
        @pl.when(z + k < NZ)
        def _():
            greet((z + k) * NY + y, t)
            greet((z + k) * NY + y_other, t)
    starts_row = jnp.logical_and(y == 0, z > 0)
    ends_row = jnp.logical_and(y == NY - 1, z < NZ - 1)

    @pl.when(ends_row)
    def _():
        greet(s + 1, t)

    half = rows // 2
    loads = [
        pltpu.make_async_copy(src, dst, w_sem.at[n])
        for n, (src, dst) in enumerate(
            [(wks, vproj.at[:, :rows]), (wvs, vproj.at[:, rows : 2 * rows]), (wqs, vproj.at[:, 2 * rows : 3 * rows]),
             (wqw, vproj.at[:, 3 * rows :]), (wkw, vkvw.at[:half]), (wvw, vkvw.at[half:]),
             (wow, vow), (wos, vos),
             (bias_in, bias), (pre_gain_in, pre_gain), (sinks_in, sinks), (sgain_in, sgain),
             (wgain_in, wgain), (post_gain_in, post_gain)]
        )
    ]
    l_proj = loads[:6]
    l_ow, l_os, *l_small = loads[6:]
    tok_load = pltpu.make_async_copy(tokens, x.at[t], tok_sem)
    tok_load.start()
    for load in l_small + loads[:8]:
        load.start()

    for j in range(1, NZ):
        @pl.when(z + j >= NZ)
        def _():
            q_all[PLACE[j]] = jnp.zeros((2, half, rows), bf)

        @pl.when(z - j < 0)
        def _():
            o_recv[j] = jnp.zeros((2, half, rows), bf)
            t_recv[j] = jnp.zeros((2, 8, rows), f32)

    for load in l_small:
        load.wait()
    tok_load.wait()
    pl.semaphore_wait(barrier, NT - 1 + NY - 1 + 2 * z + starts_row.astype(jnp.int32))

    @pl.when(starts_row)
    def _():
        pl.semaphore_signal(ready, inc=1, device_id={"sp": s - 1, "tp": t}, device_id_type=MESH)

    def remote(src, dst, ss, rs, sp, tp):
        return pltpu.make_async_remote_copy(
            src_ref=src, dst_ref=dst, send_sem=ss, recv_sem=rs,
            device_id={"sp": sp, "tp": tp}, device_id_type=MESH,
        )

    sends = []

    def x_copy(slot, sem, tp):
        return remote(x.at[slot], x.at[slot], x_ss.at[sem], x_rs.at[slot], s, tp)

    def start(copy):
        copy.start()
        sends.append(copy)

    for dx in (2, 1, 3):
        start(x_copy(t, dx, lax.rem(chip + dx, NX) * 2 + core))
    start(x_copy(t, 0, partner))

    def absorb(*slots, first=False):
        sums = None
        for slot in slots:
            v = x[slot].astype(f32)
            part = pl.ds(pl.multiple_of(slot * chunk, chunk), chunk)
            gained = (v * pre_gain[part].reshape(1, chunk)).astype(bf)
            v = v * v
            more = (
                v[:, : chunk // 2] + v[:, chunk // 2 :], dot(gained, vproj[part, :]), dot_t(gained, vkvw[:, part])
            )
            sums = more if sums is None else tuple(p + q for p, q in zip(sums, more))
        for ref, more in zip((sq_acc, proj, kvw_acc), sums):
            ref[...] = more if first else ref[...] + more

    def block(dx, relayed):
        slot = lax.rem(chip + NX - dx, NX) * 2 + (1 - core if relayed else core)
        x_copy(slot, dx, partner).wait_recv()
        if not relayed:
            start(x_copy(slot, NX + dx, partner))
        return slot

    for load in l_proj:
        load.wait()
    absorb(t, block(0, 1), first=True)
    absorb(*[block(dx, 0) for dx in (1, 3, 2)])
    absorb(*[block(dx, 1) for dx in (1, 3, 2)])
    inv = lax.rsqrt(jnp.sum(sq_acc[...], axis=1, keepdims=True) * (1.0 / feats) + EPS)

    left = lax.broadcasted_iota(jnp.int32, (rows, rows), 1) < hd
    left_half = left[:half]

    keys, values = proj[:, :rows] * inv, proj[:, rows : 2 * rows] * inv
    head0 = jnp.where(left, keys, pltpu.roll(values, hd, 1))
    head1 = jnp.where(left, pltpu.roll(keys, hd, 1), values)
    kv_all[y] = jnp.where(head == 0, head0, head1).astype(bf)
    kv_other[...] = jnp.where(head == 0, head1, head0).astype(bf)

    def kv_copy(src, slot, sem, to_y):
        return remote(src, kv_all.at[slot], kv_ss.at[sem], kv_rs.at[slot], z * NY + to_y, t)

    def kv_send(k):
        start(kv_copy(kv_other if k % 2 else kv_all.at[y], y, k, lax.rem(y + k, NY)))

    for k in (1, 7):
        kv_send(k)

    qs = proj[:, 2 * rows : 3 * rows] * inv
    q0 = jnp.where(left_half, qs[:half], pltpu.roll(qs[half:], hd, 1))
    q1 = jnp.where(left_half, pltpu.roll(qs[:half], hd, 1), qs[half:])
    q_all[0, 0] = jnp.where(head == 0, q0, q1).astype(bf)
    q_other[...] = jnp.where(head == 0, q1, q0).astype(bf)

    def q_copy(j, e, to_z):
        src = q_other if e else q_all.at[0, 0]
        return remote(
            src, q_all.at[PLACE[j], e], q_ss.at[j, e], q_rs.at[j, e], to_z * NY + (y_other if e else y), t
        )

    start(q_copy(0, 1, z))
    for j in (1, 7, 2, 6, 3, 5, 4):
        @pl.when(z - j >= 0)
        def _():
            q_copy(j, 0, z - j).start()
            q_copy(j, 1, z - j).start()

    kvw[...] = (kvw_acc[...] * inv).astype(bf)

    def prev_copy(to):
        return remote(kvw, kvw_prev, p_ss, p_rs, to, t)

    @pl.when(y < NY - 1)
    def _():
        prev_copy(s + 1).start()

    for k in (2, 6, 3, 5, 4):
        kv_send(k)

    @pl.when(ends_row)
    def _():
        pl.semaphore_wait(ready, 1)
        prev_copy(s + 1).start()

    @pl.when(s == 0)
    def _():
        kvw_prev[...] = jnp.zeros_like(kvw_prev)

    qw_buf[...] = proj[:, 3 * rows :] * inv

    def given(send, recv, ss, rs):
        for dx, dc in ((2, 0), (2, 1), (1, 0), (1, 1), (3, 0), (3, 1), (0, 1)):
            to = lax.rem(chip + dx, NX) * 2 + lax.rem(core + dc, 2)
            yield remote(send.at[to], recv.at[t], ss.at[2 * dx + dc], rs.at[t], s, to)

    def give(send, recv, ss, rs, values, weights):
        sums = jnp.sum(values * values, axis=1, keepdims=True)
        high = sums.astype(bf)
        low = (sums - high.astype(f32)).astype(bf)
        send[:, :, feats:] = jnp.where(left, high.astype(f32), low.astype(f32)).astype(bf).reshape(NT, cut, rows)
        gained, w = weights
        n_cut = 4
        part = feats // n_cut
        for n in range(n_cut):
            cols = slice(n * part, (n + 1) * part)
            send[:, :, cols] = dot(gained, w[:, cols]).astype(bf).reshape(NT, cut, part)
        for copy in given(send, recv, ss, rs):
            copy.start()

    def take(send, recv, ss, rs, acc, width):
        own = send[t].astype(f32)
        acc[...] = own[:, :feats]
        sums = own[:, feats:]
        for dx, dc in ((0, 1), (1, 0), (1, 1), (3, 0), (3, 1), (2, 0), (2, 1)):
            frm = lax.rem(chip + dx, NX) * 2 + lax.rem(core + dc, 2)
            remote(send.at[frm], recv.at[frm], ss.at[2 * dx + dc], rs.at[frm], s, partner).wait_recv()
            got = recv[frm].astype(f32)
            acc[...] += got[:, :feats]
            sums += got[:, feats:]
        return lax.rsqrt((sums[:, :1] + sums[:, hd : hd + 1]) * (1.0 / width) + EPS)

    def windowed():
        @pl.when(s > 0)
        def _():
            prev_copy(s - 1).wait_recv()

        two = 2 * rows
        r_iota = lax.broadcasted_iota(jnp.int32, (two, two), 0)
        c_iota = lax.broadcasted_iota(jnp.int32, (two, two), 1)
        dist = lax.rem(r_iota, rows) + rows - c_iota
        in_window = (dist >= 0) & (dist < WINDOW) & ((c_iota >= rows) | (s > 0))
        first_rows = lax.broadcasted_iota(jnp.int32, (two, 1), 0) < rows
        qw = qw_buf[...]
        kk = jnp.concatenate([kvw_prev[...], kvw[...]], axis=0)
        qq = jnp.concatenate([jnp.where(left, qw, 0.0), jnp.where(left, pltpu.roll(qw, hd, 1), 0.0)], axis=0).astype(bf)
        logits = jnp.where(in_window, dot_t(qq, kk) * hd**-0.5, -jnp.inf)
        sink = jnp.where(first_rows, sinks[0], sinks[1])
        top = jnp.maximum(jnp.max(logits, axis=1, keepdims=True), sink)
        grown = jnp.exp(logits - top)
        norm = jnp.sum(grown, axis=1, keepdims=True) + jnp.exp(sink - top)
        res = dot((grown / norm).astype(bf), kk)
        w_out = jnp.where(left, pltpu.roll(res[:rows], hd, 1), res[rows:]).astype(bf).astype(f32)

        l_ow.wait()
        give(b_send, b_recv, b_ss, b_rs, w_out, ((w_out * wgain[...].reshape(1, rows)).astype(bf), vow))

    def q_wait(j, e):
        frm = lax.rem(z + j, NZ) * NY + (y_other if e else y)
        remote(q_other, q_all.at[PLACE[j], e], q_ss.at[j, e], q_rs.at[j, e], frm, t).wait_recv()

    def q_waits(js):
        for j in js:
            @pl.when(z + j < NZ)
            def _():
                if j:
                    q_wait(j, 0)
                q_wait(j, 1)

    kt = 2 * rows
    mb = 2 * rows
    per = mb // rows
    later = (
        lax.broadcasted_iota(jnp.int32, (kt, kt), 0) > lax.broadcasted_iota(jnp.int32, (kt, kt), 1)
    ).astype(bf)
    row2 = lax.broadcasted_iota(jnp.int32, (mb, kt), 0)
    lane2 = lax.broadcasted_iota(jnp.int32, (mb, kt), 1)
    place = lax.rem(row2, half) + jnp.where(row2 < half, y, y_other) * rows
    left2 = lax.broadcasted_iota(jnp.int32, (mb, rows), 1) < hd
    scale = LOG2E * hd**-0.5
    head_bias = bias[head] * LOG2E

    def segment(pairs):
        weights_of = {}
        chains = []
        for m, k in pairs:
            if k not in weights_of:
                weights_of[k] = keys_of(tiles[k])
            queries = q_all[m * per : (m + 1) * per].reshape(mb, rows).astype(f32)
            for u in range(2):
                qh = jnp.where(jnp.logical_not(left2) if u else left2, queries, 0.0).astype(bf)
                chains.append((m, k, u, qh))

        def by_weights(values, flip):
            res = [None] * len(chains)
            for k in weights_of:
                for u in range(2):
                    own = [n for n, c in enumerate(chains) if c[1] == k and c[2] == u]
                    joint = jnp.concatenate([values[n] for n in own], axis=0)
                    w = weights_of[k][1 - u if flip else u]
                    got = dot(joint, w) if flip else dot_t(joint, w)
                    for at, n in enumerate(own):
                        res[n] = got[at * mb : (at + 1) * mb]
            return res

        drops = []
        holds = []
        for (m, k, u, _), raw in zip(chains, by_weights([c[3] for c in chains], False)):
            score = raw * scale + head_bias
            pos = jnp.maximum(score, 0.0)
            neg = score - pos
            soft = jnp.log2(1.0 + jnp.exp2(neg - pos))
            drop = pos + soft
            hold = neg - soft
            if m == 0:
                usable = (row2 >= rows) | (lane2 + tiles[k] * kt < place + u * half)
                drop = jnp.where(usable, drop, 0.0)
                hold = jnp.where(usable, hold, -jnp.inf)
            drops.append(drop)
            holds.append(hold)
        suffix = dot(jnp.concatenate([d.astype(bf) for d in drops], axis=0), later)
        suffix = [suffix[n * mb : (n + 1) * mb] for n in range(len(chains))]
        outs = by_weights([jnp.exp2(h - f).astype(bf) for h, f in zip(holds, suffix)], True)
        sums = [f[:, :1] + d[:, :1] for f, d in zip(suffix, drops)]
        for n in range(0, len(chains), 2):
            m, k, _, _ = chains[n]
            part = slice(m * mb, (m + 1) * mb)
            o_seg[tiles[k], part] = jnp.where(left2, outs[n], outs[n + 1])
            t_seg[tiles[k], part] = jnp.where(left2, sums[n], sums[n + 1])

    def keys_of(tile):
        straight = kv_all[pl.ds(2 * tile, 2)].reshape(kt, rows)
        return straight, pltpu.roll(straight.astype(f32), hd, 1).astype(bf)

    near = y // 2
    side = 2 * head - 1
    tiles = [lax.rem(near + k * side + NY // 2, NY // 2) for k in (0, 1, -1, 2)]

    def kv_waits(k):
        for u in range(2):
            src = 2 * tiles[k] + u

            @pl.when(src != y)
            def _():
                kv_copy(kv_other, src, 0, lax.rem(y + 1, NY)).wait_recv()

    def to_owner(j, e, sp, which):
        if which:
            return remote(o_send.at[j, e], o_recv.at[j, e], o_ss.at[j, e], o_rs.at[j, e], sp, t)
        return remote(t_send.at[j], t_recv.at[j, e], t_ss.at[j, e], t_rs.at[j, e], sp, t)

    first = lax.broadcasted_iota(jnp.int32, (8, rows), 0) < 4

    def finish(j):
        part = slice(PLACE[j] * rows, (PLACE[j] + 1) * rows)
        last = NY // 2 - 1
        acc = o_seg[last, part]
        carry = t_seg[last, part]
        for n in range(last - 1, -1, -1):
            acc = acc + jnp.exp2(-carry) * o_seg[n, part]
            carry = carry + t_seg[n, part]
        over = carry.T
        compact = jnp.where(first, over[0:8], over[hd : hd + 8])
        o_send[j] = acc.astype(bf).reshape(2, half, rows)
        t_send[j] = compact
        if j == 0:
            for which in range(2):
                start(to_owner(0, 1, z * NY + y_other, which))
        else:
            @pl.when(z + j < NZ)
            def _():
                for e in range(2):
                    for which in range(2):
                        to_owner(j, e, (z + j) * NY + (y_other if e else y), which).start()
        return acc[:half], compact

    def segments(*pairs):
        segment(pairs)

    q_waits((0, 1))
    kv_waits(0)
    segments((0, 0))
    windowed()
    kv_waits(1)
    q_waits((2, 3))
    segments((0, 1), (1, 1))
    segments((1, 0))
    kv_waits(2)
    segments((0, 2), (1, 2))
    kv_waits(3)
    segments((0, 3), (1, 3))
    own_o, own_t = finish(0)
    for j in (3, 2, 1):
        finish(j)
    q_waits((7, 6))
    segments((2, 0), (2, 1))
    segments((2, 2), (2, 3))
    for j in (6, 7):
        finish(j)
    q_waits((5, 4))
    segments((3, 0), (3, 1))
    segments((3, 2), (3, 3))
    for j in (4, 5):
        finish(j)

    def from_owner(j, e, which):
        frm = lax.rem(z + NZ - j, NZ) * NY + (y_other if e else y)
        to_owner(j, e, frm, which).wait_recv()

    def arrivals(which):
        from_owner(0, 1, which)
        for j in range(1, NZ):
            @pl.when(z - j >= 0)
            def _():
                from_owner(j, 0, which)
                from_owner(j, 1, which)

    arrivals(0)
    left8 = left[:8]
    carry = jnp.where(left8, own_t, t_recv[0, 1])
    scales = []
    for j in range(1, NZ):
        scales.append(jnp.exp2(-carry))
        carry = carry + jnp.where(left8, t_recv[j, 0], t_recv[j, 1])
    scales = jnp.concatenate(scales + [jnp.zeros((rows - 8 * (NZ - 1), rows), f32)], axis=0).T
    arrivals(1)
    acc = jnp.concatenate([own_o, o_recv[0, 1].astype(f32)], axis=0)
    for j in range(1, NZ):
        at = 8 * (j - 1)
        here = o_recv[j].reshape(rows, rows).astype(f32)
        acc = acc + jnp.where(left, scales[:, at : at + 1], scales[:, at + 4 : at + 5]) * here
    head0 = jnp.where(head == 0, acc[:half], acc[half:])
    head1 = jnp.where(head == 0, acc[half:], acc[:half])
    s_out = jnp.concatenate(
        [
            jnp.where(left_half, head0, pltpu.roll(head1, hd, 1)),
            jnp.where(left_half, pltpu.roll(head0, hd, 1), head1),
        ],
        axis=0,
    ).astype(bf).astype(f32)
    l_os.wait()
    gained = (s_out * sgain[...].reshape(1, rows)).astype(bf)
    own_sums = jnp.broadcast_to(jnp.sum(s_out * s_out, axis=1, keepdims=True), (rows, rows))
    part = feats // 2
    pieces = ((a_keep0, d_send0, d_recv0, r_send0, r_recv0), (a_keep1, d_send1, d_recv1, r_send1, r_recv1))
    left_cut = left[:cut].reshape(1, cut, rows)

    def halves(values):
        return jnp.where(core == 0, values[:, 0], values[:, 1]), jnp.where(core == 0, values[:, 1], values[:, 0])

    def in_two(values):
        high = values.astype(bf).astype(f32)
        return jnp.where(left_cut, high, values - high).astype(bf)

    def joined(values):
        return values + pltpu.roll(values, hd, values.ndim - 1)

    def across(n):
        return remote(pieces[n][1], pieces[n][2], d_ss.at[n], d_rs.at[n], s, partner)

    def along(n, dx):
        to = lax.rem(chip + dx, NX)
        return remote(
            pieces[n][3].at[to], pieces[n][4].at[chip], r_ss.at[n, dx], r_rs.at[n, chip], s, to * 2 + core
        )

    for n, (keep, d_send, _, _, _) in enumerate(pieces):
        mine, theirs = halves(dot(gained, vos[:, n * part : (n + 1) * part]).reshape(NX, 2, cut, part))
        keep[:, :, :part] = mine
        d_send[:, :, :part] = theirs.astype(bf)
        if n == 0:
            mine, theirs = halves(own_sums.reshape(NX, 2, cut, rows))
            keep[:, :, part:] = mine
            d_send[:, :, part:] = in_two(theirs)
        start(across(n))
    inv_w = take(b_send, b_recv, b_ss, b_rs, total.at[1], NT * rows)
    total[1] = total[1] * inv_w
    for n, (keep, _, d_recv, r_send, _) in enumerate(pieces):
        across(n).wait_recv()
        r_send[:, :, :part] = (keep[:, :, :part] + d_recv[:, :, :part].astype(f32)).astype(bf)
        if n == 0:
            r_send[:, :, part:] = in_two(keep[:, :, part:] + joined(d_recv[:, :, part:].astype(f32)))
        for dx in (2, 1, 3):
            start(along(n, dx))
    sums = None
    for n, (_, _, _, r_send, r_recv) in enumerate(pieces):
        got = r_send[chip].astype(f32)
        for dx in (1, 3, 2):
            frm = lax.rem(chip + dx, NX)
            remote(
                r_send.at[frm], r_recv.at[frm], r_ss.at[n, dx], r_rs.at[n, frm], s, partner
            ).wait_recv()
            got = got + r_recv[frm].astype(f32)
        total[0, :, n * part : (n + 1) * part] = got[:, :part]
        if n == 0:
            sums = joined(got[:, part:])
    inv_s = lax.rsqrt(sums[:, :1] * (1.0 / (NT * rows)) + EPS)
    both = (total[0] * inv_s + total[1]).astype(bf).astype(f32)
    stats = jnp.sum(both * both, axis=1, keepdims=True) * (1.0 / feats)
    out_buf[...] = (both * lax.rsqrt(stats + EPS) * post_gain[...].reshape(1, feats)).astype(bf)

    out_copy = pltpu.make_async_copy(out_buf, out, out_sem)
    out_copy.start()
    for copy in given(b_send, b_recv, b_ss, b_rs):
        copy.wait_send()
    for copy in sends:
        copy.wait_send()
    for j in range(1, NZ):
        for e in range(2):
            @pl.when(z - j >= 0)
            def _():
                q_copy(j, e, z - j).wait_send()

            @pl.when(z + j < NZ)
            def _():
                for which in range(2):
                    to_owner(j, e, (z + j) * NY + (y_other if e else y), which).wait_send()

    @pl.when(s < N_SP - 1)
    def _():
        prev_copy(s + 1).wait_send()

    out_copy.wait()


def one_kernel(*args):
    tokens, pre_gain, wqs, wks, wvs, wqw, wkw, wvw, bias, sinks, sgain, wgain, wos, wow, post_gain = args
    bf = jnp.bfloat16
    f32 = jnp.float32
    rows, chunk = tokens.shape
    feats = NT * chunk
    cut = rows // NT
    widths = (feats // 2 + rows, feats // 2)
    v = pltpu.VMEM
    dma = pltpu.SemaphoreType.DMA
    anywhere = pl.BlockSpec(memory_space=pl.ANY)
    scratch = [
        v(pre_gain.shape, f32), pltpu.SMEM(bias.shape, f32), pltpu.SMEM(sinks.shape, f32),
        v(sgain.shape, f32), v(wgain.shape, f32), v(post_gain.shape, f32),
        v((NT, rows, chunk), bf), v((rows, rows), f32), v((rows, 4 * rows), f32), v((feats, 4 * rows), bf),
        v((rows, rows), f32), v((rows, feats), bf),
        v(wos.shape, bf), v(wow.shape, bf),
        v((NY, rows, rows), bf), v((rows, rows), bf), v((NZ, 2, rows // 2, rows), bf), v((rows // 2, rows), bf),
        v((NY // 2, NZ * rows, rows), f32), v((NY // 2, NZ * rows, rows), f32),
        v((rows, rows), bf), v((rows, rows), f32), v((rows, rows), bf),
        v((NZ, 2, rows // 2, rows), bf), v((NZ, 2, rows // 2, rows), bf),
        v((NZ, 8, rows), f32), v((NZ, 2, 8, rows), f32),
        *(v((NX, cut, width), f32) for width in widths),
        *(v((NX, cut, width), bf) for _ in range(4) for width in widths),
        v((NT, cut, feats + rows), bf), v((NT, cut, feats + rows), bf), v((2, cut, feats), f32), v((cut, feats), bf),
        dma((14,)), dma, dma((8,)), dma((NT,)), dma((NY,)), dma((NY,)), dma((NZ, 2)), dma((NZ, 2)), dma, dma,
        dma((NZ, 2)), dma((NZ, 2)), dma((NZ, 2)), dma((NZ, 2)), dma((2,)), dma((2,)), dma((2, NX)), dma((2, NX)), dma((NT,)), dma((NT,)), dma,
        pltpu.SemaphoreType.REGULAR,
    ]
    return pl.pallas_call(
        kernel,
        out_shape=jax.ShapeDtypeStruct((cut, feats), bf),
        in_specs=[anywhere] * len(args),
        out_specs=anywhere,
        scratch_shapes=scratch,
        compiler_params=pltpu.CompilerParams(
            collective_id=0, has_side_effects=True, vmem_limit_bytes=67043328
        ),
        name="layer",
    )(*args[:6], wkw.T, wvw.T, *args[8:])


def solution(mesh):
    in_specs = (
        P("sp", "tp"),
        P(),
        P(None, "tp"),
        P(None, "tp"),
        P(None, "tp"),
        P(None, "tp"),
        P(None, "tp"),
        P(None, "tp"),
        P("tp"),
        P("tp"),
        P("tp"),
        P("tp"),
        P("tp", None),
        P("tp", None),
        P(),
    )
    return jax.shard_map(
        one_kernel,
        mesh=mesh,
        in_specs=in_specs,
        out_specs=P(("sp", "tp"), None),
        check_vma=False,
    )
```

```python
import functools

import jax
import jax.numpy as jnp
from jax import lax
from jax.experimental import pallas as pl
from jax.experimental.pallas import tpu as pltpu
from jax.sharding import PartitionSpec as P

HEAD_DIM = 64
WINDOW = 128
EPS = 1e-06
LOG2E = 1.4426950408889634
MESH = pl.DeviceIdType.MESH
NY = 8
NZ = 8
NT = 8
NX = 4
N_SP = NY * NZ
PLACE = (0, 1, 2, 3, 7, 6, 5, 4)


def dot(a, b):
    return jnp.dot(a, b, preferred_element_type=jnp.float32)


def dot_t(a, b):
    return lax.dot_general(a, b, (((1,), (1,)), ((), ())), preferred_element_type=jnp.float32)


def kernel(
    tokens, pre_gain_in, wqs, wks, wvs, wqw, wkw, wvw, bias_in, sinks_in, sgain_in, wgain_in, wos, wow,
    post_gain_in, out,
    pre_gain, bias, sinks, sgain, wgain, post_gain, x, sq_acc, proj, vproj, kvw_acc, vkvw, vos, vow,
    kv_all, kv_other, q_all, q_other, o_seg, t_seg, kvw, qw_buf, kvw_prev, o_send, o_recv, t_send, t_recv,
    a_keep0, a_keep1, d_send0, d_send1, d_recv0, d_recv1, r_send0, r_send1, r_recv0, r_recv1,
    b_send, b_recv, total, out_buf,
    w_sem, tok_sem, x_ss, x_rs, kv_ss, kv_rs, q_ss, q_rs, p_ss, p_rs, o_ss, o_rs, t_ss, t_rs,
    d_ss, d_rs, r_ss, r_rs, b_ss, b_rs, out_sem, ready,
):
    bf = jnp.bfloat16
    f32 = jnp.float32
    s = lax.axis_index("sp")
    t = lax.axis_index("tp")
    z = s // NY
    y = lax.rem(s, NY)
    chip = t // 2
    core = lax.rem(t, 2)
    head = lax.rem(y, 2)
    y_other = y + 1 - 2 * head
    partner = chip * 2 + 1 - core
    rows, chunk = tokens.shape
    feats = NT * chunk
    hd = HEAD_DIM
    cut = rows // NT

    barrier = pltpu.get_barrier_semaphore()

    def greet(sp, tp):
        pl.semaphore_signal(barrier, inc=1, device_id={"sp": sp, "tp": tp}, device_id_type=MESH)

    for k in range(1, NT):
        greet(s, lax.rem(t + k, NT))
    for k in range(1, NY):
        greet(z * NY + lax.rem(y + k, NY), t)
    for k in range(1, NZ):
        @pl.when(z + k < NZ)
        def _():
            greet((z + k) * NY + y, t)
            greet((z + k) * NY + y_other, t)
    starts_row = jnp.logical_and(y == 0, z > 0)
    ends_row = jnp.logical_and(y == NY - 1, z < NZ - 1)

    @pl.when(ends_row)
    def _():
        greet(s + 1, t)

    half = rows // 2
    loads = [
        pltpu.make_async_copy(src, dst, w_sem.at[n])
        for n, (src, dst) in enumerate(
            [(wks, vproj.at[:, :rows]), (wvs, vproj.at[:, rows : 2 * rows]), (wqs, vproj.at[:, 2 * rows : 3 * rows]),
             (wqw, vproj.at[:, 3 * rows :]), (wkw, vkvw.at[:half]), (wvw, vkvw.at[half:]),
             (wow, vow), (wos, vos),
             (bias_in, bias), (pre_gain_in, pre_gain), (sinks_in, sinks), (sgain_in, sgain),
             (wgain_in, wgain), (post_gain_in, post_gain)]
        )
    ]
    l_proj = loads[:6]
    l_ow, l_os, *l_small = loads[6:]
    tok_load = pltpu.make_async_copy(tokens, x.at[t], tok_sem)
    tok_load.start()
    for load in l_small + loads[:8]:
        load.start()

    for j in range(1, NZ):
        @pl.when(z + j >= NZ)
        def _():
            q_all[PLACE[j]] = jnp.zeros((2, half, rows), bf)

        @pl.when(z - j < 0)
        def _():
            o_recv[j] = jnp.zeros((2, half, rows), bf)
            t_recv[j] = jnp.zeros((2, 8, rows), f32)

    for load in l_small:
        load.wait()
    tok_load.wait()
    pl.semaphore_wait(barrier, NT - 1 + NY - 1 + 2 * z + starts_row.astype(jnp.int32))

    @pl.when(starts_row)
    def _():
        pl.semaphore_signal(ready, inc=1, device_id={"sp": s - 1, "tp": t}, device_id_type=MESH)

    def remote(src, dst, ss, rs, sp, tp):
        return pltpu.make_async_remote_copy(
            src_ref=src, dst_ref=dst, send_sem=ss, recv_sem=rs,
            device_id={"sp": sp, "tp": tp}, device_id_type=MESH,
        )

    sends = []

    def x_copy(slot, sem, tp):
        return remote(x.at[slot], x.at[slot], x_ss.at[sem], x_rs.at[slot], s, tp)

    def start(copy):
        copy.start()
        sends.append(copy)

    for dx in (2, 1, 3):
        start(x_copy(t, dx, lax.rem(chip + dx, NX) * 2 + core))
    start(x_copy(t, 0, partner))

    def absorb(*slots, first=False):
        sums = None
        for slot in slots:
            v = x[slot].astype(f32)
            part = pl.ds(pl.multiple_of(slot * chunk, chunk), chunk)
            gained = (v * pre_gain[part].reshape(1, chunk)).astype(bf)
            v = v * v
            more = (
                v[:, : chunk // 2] + v[:, chunk // 2 :], dot(gained, vproj[part, :]), dot_t(gained, vkvw[:, part])
            )
            sums = more if sums is None else tuple(p + q for p, q in zip(sums, more))
        for ref, more in zip((sq_acc, proj, kvw_acc), sums):
            ref[...] = more if first else ref[...] + more

    def block(dx, relayed):
        slot = lax.rem(chip + NX - dx, NX) * 2 + (1 - core if relayed else core)
        x_copy(slot, dx, partner).wait_recv()
        if not relayed:
            start(x_copy(slot, NX + dx, partner))
        return slot

    for load in l_proj:
        load.wait()
    absorb(t, block(0, 1), first=True)
    absorb(*[block(dx, 0) for dx in (1, 3, 2)])
    absorb(*[block(dx, 1) for dx in (1, 3, 2)])
    inv = lax.rsqrt(jnp.sum(sq_acc[...], axis=1, keepdims=True) * (1.0 / feats) + EPS)

    left = lax.broadcasted_iota(jnp.int32, (rows, rows), 1) < hd
    left_half = left[:half]

    keys, values = proj[:, :rows] * inv, proj[:, rows : 2 * rows] * inv
    head0 = jnp.where(left, keys, pltpu.roll(values, hd, 1))
    head1 = jnp.where(left, pltpu.roll(keys, hd, 1), values)
    kv_all[y] = jnp.where(head == 0, head0, head1).astype(bf)
    kv_other[...] = jnp.where(head == 0, head1, head0).astype(bf)

    def kv_copy(src, slot, sem, to_y):
        return remote(src, kv_all.at[slot], kv_ss.at[sem], kv_rs.at[slot], z * NY + to_y, t)

    def kv_send(k):
        start(kv_copy(kv_other if k % 2 else kv_all.at[y], y, k, lax.rem(y + k, NY)))

    qs = proj[:, 2 * rows : 3 * rows] * inv
    q0 = jnp.where(left_half, qs[:half], pltpu.roll(qs[half:], hd, 1))
    q1 = jnp.where(left_half, pltpu.roll(qs[:half], hd, 1), qs[half:])
    q_all[0, 0] = jnp.where(head == 0, q0, q1).astype(bf)
    q_other[...] = jnp.where(head == 0, q1, q0).astype(bf)

    def q_copy(j, e, to_z):
        src = q_all.at[0, e] if j > 1 or e == 0 else q_other
        to_y = y_other if e and j < 2 else y
        return remote(src, q_all.at[PLACE[j], e], q_ss.at[j, e], q_rs.at[j, e], to_z * NY + to_y, t)

    def q_send(e, *js):
        for j in js:
            @pl.when(z - j >= 0)
            def _():
                q_copy(j, e, z - j).start()

    start(q_copy(0, 1, z))
    q_send(0, 1)
    q_send(1, 1)
    for k in (1, 7):
        kv_send(k)
    q_send(0, 4, 5, 3)
    kv_send(4)
    q_send(0, 2, 6, 7)

    kvw[...] = (kvw_acc[...] * inv).astype(bf)

    def prev_copy(to):
        return remote(kvw, kvw_prev, p_ss, p_rs, to, t)

    @pl.when(y < NY - 1)
    def _():
        prev_copy(s + 1).start()

    for k in (3, 5, 2, 6):
        kv_send(k)

    @pl.when(ends_row)
    def _():
        pl.semaphore_wait(ready, 1)
        prev_copy(s + 1).start()

    @pl.when(s == 0)
    def _():
        kvw_prev[...] = jnp.zeros_like(kvw_prev)

    qw_buf[...] = proj[:, 3 * rows :] * inv

    def given(send, recv, ss, rs):
        for dx, dc in ((2, 0), (2, 1), (1, 0), (1, 1), (3, 0), (3, 1), (0, 1)):
            to = lax.rem(chip + dx, NX) * 2 + lax.rem(core + dc, 2)
            yield remote(send.at[to], recv.at[t], ss.at[2 * dx + dc], rs.at[t], s, to)

    def give(send, recv, ss, rs, values, weights):
        sums = jnp.sum(values * values, axis=1, keepdims=True)
        high = sums.astype(bf)
        low = (sums - high.astype(f32)).astype(bf)
        send[:, :, feats:] = jnp.where(left, high.astype(f32), low.astype(f32)).astype(bf).reshape(NT, cut, rows)
        gained, w = weights
        n_cut = 4
        part = feats // n_cut
        for n in range(n_cut):
            cols = slice(n * part, (n + 1) * part)
            send[:, :, cols] = dot(gained, w[:, cols]).astype(bf).reshape(NT, cut, part)
        for copy in given(send, recv, ss, rs):
            copy.start()

    def take(send, recv, ss, rs, acc, width):
        own = send[t].astype(f32)
        acc[...] = own[:, :feats]
        sums = own[:, feats:]
        for dx, dc in ((0, 1), (1, 0), (1, 1), (3, 0), (3, 1), (2, 0), (2, 1)):
            frm = lax.rem(chip + dx, NX) * 2 + lax.rem(core + dc, 2)
            remote(send.at[frm], recv.at[frm], ss.at[2 * dx + dc], rs.at[frm], s, partner).wait_recv()
            got = recv[frm].astype(f32)
            acc[...] += got[:, :feats]
            sums += got[:, feats:]
        return lax.rsqrt((sums[:, :1] + sums[:, hd : hd + 1]) * (1.0 / width) + EPS)

    def windowed():
        @pl.when(s > 0)
        def _():
            prev_copy(s - 1).wait_recv()

        two = 2 * rows
        r_iota = lax.broadcasted_iota(jnp.int32, (two, two), 0)
        c_iota = lax.broadcasted_iota(jnp.int32, (two, two), 1)
        dist = lax.rem(r_iota, rows) + rows - c_iota
        in_window = (dist >= 0) & (dist < WINDOW) & ((c_iota >= rows) | (s > 0))
        first_rows = lax.broadcasted_iota(jnp.int32, (two, 1), 0) < rows
        qw = qw_buf[...]
        kk = jnp.concatenate([kvw_prev[...], kvw[...]], axis=0)
        qq = jnp.concatenate([jnp.where(left, qw, 0.0), jnp.where(left, pltpu.roll(qw, hd, 1), 0.0)], axis=0).astype(bf)
        logits = jnp.where(in_window, dot_t(qq, kk) * hd**-0.5, -jnp.inf)
        sink = jnp.where(first_rows, sinks[0], sinks[1])
        top = jnp.maximum(jnp.max(logits, axis=1, keepdims=True), sink)
        grown = jnp.exp(logits - top)
        norm = jnp.sum(grown, axis=1, keepdims=True) + jnp.exp(sink - top)
        res = dot((grown / norm).astype(bf), kk)
        w_out = jnp.where(left, pltpu.roll(res[:rows], hd, 1), res[rows:]).astype(bf).astype(f32)

        l_ow.wait()
        give(b_send, b_recv, b_ss, b_rs, w_out, ((w_out * wgain[...].reshape(1, rows)).astype(bf), vow))

    def q_wait(j, e):
        frm = lax.rem(z + j, NZ) * NY + (y_other if e else y)
        remote(q_other, q_all.at[PLACE[j], e], q_ss.at[j, e], q_rs.at[j, e], frm, t).wait_recv()

    def q_waits(js):
        for j in js:
            @pl.when(z + j < NZ)
            def _():
                q_wait(j, 0)
                q_wait(j, 1)

    kt = 2 * rows
    mb = 2 * rows
    per = mb // rows
    later = (
        lax.broadcasted_iota(jnp.int32, (kt, kt), 0) > lax.broadcasted_iota(jnp.int32, (kt, kt), 1)
    ).astype(bf)
    row2 = lax.broadcasted_iota(jnp.int32, (mb, kt), 0)
    lane2 = lax.broadcasted_iota(jnp.int32, (mb, kt), 1)
    place = lax.rem(row2, half) + jnp.where(row2 < half, y, y_other) * rows
    left2 = lax.broadcasted_iota(jnp.int32, (mb, rows), 1) < hd
    scale = LOG2E * hd**-0.5
    head_bias = bias[head] * LOG2E

    def segment(pairs):
        weights_of = {}
        chains = []
        for m, k in pairs:
            if k not in weights_of:
                weights_of[k] = keys_of(tiles[k])
            queries = q_all[m * per : (m + 1) * per].reshape(mb, rows).astype(f32)
            for u in range(2):
                qh = jnp.where(jnp.logical_not(left2) if u else left2, queries, 0.0).astype(bf)
                chains.append((m, k, u, qh))

        def by_weights(values, flip):
            res = [None] * len(chains)
            for k in weights_of:
                for u in range(2):
                    own = [n for n, c in enumerate(chains) if c[1] == k and c[2] == u]
                    joint = jnp.concatenate([values[n] for n in own], axis=0)
                    w = weights_of[k][1 - u if flip else u]
                    got = dot(joint, w) if flip else dot_t(joint, w)
                    for at, n in enumerate(own):
                        res[n] = got[at * mb : (at + 1) * mb]
            return res

        drops = []
        holds = []
        for (m, k, u, _), raw in zip(chains, by_weights([c[3] for c in chains], False)):
            score = raw * scale + head_bias
            pos = jnp.maximum(score, 0.0)
            neg = score - pos
            soft = jnp.log2(1.0 + jnp.exp2(neg - pos))
            drop = pos + soft
            hold = neg - soft
            if m == 0:
                usable = (row2 >= rows) | (lane2 + tiles[k] * kt < place + u * half)
                drop = jnp.where(usable, drop, 0.0)
                hold = jnp.where(usable, hold, -jnp.inf)
            drops.append(drop)
            holds.append(hold)
        suffix = dot(jnp.concatenate([d.astype(bf) for d in drops], axis=0), later)
        suffix = [suffix[n * mb : (n + 1) * mb] for n in range(len(chains))]
        outs = by_weights([jnp.exp2(h - f).astype(bf) for h, f in zip(holds, suffix)], True)
        sums = [f[:, :1] + d[:, :1] for f, d in zip(suffix, drops)]
        for n in range(0, len(chains), 2):
            m, k, _, _ = chains[n]
            part = slice(m * mb, (m + 1) * mb)
            o_seg[tiles[k], part] = jnp.where(left2, outs[n], outs[n + 1])
            t_seg[tiles[k], part] = jnp.where(left2, sums[n], sums[n + 1])

    def keys_of(tile):
        straight = kv_all[pl.ds(2 * tile, 2)].reshape(kt, rows)
        return straight, pltpu.roll(straight.astype(f32), hd, 1).astype(bf)

    near = y // 2
    side = 2 * head - 1
    tiles = [lax.rem(near + k * side + NY // 2, NY // 2) for k in (0, 1, -1, 2)]

    def kv_waits(k):
        for u in range(2):
            src = 2 * tiles[k] + u

            @pl.when(src != y)
            def _():
                kv_copy(kv_other, src, 0, lax.rem(y + 1, NY)).wait_recv()

    def to_owner(j, e, sp, which):
        if which:
            return remote(o_send.at[j, e], o_recv.at[j, e], o_ss.at[j, e], o_rs.at[j, e], sp, t)
        return remote(t_send.at[j], t_recv.at[j, e], t_ss.at[j, e], t_rs.at[j, e], sp, t)

    first = lax.broadcasted_iota(jnp.int32, (8, rows), 0) < 4

    def finish(j):
        part = slice(PLACE[j] * rows, (PLACE[j] + 1) * rows)
        last = NY // 2 - 1
        acc = o_seg[last, part]
        carry = t_seg[last, part]
        for n in range(last - 1, -1, -1):
            acc = acc + jnp.exp2(-carry) * o_seg[n, part]
            carry = carry + t_seg[n, part]
        over = carry.T
        compact = jnp.where(first, over[0:8], over[hd : hd + 8])
        o_send[j] = acc.astype(bf).reshape(2, half, rows)
        t_send[j] = compact
        if j == 0:
            for which in range(2):
                start(to_owner(0, 1, z * NY + y_other, which))
        else:
            @pl.when(z + j < NZ)
            def _():
                for e in range(2):
                    for which in range(2):
                        to_owner(j, e, (z + j) * NY + (y_other if e else y), which).start()
        return acc[:half], compact

    def segments(*pairs):
        segment(pairs)

    q_wait(0, 1)
    q_send(1, 4, 5, 3, 2, 6, 7)
    q_waits((1,))
    kv_waits(0)
    segments((0, 0))
    windowed()
    kv_waits(1)
    segments((0, 1))
    kv_waits(2)
    kv_waits(3)
    segments((0, 2), (0, 3))
    own_o, own_t = finish(0)
    finish(1)

    for m, js in ((1, (3, 2)), (3, (4, 5)), (2, (6, 7))):
        @pl.when(z + min(js) < NZ)
        def _():
            q_waits(js)
            segments((m, 0), (m, 1))
            segments((m, 2), (m, 3))
            for j in js:
                finish(j)

    def from_owner(j, e, which):
        frm = lax.rem(z + NZ - j, NZ) * NY + (y_other if e else y)
        to_owner(j, e, frm, which).wait_recv()

    def arrivals(which):
        from_owner(0, 1, which)
        for j in range(1, NZ):
            @pl.when(z - j >= 0)
            def _():
                from_owner(j, 0, which)
                from_owner(j, 1, which)

    arrivals(0)
    left8 = left[:8]
    carry = jnp.where(left8, own_t, t_recv[0, 1])
    scales = []
    for j in range(1, NZ):
        scales.append(jnp.exp2(-carry))
        carry = carry + jnp.where(left8, t_recv[j, 0], t_recv[j, 1])
    scales = jnp.concatenate(scales + [jnp.zeros((rows - 8 * (NZ - 1), rows), f32)], axis=0).T
    arrivals(1)
    acc = jnp.concatenate([own_o, o_recv[0, 1].astype(f32)], axis=0)
    for j in range(1, NZ):
        at = 8 * (j - 1)
        here = o_recv[j].reshape(rows, rows).astype(f32)
        acc = acc + jnp.where(left, scales[:, at : at + 1], scales[:, at + 4 : at + 5]) * here
    head0 = jnp.where(head == 0, acc[:half], acc[half:])
    head1 = jnp.where(head == 0, acc[half:], acc[:half])
    s_out = jnp.concatenate(
        [
            jnp.where(left_half, head0, pltpu.roll(head1, hd, 1)),
            jnp.where(left_half, pltpu.roll(head0, hd, 1), head1),
        ],
        axis=0,
    ).astype(bf).astype(f32)
    l_os.wait()
    gained = (s_out * sgain[...].reshape(1, rows)).astype(bf)
    own_sums = jnp.broadcast_to(jnp.sum(s_out * s_out, axis=1, keepdims=True), (rows, rows))
    part = feats // 2
    pieces = ((a_keep0, d_send0, d_recv0, r_send0, r_recv0), (a_keep1, d_send1, d_recv1, r_send1, r_recv1))
    left_cut = left[:cut].reshape(1, cut, rows)

    def halves(values):
        return jnp.where(core == 0, values[:, 0], values[:, 1]), jnp.where(core == 0, values[:, 1], values[:, 0])

    def in_two(values):
        high = values.astype(bf).astype(f32)
        return jnp.where(left_cut, high, values - high).astype(bf)

    def joined(values):
        return values + pltpu.roll(values, hd, values.ndim - 1)

    def across(n):
        return remote(pieces[n][1], pieces[n][2], d_ss.at[n], d_rs.at[n], s, partner)

    def along(n, dx):
        to = lax.rem(chip + dx, NX)
        return remote(
            pieces[n][3].at[to], pieces[n][4].at[chip], r_ss.at[n, dx], r_rs.at[n, chip], s, to * 2 + core
        )

    for n, (keep, d_send, _, _, _) in enumerate(pieces):
        mine, theirs = halves(dot(gained, vos[:, n * part : (n + 1) * part]).reshape(NX, 2, cut, part))
        keep[:, :, :part] = mine
        d_send[:, :, :part] = theirs.astype(bf)
        if n == 0:
            mine, theirs = halves(own_sums.reshape(NX, 2, cut, rows))
            keep[:, :, part:] = mine
            d_send[:, :, part:] = in_two(theirs)
        start(across(n))
    inv_w = take(b_send, b_recv, b_ss, b_rs, total.at[1], NT * rows)
    total[1] = total[1] * inv_w
    for n, (keep, _, d_recv, r_send, _) in enumerate(pieces):
        across(n).wait_recv()
        r_send[:, :, :part] = (keep[:, :, :part] + d_recv[:, :, :part].astype(f32)).astype(bf)
        if n == 0:
            r_send[:, :, part:] = in_two(keep[:, :, part:] + joined(d_recv[:, :, part:].astype(f32)))
        for dx in (2, 1, 3):
            start(along(n, dx))
    sums = None
    for n, (_, _, _, r_send, r_recv) in enumerate(pieces):
        got = r_send[chip].astype(f32)
        for dx in (1, 3, 2):
            frm = lax.rem(chip + dx, NX)
            remote(
                r_send.at[frm], r_recv.at[frm], r_ss.at[n, dx], r_rs.at[n, frm], s, partner
            ).wait_recv()
            got = got + r_recv[frm].astype(f32)
        total[0, :, n * part : (n + 1) * part] = got[:, :part]
        if n == 0:
            sums = joined(got[:, part:])
    inv_s = lax.rsqrt(sums[:, :1] * (1.0 / (NT * rows)) + EPS)
    both = (total[0] * inv_s + total[1]).astype(bf).astype(f32)
    stats = jnp.sum(both * both, axis=1, keepdims=True) * (1.0 / feats)
    out_buf[...] = (both * lax.rsqrt(stats + EPS) * post_gain[...].reshape(1, feats)).astype(bf)

    out_copy = pltpu.make_async_copy(out_buf, out, out_sem)
    out_copy.start()
    for copy in given(b_send, b_recv, b_ss, b_rs):
        copy.wait_send()
    for copy in sends:
        copy.wait_send()
    for j in range(1, NZ):
        for e in range(2):
            @pl.when(z - j >= 0)
            def _():
                q_copy(j, e, z - j).wait_send()

            @pl.when(z + j < NZ)
            def _():
                for which in range(2):
                    to_owner(j, e, (z + j) * NY + (y_other if e else y), which).wait_send()

    @pl.when(s < N_SP - 1)
    def _():
        prev_copy(s + 1).wait_send()

    out_copy.wait()


def one_kernel(*args):
    tokens, pre_gain, wqs, wks, wvs, wqw, wkw, wvw, bias, sinks, sgain, wgain, wos, wow, post_gain = args
    bf = jnp.bfloat16
    f32 = jnp.float32
    rows, chunk = tokens.shape
    feats = NT * chunk
    cut = rows // NT
    widths = (feats // 2 + rows, feats // 2)
    v = pltpu.VMEM
    dma = pltpu.SemaphoreType.DMA
    anywhere = pl.BlockSpec(memory_space=pl.ANY)
    scratch = [
        v(pre_gain.shape, f32), pltpu.SMEM(bias.shape, f32), pltpu.SMEM(sinks.shape, f32),
        v(sgain.shape, f32), v(wgain.shape, f32), v(post_gain.shape, f32),
        v((NT, rows, chunk), bf), v((rows, rows), f32), v((rows, 4 * rows), f32), v((feats, 4 * rows), bf),
        v((rows, rows), f32), v((rows, feats), bf),
        v(wos.shape, bf), v(wow.shape, bf),
        v((NY, rows, rows), bf), v((rows, rows), bf), v((NZ, 2, rows // 2, rows), bf), v((rows // 2, rows), bf),
        v((NY // 2, NZ * rows, rows), f32), v((NY // 2, NZ * rows, rows), f32),
        v((rows, rows), bf), v((rows, rows), f32), v((rows, rows), bf),
        v((NZ, 2, rows // 2, rows), bf), v((NZ, 2, rows // 2, rows), bf),
        v((NZ, 8, rows), f32), v((NZ, 2, 8, rows), f32),
        *(v((NX, cut, width), f32) for width in widths),
        *(v((NX, cut, width), bf) for _ in range(4) for width in widths),
        v((NT, cut, feats + rows), bf), v((NT, cut, feats + rows), bf), v((2, cut, feats), f32), v((cut, feats), bf),
        dma((14,)), dma, dma((8,)), dma((NT,)), dma((NY,)), dma((NY,)), dma((NZ, 2)), dma((NZ, 2)), dma, dma,
        dma((NZ, 2)), dma((NZ, 2)), dma((NZ, 2)), dma((NZ, 2)), dma((2,)), dma((2,)), dma((2, NX)), dma((2, NX)), dma((NT,)), dma((NT,)), dma,
        pltpu.SemaphoreType.REGULAR,
    ]
    return pl.pallas_call(
        kernel,
        out_shape=jax.ShapeDtypeStruct((cut, feats), bf),
        in_specs=[anywhere] * len(args),
        out_specs=anywhere,
        scratch_shapes=scratch,
        compiler_params=pltpu.CompilerParams(
            collective_id=0, has_side_effects=True, vmem_limit_bytes=67043328
        ),
        name="layer",
    )(*args[:6], wkw.T, wvw.T, *args[8:])


def solution(mesh):
    in_specs = (
        P("sp", "tp"),
        P(),
        P(None, "tp"),
        P(None, "tp"),
        P(None, "tp"),
        P(None, "tp"),
        P(None, "tp"),
        P(None, "tp"),
        P("tp"),
        P("tp"),
        P("tp"),
        P("tp"),
        P("tp", None),
        P("tp", None),
        P(),
    )
    return jax.shard_map(
        one_kernel,
        mesh=mesh,
        in_specs=in_specs,
        out_specs=P(("sp", "tp"), None),
        check_vma=False,
    )
```

```python
import functools

import jax
import jax.numpy as jnp
from jax import lax
from jax.experimental import pallas as pl
from jax.experimental.pallas import tpu as pltpu
from jax.sharding import PartitionSpec as P

HEAD_DIM = 64
WINDOW = 128
EPS = 1e-06
LOG2E = 1.4426950408889634
MESH = pl.DeviceIdType.MESH
NY = 8
NZ = 8
NT = 8
NX = 4
N_SP = NY * NZ
PLACE = (0, 1, 2, 3, 7, 6, 5, 4)


def dot(a, b):
    return jnp.dot(a, b, preferred_element_type=jnp.float32)


def dot_t(a, b):
    return lax.dot_general(a, b, (((1,), (1,)), ((), ())), preferred_element_type=jnp.float32)


def kernel(
    tokens, pre_gain_in, wqs, wks, wvs, wqw, wkw, wvw, bias_in, sinks_in, sgain_in, wgain_in, wos, wow,
    post_gain_in, out,
    pre_gain, bias, sinks, sgain, wgain, post_gain, x, sq_acc, proj, vproj, kvw_acc, vkvw, vos, vow,
    kv_all, kv_other, q_all, q_other, o_seg, t_seg, kvw, qw_buf, kvw_prev, o_send, o_recv,
    a_keep0, a_keep1, d_send0, d_send1, d_recv0, d_recv1, r_send0, r_send1, r_recv0, r_recv1,
    b_send, b_recv, total, out_buf,
    w_sem, tok_sem, x_ss, x_rs, kv_ss, kv_rs, q_ss, q_rs, p_ss, p_rs, o_ss, o_rs,
    d_ss, d_rs, r_ss, r_rs, b_ss, b_rs, out_sem, ready,
):
    bf = jnp.bfloat16
    f32 = jnp.float32
    s = lax.axis_index("sp")
    t = lax.axis_index("tp")
    z = s // NY
    y = lax.rem(s, NY)
    chip = t // 2
    core = lax.rem(t, 2)
    head = lax.rem(y, 2)
    y_other = y + 1 - 2 * head
    partner = chip * 2 + 1 - core
    rows, chunk = tokens.shape
    feats = NT * chunk
    hd = HEAD_DIM
    cut = rows // NT

    barrier = pltpu.get_barrier_semaphore()

    def greet(sp, tp):
        pl.semaphore_signal(barrier, inc=1, device_id={"sp": sp, "tp": tp}, device_id_type=MESH)

    for k in range(1, NT):
        greet(s, lax.rem(t + k, NT))
    for k in range(1, NY):
        greet(z * NY + lax.rem(y + k, NY), t)
    for k in range(1, NZ):
        @pl.when(z + k < NZ)
        def _():
            greet((z + k) * NY + y, t)
            greet((z + k) * NY + y_other, t)
    starts_row = jnp.logical_and(y == 0, z > 0)
    ends_row = jnp.logical_and(y == NY - 1, z < NZ - 1)

    @pl.when(ends_row)
    def _():
        greet(s + 1, t)

    half = rows // 2
    loads = [
        pltpu.make_async_copy(src, dst, w_sem.at[n])
        for n, (src, dst) in enumerate(
            [(wks, vproj.at[:, :rows]), (wvs, vproj.at[:, rows : 2 * rows]), (wqs, vproj.at[:, 2 * rows : 3 * rows]),
             (wqw, vproj.at[:, 3 * rows :]), (wkw, vkvw.at[:half]), (wvw, vkvw.at[half:]),
             (wow, vow), (wos, vos),
             (bias_in, bias), (pre_gain_in, pre_gain), (sinks_in, sinks), (sgain_in, sgain),
             (wgain_in, wgain), (post_gain_in, post_gain)]
        )
    ]
    l_proj = loads[:6]
    l_ow, l_os, *l_small = loads[6:]
    tok_load = pltpu.make_async_copy(tokens, x.at[t], tok_sem)
    tok_load.start()
    for load in l_small + loads[:8]:
        load.start()

    for j in range(1, NZ):
        @pl.when(z + j >= NZ)
        def _():
            q_all[PLACE[j]] = jnp.zeros((2, half, rows), bf)

        @pl.when(z - j < 0)
        def _():
            o_recv[j] = jnp.zeros((2, half + 8, rows), bf)

    for load in l_small:
        load.wait()
    tok_load.wait()
    pl.semaphore_wait(barrier, NT - 1 + NY - 1 + 2 * z + starts_row.astype(jnp.int32))

    @pl.when(starts_row)
    def _():
        pl.semaphore_signal(ready, inc=1, device_id={"sp": s - 1, "tp": t}, device_id_type=MESH)

    def remote(src, dst, ss, rs, sp, tp):
        return pltpu.make_async_remote_copy(
            src_ref=src, dst_ref=dst, send_sem=ss, recv_sem=rs,
            device_id={"sp": sp, "tp": tp}, device_id_type=MESH,
        )

    sends = []

    def x_copy(slot, sem, tp):
        return remote(x.at[slot], x.at[slot], x_ss.at[sem], x_rs.at[slot], s, tp)

    def start(copy):
        copy.start()
        sends.append(copy)

    for dx in (2, 1, 3):
        start(x_copy(t, dx, lax.rem(chip + dx, NX) * 2 + core))
    start(x_copy(t, 0, partner))

    def absorb(*slots, first=False):
        sums = None
        for slot in slots:
            v = x[slot].astype(f32)
            part = pl.ds(pl.multiple_of(slot * chunk, chunk), chunk)
            gained = (v * pre_gain[part].reshape(1, chunk)).astype(bf)
            v = v * v
            more = (
                v[:, : chunk // 2] + v[:, chunk // 2 :], dot(gained, vproj[part, :]), dot_t(gained, vkvw[:, part])
            )
            sums = more if sums is None else tuple(p + q for p, q in zip(sums, more))
        for ref, more in zip((sq_acc, proj, kvw_acc), sums):
            ref[...] = more if first else ref[...] + more

    def block(dx, relayed):
        slot = lax.rem(chip + NX - dx, NX) * 2 + (1 - core if relayed else core)
        x_copy(slot, dx, partner).wait_recv()
        if not relayed:
            start(x_copy(slot, NX + dx, partner))
        return slot

    for load in l_proj:
        load.wait()
    absorb(t, block(0, 1), first=True)
    absorb(*[block(dx, 0) for dx in (1, 3, 2)])
    absorb(*[block(dx, 1) for dx in (1, 3, 2)])
    inv = lax.rsqrt(jnp.sum(sq_acc[...], axis=1, keepdims=True) * (1.0 / feats) + EPS)

    left = lax.broadcasted_iota(jnp.int32, (rows, rows), 1) < hd
    left_half = left[:half]

    keys, values = proj[:, :rows] * inv, proj[:, rows : 2 * rows] * inv
    head0 = jnp.where(left, keys, pltpu.roll(values, hd, 1))
    head1 = jnp.where(left, pltpu.roll(keys, hd, 1), values)
    kv_all[y] = jnp.where(head == 0, head0, head1).astype(bf)
    kv_other[...] = jnp.where(head == 0, head1, head0).astype(bf)

    def kv_copy(src, slot, sem, to_y):
        return remote(src, kv_all.at[slot], kv_ss.at[sem], kv_rs.at[slot], z * NY + to_y, t)

    def kv_send(k):
        start(kv_copy(kv_other if k % 2 else kv_all.at[y], y, k, lax.rem(y + k, NY)))

    qs = proj[:, 2 * rows : 3 * rows] * inv
    q0 = jnp.where(left_half, qs[:half], pltpu.roll(qs[half:], hd, 1))
    q1 = jnp.where(left_half, pltpu.roll(qs[:half], hd, 1), qs[half:])
    q_all[0, 0] = jnp.where(head == 0, q0, q1).astype(bf)
    q_other[...] = jnp.where(head == 0, q1, q0).astype(bf)

    def q_copy(j, e, to_z):
        src = q_all.at[0, e] if j > 1 or e == 0 else q_other
        to_y = y_other if e and j < 2 else y
        return remote(src, q_all.at[PLACE[j], e], q_ss.at[j, e], q_rs.at[j, e], to_z * NY + to_y, t)

    def q_send(e, *js):
        for j in js:
            @pl.when(z - j >= 0)
            def _():
                q_copy(j, e, z - j).start()

    start(q_copy(0, 1, z))
    q_send(0, 1)
    q_send(1, 1)
    for k in (1, 7):
        kv_send(k)
    q_send(0, 4, 5, 3)
    kv_send(4)
    q_send(0, 2, 6, 7)

    kvw[...] = (kvw_acc[...] * inv).astype(bf)

    def prev_copy(to):
        return remote(kvw, kvw_prev, p_ss, p_rs, to, t)

    @pl.when(y < NY - 1)
    def _():
        prev_copy(s + 1).start()

    for k in (3, 5, 2, 6):
        kv_send(k)

    @pl.when(ends_row)
    def _():
        pl.semaphore_wait(ready, 1)
        prev_copy(s + 1).start()

    @pl.when(s == 0)
    def _():
        kvw_prev[...] = jnp.zeros_like(kvw_prev)

    qw_buf[...] = proj[:, 3 * rows :] * inv

    def given(send, recv, ss, rs):
        for dx, dc in ((2, 0), (2, 1), (1, 0), (1, 1), (3, 0), (3, 1), (0, 1)):
            to = lax.rem(chip + dx, NX) * 2 + lax.rem(core + dc, 2)
            yield remote(send.at[to], recv.at[t], ss.at[2 * dx + dc], rs.at[t], s, to)

    def give(send, recv, ss, rs, values, weights):
        sums = jnp.sum(values * values, axis=1, keepdims=True)
        high = sums.astype(bf)
        low = (sums - high.astype(f32)).astype(bf)
        send[:, :, feats:] = jnp.where(left, high.astype(f32), low.astype(f32)).astype(bf).reshape(NT, cut, rows)
        gained, w = weights
        n_cut = 4
        part = feats // n_cut
        for n in range(n_cut):
            cols = slice(n * part, (n + 1) * part)
            send[:, :, cols] = dot(gained, w[:, cols]).astype(bf).reshape(NT, cut, part)
        for copy in given(send, recv, ss, rs):
            copy.start()

    def take(send, recv, ss, rs, acc, width):
        own = send[t].astype(f32)
        acc[...] = own[:, :feats]
        sums = own[:, feats:]
        for dx, dc in ((0, 1), (1, 0), (1, 1), (3, 0), (3, 1), (2, 0), (2, 1)):
            frm = lax.rem(chip + dx, NX) * 2 + lax.rem(core + dc, 2)
            remote(send.at[frm], recv.at[frm], ss.at[2 * dx + dc], rs.at[frm], s, partner).wait_recv()
            got = recv[frm].astype(f32)
            acc[...] += got[:, :feats]
            sums += got[:, feats:]
        return lax.rsqrt((sums[:, :1] + sums[:, hd : hd + 1]) * (1.0 / width) + EPS)

    def windowed():
        @pl.when(s > 0)
        def _():
            prev_copy(s - 1).wait_recv()

        two = 2 * rows
        r_iota = lax.broadcasted_iota(jnp.int32, (two, two), 0)
        c_iota = lax.broadcasted_iota(jnp.int32, (two, two), 1)
        dist = lax.rem(r_iota, rows) + rows - c_iota
        in_window = (dist >= 0) & (dist < WINDOW) & ((c_iota >= rows) | (s > 0))
        first_rows = lax.broadcasted_iota(jnp.int32, (two, 1), 0) < rows
        qw = qw_buf[...]
        kk = jnp.concatenate([kvw_prev[...], kvw[...]], axis=0)
        qq = jnp.concatenate([jnp.where(left, qw, 0.0), jnp.where(left, pltpu.roll(qw, hd, 1), 0.0)], axis=0).astype(bf)
        logits = jnp.where(in_window, dot_t(qq, kk) * hd**-0.5, -jnp.inf)
        sink = jnp.where(first_rows, sinks[0], sinks[1])
        top = jnp.maximum(jnp.max(logits, axis=1, keepdims=True), sink)
        grown = jnp.exp(logits - top)
        norm = jnp.sum(grown, axis=1, keepdims=True) + jnp.exp(sink - top)
        res = dot((grown / norm).astype(bf), kk)
        w_out = jnp.where(left, pltpu.roll(res[:rows], hd, 1), res[rows:]).astype(bf).astype(f32)

        l_ow.wait()
        give(b_send, b_recv, b_ss, b_rs, w_out, ((w_out * wgain[...].reshape(1, rows)).astype(bf), vow))

    def q_wait(j, e):
        frm = lax.rem(z + j, NZ) * NY + (y_other if e else y)
        remote(q_other, q_all.at[PLACE[j], e], q_ss.at[j, e], q_rs.at[j, e], frm, t).wait_recv()

    def q_waits(js):
        for j in js:
            @pl.when(z + j < NZ)
            def _():
                q_wait(j, 0)
                q_wait(j, 1)

    kt = 2 * rows
    mb = 2 * rows
    per = mb // rows
    later = (
        lax.broadcasted_iota(jnp.int32, (kt, kt), 0) > lax.broadcasted_iota(jnp.int32, (kt, kt), 1)
    ).astype(bf)
    row2 = lax.broadcasted_iota(jnp.int32, (mb, kt), 0)
    lane2 = lax.broadcasted_iota(jnp.int32, (mb, kt), 1)
    place = lax.rem(row2, half) + jnp.where(row2 < half, y, y_other) * rows
    left2 = lax.broadcasted_iota(jnp.int32, (mb, rows), 1) < hd
    scale = LOG2E * hd**-0.5
    head_bias = bias[head] * LOG2E

    def segment(pairs):
        weights_of = {}
        chains = []
        for m, k in pairs:
            if k not in weights_of:
                weights_of[k] = keys_of(tiles[k])
            queries = q_all[m * per : (m + 1) * per].reshape(mb, rows).astype(f32)
            for u in range(2):
                qh = jnp.where(jnp.logical_not(left2) if u else left2, queries, 0.0).astype(bf)
                chains.append((m, k, u, qh))

        def by_weights(values, flip):
            res = [None] * len(chains)
            for k in weights_of:
                for u in range(2):
                    own = [n for n, c in enumerate(chains) if c[1] == k and c[2] == u]
                    joint = jnp.concatenate([values[n] for n in own], axis=0)
                    w = weights_of[k][1 - u if flip else u]
                    got = dot(joint, w) if flip else dot_t(joint, w)
                    for at, n in enumerate(own):
                        res[n] = got[at * mb : (at + 1) * mb]
            return res

        drops = []
        holds = []
        for (m, k, u, _), raw in zip(chains, by_weights([c[3] for c in chains], False)):
            score = raw * scale + head_bias
            pos = jnp.maximum(score, 0.0)
            neg = score - pos
            soft = jnp.log2(1.0 + jnp.exp2(neg - pos))
            drop = pos + soft
            hold = neg - soft
            if m == 0:
                usable = (row2 >= rows) | (lane2 + tiles[k] * kt < place + u * half)
                drop = jnp.where(usable, drop, 0.0)
                hold = jnp.where(usable, hold, -jnp.inf)
            drops.append(drop)
            holds.append(hold)
        suffix = dot(jnp.concatenate([d.astype(bf) for d in drops], axis=0), later)
        suffix = [suffix[n * mb : (n + 1) * mb] for n in range(len(chains))]
        outs = by_weights([jnp.exp2(h - f).astype(bf) for h, f in zip(holds, suffix)], True)
        sums = [f[:, :1] + d[:, :1] for f, d in zip(suffix, drops)]
        for n in range(0, len(chains), 2):
            m, k, _, _ = chains[n]
            part = slice(m * mb, (m + 1) * mb)
            o_seg[tiles[k], part] = jnp.where(left2, outs[n], outs[n + 1])
            t_seg[tiles[k], part] = jnp.where(left2, sums[n], sums[n + 1])

    def keys_of(tile):
        straight = kv_all[pl.ds(2 * tile, 2)].reshape(kt, rows)
        return straight, pltpu.roll(straight.astype(f32), hd, 1).astype(bf)

    near = y // 2
    side = 2 * head - 1
    tiles = [lax.rem(near + k * side + NY // 2, NY // 2) for k in (0, 1, -1, 2)]

    def kv_waits(k):
        for u in range(2):
            src = 2 * tiles[k] + u

            @pl.when(src != y)
            def _():
                kv_copy(kv_other, src, 0, lax.rem(y + 1, NY)).wait_recv()

    def to_owner(j, e, sp):
        return remote(o_send.at[j, e], o_recv.at[j, e], o_ss.at[j, e], o_rs.at[j, e], sp, t)

    sublane = lax.broadcasted_iota(jnp.int32, (8, rows), 0)
    first = sublane < 4

    def finish(j):
        part = slice(PLACE[j] * rows, (PLACE[j] + 1) * rows)
        last = NY // 2 - 1
        acc = o_seg[last, part]
        carry = t_seg[last, part]
        for n in range(last - 1, -1, -1):
            acc = acc + jnp.exp2(-carry) * o_seg[n, part]
            carry = carry + t_seg[n, part]
        over = carry.T
        compact = jnp.where(first, over[0:8], over[hd : hd + 8])
        high = compact.astype(bf).astype(f32)
        parted = jnp.where(lax.rem(sublane, 4) < 2, high, compact - high).astype(bf)
        for e in range(2):
            o_send[j, e, :half] = acc[e * half : (e + 1) * half].astype(bf)
            o_send[j, e, half:] = parted
        if j == 0:
            start(to_owner(0, 1, z * NY + y_other))
        else:
            @pl.when(z + j < NZ)
            def _():
                for e in range(2):
                    to_owner(j, e, (z + j) * NY + (y_other if e else y)).start()
        return acc[:half], compact

    def segments(*pairs):
        segment(pairs)

    q_wait(0, 1)
    q_send(1, 4, 5, 3, 2, 6, 7)
    q_waits((1,))
    kv_waits(0)
    segments((0, 0))
    windowed()
    kv_waits(1)
    kv_waits(2)
    kv_waits(3)
    segments((0, 1), (0, 2), (0, 3))
    own_o, own_t = finish(0)
    finish(1)

    for m, js in ((1, (3, 2)), (3, (4, 5)), (2, (6, 7))):
        @pl.when(z + min(js) < NZ)
        def _():
            q_waits(js)
            segments(*((m, k) for k in range(NY // 2)))
            for j in js:
                finish(j)

    def from_owner(j, e):
        frm = lax.rem(z + NZ - j, NZ) * NY + (y_other if e else y)
        to_owner(j, e, frm).wait_recv()

    def logs_of(j, e):
        parted = o_recv[j, e, half:].astype(f32)
        return parted + pltpu.roll(parted, 6, 0)

    from_owner(0, 1)
    for j in range(1, NZ):
        @pl.when(z - j >= 0)
        def _():
            from_owner(j, 0)
            from_owner(j, 1)

    left8 = left[:8]
    carry = jnp.where(left8, own_t, logs_of(0, 1))
    scales = []
    for j in range(1, NZ):
        scales.append(jnp.exp2(-carry))
        carry = carry + jnp.where(left8, logs_of(j, 0), logs_of(j, 1))
    scales = jnp.concatenate(scales + [jnp.zeros((rows - 8 * (NZ - 1), rows), f32)], axis=0).T
    acc = jnp.concatenate([own_o, o_recv[0, 1, :half].astype(f32)], axis=0)
    for j in range(1, NZ):
        at = 8 * (j - 1)
        here = jnp.concatenate([o_recv[j, 0, :half].astype(f32), o_recv[j, 1, :half].astype(f32)], axis=0)
        acc = acc + jnp.where(left, scales[:, at : at + 1], scales[:, at + 4 : at + 5]) * here
    head0 = jnp.where(head == 0, acc[:half], acc[half:])
    head1 = jnp.where(head == 0, acc[half:], acc[:half])
    s_out = jnp.concatenate(
        [
            jnp.where(left_half, head0, pltpu.roll(head1, hd, 1)),
            jnp.where(left_half, pltpu.roll(head0, hd, 1), head1),
        ],
        axis=0,
    ).astype(bf).astype(f32)
    l_os.wait()
    gained = (s_out * sgain[...].reshape(1, rows)).astype(bf)
    own_sums = jnp.broadcast_to(jnp.sum(s_out * s_out, axis=1, keepdims=True), (rows, rows))
    part = feats // 2
    pieces = ((a_keep0, d_send0, d_recv0, r_send0, r_recv0), (a_keep1, d_send1, d_recv1, r_send1, r_recv1))
    left_cut = left[:cut].reshape(1, cut, rows)

    def halves(values):
        return jnp.where(core == 0, values[:, 0], values[:, 1]), jnp.where(core == 0, values[:, 1], values[:, 0])

    def in_two(values):
        high = values.astype(bf).astype(f32)
        return jnp.where(left_cut, high, values - high).astype(bf)

    def joined(values):
        return values + pltpu.roll(values, hd, values.ndim - 1)

    def across(n):
        return remote(pieces[n][1], pieces[n][2], d_ss.at[n], d_rs.at[n], s, partner)

    def along(n, dx):
        to = lax.rem(chip + dx, NX)
        return remote(
            pieces[n][3].at[to], pieces[n][4].at[chip], r_ss.at[n, dx], r_rs.at[n, chip], s, to * 2 + core
        )

    for n, (keep, d_send, _, _, _) in enumerate(pieces):
        mine, theirs = halves(dot(gained, vos[:, n * part : (n + 1) * part]).reshape(NX, 2, cut, part))
        keep[:, :, :part] = mine
        d_send[:, :, :part] = theirs.astype(bf)
        if n == 0:
            mine, theirs = halves(own_sums.reshape(NX, 2, cut, rows))
            keep[:, :, part:] = mine
            d_send[:, :, part:] = in_two(theirs)
        start(across(n))
    inv_w = take(b_send, b_recv, b_ss, b_rs, total.at[1], NT * rows)
    total[1] = total[1] * inv_w
    for n, (keep, _, d_recv, r_send, _) in enumerate(pieces):
        across(n).wait_recv()
        r_send[:, :, :part] = (keep[:, :, :part] + d_recv[:, :, :part].astype(f32)).astype(bf)
        if n == 0:
            r_send[:, :, part:] = in_two(keep[:, :, part:] + joined(d_recv[:, :, part:].astype(f32)))
        for dx in (2, 1, 3):
            start(along(n, dx))
    sums = None
    for n, (_, _, _, r_send, r_recv) in enumerate(pieces):
        got = r_send[chip].astype(f32)
        for dx in (1, 3, 2):
            frm = lax.rem(chip + dx, NX)
            remote(
                r_send.at[frm], r_recv.at[frm], r_ss.at[n, dx], r_rs.at[n, frm], s, partner
            ).wait_recv()
            got = got + r_recv[frm].astype(f32)
        total[0, :, n * part : (n + 1) * part] = got[:, :part]
        if n == 0:
            sums = joined(got[:, part:])
    inv_s = lax.rsqrt(sums[:, :1] * (1.0 / (NT * rows)) + EPS)
    both = (total[0] * inv_s + total[1]).astype(bf).astype(f32)
    stats = jnp.sum(both * both, axis=1, keepdims=True) * (1.0 / feats)
    out_buf[...] = (both * lax.rsqrt(stats + EPS) * post_gain[...].reshape(1, feats)).astype(bf)

    out_copy = pltpu.make_async_copy(out_buf, out, out_sem)
    out_copy.start()
    for copy in given(b_send, b_recv, b_ss, b_rs):
        copy.wait_send()
    for copy in sends:
        copy.wait_send()
    for j in range(1, NZ):
        for e in range(2):
            @pl.when(z - j >= 0)
            def _():
                q_copy(j, e, z - j).wait_send()

            @pl.when(z + j < NZ)
            def _():
                to_owner(j, e, (z + j) * NY + (y_other if e else y)).wait_send()

    @pl.when(s < N_SP - 1)
    def _():
        prev_copy(s + 1).wait_send()

    out_copy.wait()


def one_kernel(*args):
    tokens, pre_gain, wqs, wks, wvs, wqw, wkw, wvw, bias, sinks, sgain, wgain, wos, wow, post_gain = args
    bf = jnp.bfloat16
    f32 = jnp.float32
    rows, chunk = tokens.shape
    feats = NT * chunk
    cut = rows // NT
    widths = (feats // 2 + rows, feats // 2)
    v = pltpu.VMEM
    dma = pltpu.SemaphoreType.DMA
    anywhere = pl.BlockSpec(memory_space=pl.ANY)
    scratch = [
        v(pre_gain.shape, f32), pltpu.SMEM(bias.shape, f32), pltpu.SMEM(sinks.shape, f32),
        v(sgain.shape, f32), v(wgain.shape, f32), v(post_gain.shape, f32),
        v((NT, rows, chunk), bf), v((rows, rows), f32), v((rows, 4 * rows), f32), v((feats, 4 * rows), bf),
        v((rows, rows), f32), v((rows, feats), bf),
        v(wos.shape, bf), v(wow.shape, bf),
        v((NY, rows, rows), bf), v((rows, rows), bf), v((NZ, 2, rows // 2, rows), bf), v((rows // 2, rows), bf),
        v((NY // 2, NZ * rows, rows), f32), v((NY // 2, NZ * rows, rows), f32),
        v((rows, rows), bf), v((rows, rows), f32), v((rows, rows), bf),
        v((NZ, 2, rows // 2 + 8, rows), bf), v((NZ, 2, rows // 2 + 8, rows), bf),
        *(v((NX, cut, width), f32) for width in widths),
        *(v((NX, cut, width), bf) for _ in range(4) for width in widths),
        v((NT, cut, feats + rows), bf), v((NT, cut, feats + rows), bf), v((2, cut, feats), f32), v((cut, feats), bf),
        dma((14,)), dma, dma((8,)), dma((NT,)), dma((NY,)), dma((NY,)), dma((NZ, 2)), dma((NZ, 2)), dma, dma,
        dma((NZ, 2)), dma((NZ, 2)), dma((2,)), dma((2,)), dma((2, NX)), dma((2, NX)), dma((NT,)), dma((NT,)), dma,
        pltpu.SemaphoreType.REGULAR,
    ]
    return pl.pallas_call(
        kernel,
        out_shape=jax.ShapeDtypeStruct((cut, feats), bf),
        in_specs=[anywhere] * len(args),
        out_specs=anywhere,
        scratch_shapes=scratch,
        compiler_params=pltpu.CompilerParams(
            collective_id=0, has_side_effects=True, vmem_limit_bytes=67043328
        ),
        name="layer",
    )(*args[:6], wkw.T, wvw.T, *args[8:])


def solution(mesh):
    in_specs = (
        P("sp", "tp"),
        P(),
        P(None, "tp"),
        P(None, "tp"),
        P(None, "tp"),
        P(None, "tp"),
        P(None, "tp"),
        P(None, "tp"),
        P("tp"),
        P("tp"),
        P("tp"),
        P("tp"),
        P("tp", None),
        P("tp", None),
        P(),
    )
    return jax.shard_map(
        one_kernel,
        mesh=mesh,
        in_specs=in_specs,
        out_specs=P(("sp", "tp"), None),
        check_vma=False,
    )
```

```python
import functools

import jax
import jax.numpy as jnp
from jax import lax
from jax.experimental import pallas as pl
from jax.experimental.pallas import tpu as pltpu
from jax.sharding import PartitionSpec as P

HEAD_DIM = 64
WINDOW = 128
EPS = 1e-06
LOG2E = 1.4426950408889634
MESH = pl.DeviceIdType.MESH
NY = 8
NZ = 8
NT = 8
NX = 4
N_SP = NY * NZ
PLACE = (0, 1, 2, 3, 7, 6, 5, 4)


def dot(a, b):
    return jnp.dot(a, b, preferred_element_type=jnp.float32)


def dot_t(a, b):
    return lax.dot_general(a, b, (((1,), (1,)), ((), ())), preferred_element_type=jnp.float32)


def kernel(
    tokens, pre_gain_in, wqs, wks, wvs, wqw, wkw, wvw, bias_in, sinks_in, sgain_in, wgain_in, wos, wow,
    post_gain_in, out,
    pre_gain, bias, sinks, sgain, wgain, post_gain, x, sq_acc, proj, vproj, kvw_acc, vkvw, vos, vow,
    kv_all, kv_other, q_all, q_other, o_seg, t_seg, kvw, qw_buf, kvw_prev, o_send, o_recv,
    a_keep0, a_keep1, d_send0, d_send1, d_recv0, d_recv1, r_send0, r_send1, r_recv0, r_recv1,
    b_send, b_recv, total, out_buf,
    w_sem, tok_sem, x_ss, x_rs, kv_ss, kv_rs, q_ss, q_rs, p_ss, p_rs, o_ss, o_rs,
    d_ss, d_rs, r_ss, r_rs, b_ss, b_rs, out_sem, ready,
):
    bf = jnp.bfloat16
    f32 = jnp.float32
    s = lax.axis_index("sp")
    t = lax.axis_index("tp")
    z = s // NY
    y = lax.rem(s, NY)
    chip = t // 2
    core = lax.rem(t, 2)
    head = lax.rem(y, 2)
    y_other = y + 1 - 2 * head
    partner = chip * 2 + 1 - core
    rows, chunk = tokens.shape
    feats = NT * chunk
    hd = HEAD_DIM
    cut = rows // NT

    barrier = pltpu.get_barrier_semaphore()

    def greet(sp, tp):
        pl.semaphore_signal(barrier, inc=1, device_id={"sp": sp, "tp": tp}, device_id_type=MESH)

    for k in range(1, NT):
        greet(s, lax.rem(t + k, NT))
    for k in range(1, NY):
        greet(z * NY + lax.rem(y + k, NY), t)
    for k in range(1, NZ):
        @pl.when(z + k < NZ)
        def _():
            greet((z + k) * NY + y, t)
            greet((z + k) * NY + y_other, t)
    starts_row = jnp.logical_and(y == 0, z > 0)
    ends_row = jnp.logical_and(y == NY - 1, z < NZ - 1)

    @pl.when(ends_row)
    def _():
        greet(s + 1, t)

    half = rows // 2
    loads = [
        pltpu.make_async_copy(src, dst, w_sem.at[n])
        for n, (src, dst) in enumerate(
            [(wks, vproj.at[:, :rows]), (wvs, vproj.at[:, rows : 2 * rows]), (wqs, vproj.at[:, 2 * rows : 3 * rows]),
             (wqw, vproj.at[:, 3 * rows :]), (wkw, vkvw.at[:half]), (wvw, vkvw.at[half:]),
             (wow, vow), (wos, vos),
             (bias_in, bias), (pre_gain_in, pre_gain), (sinks_in, sinks), (sgain_in, sgain),
             (wgain_in, wgain), (post_gain_in, post_gain)]
        )
    ]
    l_proj = loads[:6]
    l_ow, l_os, *l_small = loads[6:]
    tok_load = pltpu.make_async_copy(tokens, x.at[t], tok_sem)
    tok_load.start()
    for load in l_small + loads[:8]:
        load.start()

    for j in range(1, NZ):
        @pl.when(z + j >= NZ)
        def _():
            q_all[PLACE[j]] = jnp.zeros((2, half, rows), bf)

        @pl.when(z - j < 0)
        def _():
            o_recv[j] = jnp.zeros((2, half + 8, rows), bf)

    for load in l_small:
        load.wait()
    tok_load.wait()
    pl.semaphore_wait(barrier, NT - 1 + NY - 1 + 2 * z + starts_row.astype(jnp.int32))

    @pl.when(starts_row)
    def _():
        pl.semaphore_signal(ready, inc=1, device_id={"sp": s - 1, "tp": t}, device_id_type=MESH)

    def remote(src, dst, ss, rs, sp, tp):
        return pltpu.make_async_remote_copy(
            src_ref=src, dst_ref=dst, send_sem=ss, recv_sem=rs,
            device_id={"sp": sp, "tp": tp}, device_id_type=MESH,
        )

    sends = []

    def x_copy(slot, sem, tp):
        return remote(x.at[slot], x.at[slot], x_ss.at[sem], x_rs.at[slot], s, tp)

    def start(copy):
        copy.start()
        sends.append(copy)

    for dx in (2, 1, 3):
        start(x_copy(t, dx, lax.rem(chip + dx, NX) * 2 + core))
    start(x_copy(t, 0, partner))

    def absorb(*slots, first=False):
        sums = None
        for slot in slots:
            v = x[slot].astype(f32)
            part = pl.ds(pl.multiple_of(slot * chunk, chunk), chunk)
            gained = (v * pre_gain[part].reshape(1, chunk)).astype(bf)
            v = v * v
            more = (
                v[:, : chunk // 2] + v[:, chunk // 2 :], dot(gained, vproj[part, :]), dot_t(gained, vkvw[:, part])
            )
            sums = more if sums is None else tuple(p + q for p, q in zip(sums, more))
        for ref, more in zip((sq_acc, proj, kvw_acc), sums):
            ref[...] = more if first else ref[...] + more

    def block(dx, relayed):
        slot = lax.rem(chip + NX - dx, NX) * 2 + (1 - core if relayed else core)
        x_copy(slot, dx, partner).wait_recv()
        if not relayed:
            start(x_copy(slot, NX + dx, partner))
        return slot

    for load in l_proj:
        load.wait()
    absorb(t, block(0, 1), first=True)
    absorb(*[block(dx, 0) for dx in (1, 3, 2)])
    absorb(*[block(dx, 1) for dx in (1, 3)])
    absorb(block(2, 1))
    inv = lax.rsqrt(jnp.sum(sq_acc[...], axis=1, keepdims=True) * (1.0 / feats) + EPS)

    left = lax.broadcasted_iota(jnp.int32, (rows, rows), 1) < hd
    left_half = left[:half]

    keys, values = proj[:, :rows] * inv, proj[:, rows : 2 * rows] * inv
    head0 = jnp.where(left, keys, pltpu.roll(values, hd, 1))
    head1 = jnp.where(left, pltpu.roll(keys, hd, 1), values)
    kv_all[y] = jnp.where(head == 0, head0, head1).astype(bf)
    kv_other[...] = jnp.where(head == 0, head1, head0).astype(bf)

    def kv_copy(src, slot, sem, to_y):
        return remote(src, kv_all.at[slot], kv_ss.at[sem], kv_rs.at[slot], z * NY + to_y, t)

    def kv_send(k):
        start(kv_copy(kv_other if k % 2 else kv_all.at[y], y, k, lax.rem(y + k, NY)))

    qs = proj[:, 2 * rows : 3 * rows] * inv
    q0 = jnp.where(left_half, qs[:half], pltpu.roll(qs[half:], hd, 1))
    q1 = jnp.where(left_half, pltpu.roll(qs[:half], hd, 1), qs[half:])
    q_all[0, 0] = jnp.where(head == 0, q0, q1).astype(bf)
    q_other[...] = jnp.where(head == 0, q1, q0).astype(bf)

    def q_copy(j, e, to_z):
        src = q_all.at[0, e] if j > 1 or e == 0 else q_other
        to_y = y_other if e and j < 2 else y
        return remote(src, q_all.at[PLACE[j], e], q_ss.at[j, e], q_rs.at[j, e], to_z * NY + to_y, t)

    def q_send(e, *js):
        for j in js:
            @pl.when(z - j >= 0)
            def _():
                q_copy(j, e, z - j).start()

    start(q_copy(0, 1, z))
    q_send(0, 1)
    q_send(1, 1)
    for k in (1, 7):
        kv_send(k)
    q_send(0, 4, 5, 3)
    kv_send(4)
    q_send(0, 2, 6, 7)

    kvw[...] = (kvw_acc[...] * inv).astype(bf)

    def prev_copy(to):
        return remote(kvw, kvw_prev, p_ss, p_rs, to, t)

    @pl.when(y < NY - 1)
    def _():
        prev_copy(s + 1).start()

    for k in (3, 5, 2, 6):
        kv_send(k)

    @pl.when(ends_row)
    def _():
        pl.semaphore_wait(ready, 1)
        prev_copy(s + 1).start()

    @pl.when(s == 0)
    def _():
        kvw_prev[...] = jnp.zeros_like(kvw_prev)

    qw_buf[...] = proj[:, 3 * rows :] * inv

    def given(send, recv, ss, rs):
        for dx, dc in ((2, 0), (2, 1), (1, 0), (1, 1), (3, 0), (3, 1), (0, 1)):
            to = lax.rem(chip + dx, NX) * 2 + lax.rem(core + dc, 2)
            yield remote(send.at[to], recv.at[t], ss.at[2 * dx + dc], rs.at[t], s, to)

    def give(send, recv, ss, rs, values, weights):
        sums = jnp.sum(values * values, axis=1, keepdims=True)
        high = sums.astype(bf)
        low = (sums - high.astype(f32)).astype(bf)
        send[:, :, feats:] = jnp.where(left, high.astype(f32), low.astype(f32)).astype(bf).reshape(NT, cut, rows)
        gained, w = weights
        n_cut = 4
        part = feats // n_cut
        for n in range(n_cut):
            cols = slice(n * part, (n + 1) * part)
            send[:, :, cols] = dot(gained, w[:, cols]).astype(bf).reshape(NT, cut, part)
        for copy in given(send, recv, ss, rs):
            copy.start()

    def take(send, recv, ss, rs, acc, width):
        own = send[t].astype(f32)
        acc[...] = own[:, :feats]
        sums = own[:, feats:]
        for dx, dc in ((0, 1), (1, 0), (1, 1), (3, 0), (3, 1), (2, 0), (2, 1)):
            frm = lax.rem(chip + dx, NX) * 2 + lax.rem(core + dc, 2)
            remote(send.at[frm], recv.at[frm], ss.at[2 * dx + dc], rs.at[frm], s, partner).wait_recv()
            got = recv[frm].astype(f32)
            acc[...] += got[:, :feats]
            sums += got[:, feats:]
        return lax.rsqrt((sums[:, :1] + sums[:, hd : hd + 1]) * (1.0 / width) + EPS)

    def windowed():
        @pl.when(s > 0)
        def _():
            prev_copy(s - 1).wait_recv()

        two = 2 * rows
        r_iota = lax.broadcasted_iota(jnp.int32, (two, two), 0)
        c_iota = lax.broadcasted_iota(jnp.int32, (two, two), 1)
        dist = lax.rem(r_iota, rows) + rows - c_iota
        in_window = (dist >= 0) & (dist < WINDOW) & ((c_iota >= rows) | (s > 0))
        first_rows = lax.broadcasted_iota(jnp.int32, (two, 1), 0) < rows
        qw = qw_buf[...]
        kk = jnp.concatenate([kvw_prev[...], kvw[...]], axis=0)
        qq = jnp.concatenate([jnp.where(left, qw, 0.0), jnp.where(left, pltpu.roll(qw, hd, 1), 0.0)], axis=0).astype(bf)
        logits = jnp.where(in_window, dot_t(qq, kk) * hd**-0.5, -jnp.inf)
        sink = jnp.where(first_rows, sinks[0], sinks[1])
        top = jnp.maximum(jnp.max(logits, axis=1, keepdims=True), sink)
        grown = jnp.exp(logits - top)
        norm = jnp.sum(grown, axis=1, keepdims=True) + jnp.exp(sink - top)
        res = dot((grown / norm).astype(bf), kk)
        w_out = jnp.where(left, pltpu.roll(res[:rows], hd, 1), res[rows:]).astype(bf).astype(f32)

        l_ow.wait()
        give(b_send, b_recv, b_ss, b_rs, w_out, ((w_out * wgain[...].reshape(1, rows)).astype(bf), vow))

    def q_wait(j, e):
        frm = lax.rem(z + j, NZ) * NY + (y_other if e else y)
        remote(q_other, q_all.at[PLACE[j], e], q_ss.at[j, e], q_rs.at[j, e], frm, t).wait_recv()

    def q_waits(js):
        for j in js:
            @pl.when(z + j < NZ)
            def _():
                q_wait(j, 0)
                q_wait(j, 1)

    kt = 2 * rows
    mb = 2 * rows
    per = mb // rows
    later = (
        lax.broadcasted_iota(jnp.int32, (kt, kt), 0) > lax.broadcasted_iota(jnp.int32, (kt, kt), 1)
    ).astype(bf)
    row2 = lax.broadcasted_iota(jnp.int32, (mb, kt), 0)
    lane2 = lax.broadcasted_iota(jnp.int32, (mb, kt), 1)
    place = lax.rem(row2, half) + jnp.where(row2 < half, y, y_other) * rows
    left2 = lax.broadcasted_iota(jnp.int32, (mb, rows), 1) < hd
    scale = LOG2E * hd**-0.5
    head_bias = bias[head] * LOG2E

    def segment(pairs):
        weights_of = {}
        chains = []
        for m, k in pairs:
            if k not in weights_of:
                weights_of[k] = keys_of(tiles[k])
            queries = q_all[m * per : (m + 1) * per].reshape(mb, rows).astype(f32)
            for u in range(2):
                qh = jnp.where(jnp.logical_not(left2) if u else left2, queries, 0.0).astype(bf)
                chains.append((m, k, u, qh))

        def by_weights(values, flip):
            res = [None] * len(chains)
            for k in weights_of:
                for u in range(2):
                    own = [n for n, c in enumerate(chains) if c[1] == k and c[2] == u]
                    joint = jnp.concatenate([values[n] for n in own], axis=0)
                    w = weights_of[k][1 - u if flip else u]
                    got = dot(joint, w) if flip else dot_t(joint, w)
                    for at, n in enumerate(own):
                        res[n] = got[at * mb : (at + 1) * mb]
            return res

        drops = []
        holds = []
        for (m, k, u, _), raw in zip(chains, by_weights([c[3] for c in chains], False)):
            score = raw * scale + head_bias
            pos = jnp.maximum(score, 0.0)
            neg = score - pos
            soft = jnp.log2(1.0 + jnp.exp2(neg - pos))
            drop = pos + soft
            hold = neg - soft
            if m == 0:
                usable = (row2 >= rows) | (lane2 + tiles[k] * kt < place + u * half)
                drop = jnp.where(usable, drop, 0.0)
                hold = jnp.where(usable, hold, -jnp.inf)
            drops.append(drop)
            holds.append(hold)
        suffix = dot(jnp.concatenate([d.astype(bf) for d in drops], axis=0), later)
        suffix = [suffix[n * mb : (n + 1) * mb] for n in range(len(chains))]
        outs = by_weights([jnp.exp2(h - f).astype(bf) for h, f in zip(holds, suffix)], True)
        sums = [f[:, :1] + d[:, :1] for f, d in zip(suffix, drops)]
        for n in range(0, len(chains), 2):
            m, k, _, _ = chains[n]
            part = slice(m * mb, (m + 1) * mb)
            o_seg[tiles[k], part] = jnp.where(left2, outs[n], outs[n + 1])
            t_seg[tiles[k], part] = jnp.where(left2, sums[n], sums[n + 1])

    def keys_of(tile):
        straight = kv_all[pl.ds(2 * tile, 2)].reshape(kt, rows)
        return straight, pltpu.roll(straight.astype(f32), hd, 1).astype(bf)

    near = y // 2
    side = 2 * head - 1
    tiles = [lax.rem(near + k * side + NY // 2, NY // 2) for k in (0, 1, -1, 2)]

    def kv_waits(k):
        for u in range(2):
            src = 2 * tiles[k] + u

            @pl.when(src != y)
            def _():
                kv_copy(kv_other, src, 0, lax.rem(y + 1, NY)).wait_recv()

    def to_owner(j, e, sp):
        return remote(o_send.at[j, e], o_recv.at[j, e], o_ss.at[j, e], o_rs.at[j, e], sp, t)

    sublane = lax.broadcasted_iota(jnp.int32, (8, rows), 0)
    first = sublane < 4

    def finish(j):
        part = slice(PLACE[j] * rows, (PLACE[j] + 1) * rows)
        last = NY // 2 - 1
        acc = o_seg[last, part]
        carry = t_seg[last, part]
        for n in range(last - 1, -1, -1):
            acc = acc + jnp.exp2(-carry) * o_seg[n, part]
            carry = carry + t_seg[n, part]
        over = carry.T
        compact = jnp.where(first, over[0:8], over[hd : hd + 8])
        high = compact.astype(bf).astype(f32)
        parted = jnp.where(lax.rem(sublane, 4) < 2, high, compact - high).astype(bf)
        for e in range(2):
            o_send[j, e, :half] = acc[e * half : (e + 1) * half].astype(bf)
            o_send[j, e, half:] = parted
        if j == 0:
            start(to_owner(0, 1, z * NY + y_other))
        else:
            @pl.when(z + j < NZ)
            def _():
                for e in range(2):
                    to_owner(j, e, (z + j) * NY + (y_other if e else y)).start()
        return acc[:half], compact

    def segments(*pairs):
        segment(pairs)

    q_wait(0, 1)
    q_send(1, 4, 5, 3, 2, 6, 7)
    q_waits((1,))
    kv_waits(0)
    segments((0, 0))
    windowed()
    kv_waits(1)
    kv_waits(2)
    kv_waits(3)
    segments((0, 1), (0, 2), (0, 3))
    own_o, own_t = finish(0)
    finish(1)

    for m, js in ((1, (3, 2)), (3, (4, 5)), (2, (6, 7))):
        @pl.when(z + min(js) < NZ)
        def _():
            q_waits(js)
            segments(*((m, k) for k in range(NY // 2)))
            for j in js:
                finish(j)

    def from_owner(j, e):
        frm = lax.rem(z + NZ - j, NZ) * NY + (y_other if e else y)
        to_owner(j, e, frm).wait_recv()

    def logs_of(j, e):
        parted = o_recv[j, e, half:].astype(f32)
        return parted + pltpu.roll(parted, 6, 0)

    from_owner(0, 1)
    for j in range(1, NZ):
        @pl.when(z - j >= 0)
        def _():
            from_owner(j, 0)
            from_owner(j, 1)

    left8 = left[:8]
    carry = jnp.where(left8, own_t, logs_of(0, 1))
    scales = []
    for j in range(1, NZ):
        scales.append(jnp.exp2(-carry))
        carry = carry + jnp.where(left8, logs_of(j, 0), logs_of(j, 1))
    scales = jnp.concatenate(scales + [jnp.zeros((rows - 8 * (NZ - 1), rows), f32)], axis=0).T
    acc = jnp.concatenate([own_o, o_recv[0, 1, :half].astype(f32)], axis=0)
    for j in range(1, NZ):
        at = 8 * (j - 1)
        here = jnp.concatenate([o_recv[j, 0, :half].astype(f32), o_recv[j, 1, :half].astype(f32)], axis=0)
        acc = acc + jnp.where(left, scales[:, at : at + 1], scales[:, at + 4 : at + 5]) * here
    head0 = jnp.where(head == 0, acc[:half], acc[half:])
    head1 = jnp.where(head == 0, acc[half:], acc[:half])
    s_out = jnp.concatenate(
        [
            jnp.where(left_half, head0, pltpu.roll(head1, hd, 1)),
            jnp.where(left_half, pltpu.roll(head0, hd, 1), head1),
        ],
        axis=0,
    ).astype(bf).astype(f32)
    l_os.wait()
    gained = (s_out * sgain[...].reshape(1, rows)).astype(bf)
    own_sums = jnp.broadcast_to(jnp.sum(s_out * s_out, axis=1, keepdims=True), (rows, rows))
    part = feats // 2
    pieces = ((a_keep0, d_send0, d_recv0, r_send0, r_recv0), (a_keep1, d_send1, d_recv1, r_send1, r_recv1))
    left_cut = left[:cut].reshape(1, cut, rows)

    def halves(values):
        return jnp.where(core == 0, values[:, 0], values[:, 1]), jnp.where(core == 0, values[:, 1], values[:, 0])

    def in_two(values):
        high = values.astype(bf).astype(f32)
        return jnp.where(left_cut, high, values - high).astype(bf)

    def joined(values):
        return values + pltpu.roll(values, hd, values.ndim - 1)

    def across(n):
        return remote(pieces[n][1], pieces[n][2], d_ss.at[n], d_rs.at[n], s, partner)

    def along(n, dx):
        to = lax.rem(chip + dx, NX)
        return remote(
            pieces[n][3].at[to], pieces[n][4].at[chip], r_ss.at[n, dx], r_rs.at[n, chip], s, to * 2 + core
        )

    for n, (keep, d_send, _, _, _) in enumerate(pieces):
        mine, theirs = halves(dot(gained, vos[:, n * part : (n + 1) * part]).reshape(NX, 2, cut, part))
        keep[:, :, :part] = mine
        d_send[:, :, :part] = theirs.astype(bf)
        if n == 0:
            mine, theirs = halves(own_sums.reshape(NX, 2, cut, rows))
            keep[:, :, part:] = mine
            d_send[:, :, part:] = in_two(theirs)
        start(across(n))
    inv_w = take(b_send, b_recv, b_ss, b_rs, total.at[1], NT * rows)
    total[1] = total[1] * inv_w
    for n, (keep, _, d_recv, r_send, _) in enumerate(pieces):
        across(n).wait_recv()
        r_send[:, :, :part] = (keep[:, :, :part] + d_recv[:, :, :part].astype(f32)).astype(bf)
        if n == 0:
            r_send[:, :, part:] = in_two(keep[:, :, part:] + joined(d_recv[:, :, part:].astype(f32)))
        for dx in (2, 1, 3):
            start(along(n, dx))
    sums = None
    for n, (_, _, _, r_send, r_recv) in enumerate(pieces):
        got = r_send[chip].astype(f32)
        for dx in (1, 3, 2):
            frm = lax.rem(chip + dx, NX)
            remote(
                r_send.at[frm], r_recv.at[frm], r_ss.at[n, dx], r_rs.at[n, frm], s, partner
            ).wait_recv()
            got = got + r_recv[frm].astype(f32)
        total[0, :, n * part : (n + 1) * part] = got[:, :part]
        if n == 0:
            sums = joined(got[:, part:])
    inv_s = lax.rsqrt(sums[:, :1] * (1.0 / (NT * rows)) + EPS)
    both = (total[0] * inv_s + total[1]).astype(bf).astype(f32)
    stats = jnp.sum(both * both, axis=1, keepdims=True) * (1.0 / feats)
    out_buf[...] = both * lax.rsqrt(stats + EPS)

    out_copy = pltpu.make_async_copy(out_buf, out, out_sem)
    out_copy.start()
    for copy in given(b_send, b_recv, b_ss, b_rs):
        copy.wait_send()
    for copy in sends:
        copy.wait_send()
    for j in range(1, NZ):
        for e in range(2):
            @pl.when(z - j >= 0)
            def _():
                q_copy(j, e, z - j).wait_send()

            @pl.when(z + j < NZ)
            def _():
                to_owner(j, e, (z + j) * NY + (y_other if e else y)).wait_send()

    @pl.when(s < N_SP - 1)
    def _():
        prev_copy(s + 1).wait_send()

    out_copy.wait()


def one_kernel(*args):
    tokens, pre_gain, wqs, wks, wvs, wqw, wkw, wvw, bias, sinks, sgain, wgain, wos, wow, post_gain = args
    bf = jnp.bfloat16
    f32 = jnp.float32
    rows, chunk = tokens.shape
    feats = NT * chunk
    cut = rows // NT
    widths = (feats // 2 + rows, feats // 2)
    v = pltpu.VMEM
    dma = pltpu.SemaphoreType.DMA
    anywhere = pl.BlockSpec(memory_space=pl.ANY)
    scratch = [
        v(pre_gain.shape, f32), pltpu.SMEM(bias.shape, f32), pltpu.SMEM(sinks.shape, f32),
        v(sgain.shape, f32), v(wgain.shape, f32), v(post_gain.shape, f32),
        v((NT, rows, chunk), bf), v((rows, rows), f32), v((rows, 4 * rows), f32), v((feats, 4 * rows), bf),
        v((rows, rows), f32), v((rows, feats), bf),
        v(wos.shape, bf), v(wow.shape, bf),
        v((NY, rows, rows), bf), v((rows, rows), bf), v((NZ, 2, rows // 2, rows), bf), v((rows // 2, rows), bf),
        v((NY // 2, NZ * rows, rows), f32), v((NY // 2, NZ * rows, rows), f32),
        v((rows, rows), bf), v((rows, rows), f32), v((rows, rows), bf),
        v((NZ, 2, rows // 2 + 8, rows), bf), v((NZ, 2, rows // 2 + 8, rows), bf),
        *(v((NX, cut, width), f32) for width in widths),
        *(v((NX, cut, width), bf) for _ in range(4) for width in widths),
        v((NT, cut, feats + rows), bf), v((NT, cut, feats + rows), bf), v((2, cut, feats), f32), v((cut, feats), f32),
        dma((14,)), dma, dma((8,)), dma((NT,)), dma((NY,)), dma((NY,)), dma((NZ, 2)), dma((NZ, 2)), dma, dma,
        dma((NZ, 2)), dma((NZ, 2)), dma((2,)), dma((2,)), dma((2, NX)), dma((2, NX)), dma((NT,)), dma((NT,)), dma,
        pltpu.SemaphoreType.REGULAR,
    ]
    normed = pl.pallas_call(
        kernel,
        out_shape=jax.ShapeDtypeStruct((cut, feats), f32),
        in_specs=[anywhere] * len(args),
        out_specs=anywhere,
        scratch_shapes=scratch,
        compiler_params=pltpu.CompilerParams(
            collective_id=0, has_side_effects=True, vmem_limit_bytes=67043328
        ),
        name="layer",
    )(*args[:6], wkw.T, wvw.T, *args[8:])
    return (normed * post_gain.reshape(1, feats)).astype(bf)


def solution(mesh):
    in_specs = (
        P("sp", "tp"),
        P(),
        P(None, "tp"),
        P(None, "tp"),
        P(None, "tp"),
        P(None, "tp"),
        P(None, "tp"),
        P(None, "tp"),
        P("tp"),
        P("tp"),
        P("tp"),
        P("tp"),
        P("tp", None),
        P("tp", None),
        P(),
    )
    return jax.shard_map(
        one_kernel,
        mesh=mesh,
        in_specs=in_specs,
        out_specs=P(("sp", "tp"), None),
        check_vma=False,
    )
```
